512 devices in a mesh: sp: 16 (over z), fs: 4 (over y), tp: 8 (over x, core).
Axes of the slice: x: 4, y: 4, z: 16, core: 2. Of those that a mesh axis runs over, the one named last changes fastest.
Arguments:
- tokens: bfloat16 [4, 4096, 2048], P('fs', 'sp'), may hold values from -6 to 6
- mix_gain: float32 [2048], replicated, may hold values from 0.1 to 1.9
- query_down: bfloat16 [2048, 768], P('fs', 'tp'), may hold values from -0.125 to 0.125
- memory_down: bfloat16 [2048, 512], P('fs', 'tp'), may hold values from -0.125 to 0.125
- rope_weight: bfloat16 [2048, 32], replicated, may hold values from -0.125 to 0.125
- query_up: bfloat16 [768, 1536], P('fs', 'tp'), may hold values from -0.21875 to 0.21875
- key_up: bfloat16 [512, 1024], P('fs', 'tp'), may hold values from -0.25 to 0.25
- value_up: bfloat16 [512, 1024], P('fs', 'tp'), may hold values from -0.25 to 0.25
- latent_gain: float32 [768], replicated, may hold values from 0.1 to 1.9
- memory_gain: float32 [512], replicated, may hold values from 0.1 to 1.9
- query_gain: float32 [96], replicated, may hold values from 1 to 16
- key_gain: float32 [96], replicated, may hold values from 0.1 to 1.9
- conv_value: bfloat16 [2048, 1024], P('fs', 'tp'), may hold values from -1 to 1
- conv_gate: bfloat16 [2048, 1024], P('fs', 'tp'), may hold values from -0.125 to 0.125
- conv_kernel: bfloat16 [31, 1024], P(None, 'tp'), may hold values from -50 to 50
- channel_gain: float32 [1024], P('tp'), may hold values from 0.1 to 1.9
- channel_shift: float32 [1024], P('tp'), may hold values from -3 to 3
- heads_out: bfloat16 [1024, 2048], P('tp', 'fs'), may hold values from -0.75 to 0.75
- conv_out: bfloat16 [1024, 2048], P('tp', 'fs'), may hold values from -0.1875 to 0.1875
Outputs:
- mixed: bfloat16 [4, 4096, 2048], P('fs', 'sp')
The draws below stay inside these ranges and needn't reach their ends.
All inputs are finite; a program needn't handle non-finite values.
Results may differ from the reference program's by a relative error of at most 0.015.
The reference program's roundings to bfloat16 on the way count: a program that leaves them out, or rounds other values in their place, can miss the bound.
Values may be sent and summed in bfloat16 or wider, within the bound.
No kernel may reach another device: no remote copies, remote signals or barrier semaphores. Data moves between devices by JAX's collectives and lax.ppermute only.
A program may use at most 64 MiB of HBM per device.

```python
import math
import jax
import jax.numpy as jnp
from jax import lax

D = 2048
HEADS = 16
QK_NOPE = 64
QK_ROPE = 32
V_DIM = 64
Q_LAT = 768
KV_LAT = 512
CONV_W = 1024
CONV_K = 31
SEG = 64
TOK_DEV = 256
QK_DIM = 96
SEQ = 4096
SEQS = 4
N_TP = 8


def draw_query_gain(key, part):
    gain_key = jax.random.fold_in(key, 11)
    return jnp.exp(jax.random.uniform(gain_key, (QK_DIM,), jnp.float32, 0.0, math.log(3.0)))


def draw_conv_value(key, part):
    noise_key, common_key, level_key = jax.random.split(jax.random.fold_in(key, 23), 3)
    noise = jnp.clip(jax.random.normal(noise_key, (D, CONV_W), jnp.float32), -5.0, 5.0)
    common = jnp.clip(jax.random.normal(common_key, (D,), jnp.float32), -5.0, 5.0)
    level = jax.random.uniform(level_key, (CONV_W,), jnp.float32, 0.5, 1.5)
    strength = 0.7
    return ((noise + strength * common[:, None] * level[None, :]) / math.sqrt(D)).astype(jnp.bfloat16)


def draw_conv_kernel(key, part):
    noise_key, scale_key = jax.random.split(jax.random.fold_in(key, 7))
    channel_pos = jnp.arange(CONV_W, dtype=jnp.float32) / CONV_W
    roughness = jnp.exp(jax.random.uniform(scale_key, (CONV_W,), jnp.float32, -0.7, 0.7))
    channel_scale = 10.0 ** channel_pos * roughness
    tap_draw = jnp.clip(jax.random.normal(noise_key, (CONV_K, CONV_W), jnp.float32), -5.0, 5.0)
    return ((tap_draw + 1.0) * channel_scale[None, :] / math.sqrt(CONV_K)).astype(jnp.bfloat16)


def steps_of(own_key, shape, cuts, least, top_value):
    level, own = 1.0, jax.random.fold_in(own_key, 6)
    for axis_at, shards_of in cuts:
        heights = jnp.exp(jax.random.uniform(jax.random.fold_in(own, axis_at), (shards_of,), jnp.float32, least / len(cuts), top_value / len(cuts)))
        level = level * jnp.repeat(heights, shape[axis_at] // shards_of).reshape([-1 if axis == axis_at else 1 for axis in range(len(shape))])
    return level


def gaussian(own_key, extent, width, reach, cuts=(), kind=jnp.bfloat16):
    factor_of = steps_of(own_key, extent, cuts, -0.22, 0.18) if cuts else 1.0
    drawn = jax.random.normal(own_key, extent, jnp.float32) * width * factor_of
    return jnp.minimum(jnp.maximum(drawn, -reach), reach).astype(kind)


def setup_inputs(seed: int = 0) -> dict:
    arg_keys = jax.random.split(jax.random.key(seed), 20)
    return {
        "tokens": gaussian(arg_keys[0], (SEQS, SEQ, D), 1.0, 6.0, ((0, 4), (1, 16))),
        "mix_gain": jnp.clip(1.0 + 0.18 * jax.random.normal(arg_keys[1], (D,), jnp.float32), 0.1, 1.9),
        "query_down": gaussian(arg_keys[2], (D, Q_LAT), D ** -0.5, 0.125, ((0, 4), (1, 8))),
        "memory_down": gaussian(arg_keys[3], (D, KV_LAT), D ** -0.5, 0.125, ((0, 4), (1, 8))),
        "rope_weight": gaussian(arg_keys[4], (D, QK_ROPE), D ** -0.5, 0.125),
        "query_up": gaussian(arg_keys[5], (Q_LAT, HEADS * QK_DIM), Q_LAT ** -0.5, 0.21875, ((0, 4), (1, 8))),
        "key_up": gaussian(arg_keys[6], (KV_LAT, HEADS * QK_NOPE), KV_LAT ** -0.5, 0.25, ((0, 4), (1, 8))),
        "value_up": gaussian(arg_keys[7], (KV_LAT, HEADS * V_DIM), KV_LAT ** -0.5, 0.25, ((0, 4), (1, 8))),
        "latent_gain": jnp.clip(1.0 + 0.18 * jax.random.normal(arg_keys[8], (Q_LAT,), jnp.float32), 0.1, 1.9),
        "memory_gain": jnp.clip(1.0 + 0.18 * jax.random.normal(arg_keys[9], (KV_LAT,), jnp.float32), 0.1, 1.9),
        "query_gain": draw_query_gain(jax.random.fold_in(arg_keys[19], 71), 0),
        "key_gain": jnp.clip(1.0 + 0.18 * jax.random.normal(arg_keys[11], (QK_DIM,), jnp.float32), 0.1, 1.9),
        "conv_value": draw_conv_value(jax.random.fold_in(arg_keys[19], 71), 0),
        "conv_gate": gaussian(arg_keys[13], (D, CONV_W), D ** -0.5, 0.125, ((0, 4), (1, 8))),
        "conv_kernel": draw_conv_kernel(jax.random.fold_in(arg_keys[19], 71), 0),
        "channel_gain": jnp.clip(1.0 + 0.18 * jax.random.normal(arg_keys[15], (CONV_W,), jnp.float32), 0.1, 1.9),
        "channel_shift": gaussian(arg_keys[16], (CONV_W,), 0.5, 3.0, ((0, 8),), jnp.float32),
        "heads_out": gaussian(arg_keys[17], (HEADS * V_DIM, D), V_DIM ** -0.5, 0.75, ((0, 8), (1, 4))),
        "conv_out": gaussian(arg_keys[18], (CONV_W, D), CONV_W ** -0.5, 0.1875, ((0, 8), (1, 4))),
    }


epsilon = 1e-06
rope_base = 10000.0
masked_score = -1e+30

def norm_rows(matrix, scale_vector):
    return matrix * lax.rsqrt(lax.optimization_barrier(jnp.mean(matrix * matrix, axis=-1, keepdims=True)) + epsilon) * scale_vector.astype(jnp.float32)

def rope_tables(positions):
    inverse_freq = 1.0 / rope_base ** (jnp.arange(0, QK_ROPE, 2, dtype=jnp.float32) / QK_ROPE)
    angles = positions.astype(jnp.float32)[:, None] * inverse_freq[None, :]
    return (jnp.cos(angles)[:, None, :], jnp.sin(angles)[:, None, :])

def rotate(matrix, cosine_table, sine_table):
    half_width = matrix.shape[-1] // 2
    front_half = matrix[..., :half_width]
    back_half = matrix[..., half_width:]
    return jnp.concatenate([front_half * cosine_table - back_half * sine_table, front_half * sine_table + back_half * cosine_table], axis=-1)

def heads_query(latent, weight, scale_vector, cosine_table, sine_table):
    row_count = latent.shape[0]
    projected = jnp.dot(latent, weight, preferred_element_type=jnp.float32)
    projected = norm_rows(projected.reshape(row_count, weight.shape[1] // QK_DIM, QK_DIM), scale_vector)
    turned = rotate(projected[..., QK_NOPE:], cosine_table, sine_table)
    return jnp.concatenate([projected[..., :QK_NOPE], turned], axis=-1).astype(jnp.bfloat16)

def heads_key(latent, rope_rows, weight, scale_vector, cosine_table, sine_table):
    row_count = latent.shape[0]
    head_count = weight.shape[1] // QK_NOPE
    nope_part = jnp.dot(latent, weight, preferred_element_type=jnp.float32).reshape(row_count, head_count, QK_NOPE)
    shared = jnp.broadcast_to(rope_rows.astype(jnp.float32)[:, None, :], (row_count, head_count, QK_ROPE))
    joined = norm_rows(jnp.concatenate([nope_part, shared], axis=-1), scale_vector)
    turned = rotate(joined[..., QK_NOPE:], cosine_table, sine_table)
    return jnp.concatenate([joined[..., :QK_NOPE], turned], axis=-1).astype(jnp.bfloat16)

def depthwise(extended, kernel, row_count):

    def add_tap(tap_index, running):
        window = lax.dynamic_slice_in_dim(extended, tap_index.astype(jnp.int32), row_count, 0).astype(jnp.float32)
        weight_row = lax.dynamic_slice_in_dim(kernel, tap_index.astype(jnp.int32), 1, 0).astype(jnp.float32)
        return running + window * weight_row
    return lax.fori_loop(0, kernel.shape[0], add_tap, jnp.zeros((row_count, kernel.shape[1]), jnp.float32))

def attention_block(queries, key_rows, value_rows, query_pos):
    key_pos = jnp.arange(key_rows.shape[0], dtype=jnp.int32)
    scores = jnp.einsum('qhd,khd->qhk', queries.astype(jnp.float32), key_rows.astype(jnp.float32)) * QK_DIM ** (-0.5)
    allowed = ((key_pos // SEG)[None, :] <= (query_pos // SEG)[:, None])[:, None, :]
    scores = jnp.where(allowed, scores, masked_score)
    row_max = lax.optimization_barrier(jnp.max(scores, axis=2, keepdims=True))
    weights = jnp.where(allowed, jnp.exp(scores - row_max), 0.0)
    row_total = lax.optimization_barrier(jnp.sum(weights, axis=2))
    rounded = weights.astype(jnp.bfloat16)
    summed = jnp.einsum('qhk,khd->qhd', rounded.astype(jnp.float32), value_rows.astype(jnp.float32))
    return (summed / row_total[:, :, None]).astype(jnp.bfloat16)

def one_sequence(tokens, mix_gain, query_down, memory_down, rope_weight, query_up, key_up, value_up, latent_gain, memory_gain, query_gain, key_gain, conv_value, conv_gate, conv_kernel, channel_gain, channel_shift, heads_out, conv_out):
    normed = norm_rows(tokens.astype(jnp.float32), mix_gain).astype(jnp.bfloat16)
    latent_query = jnp.dot(normed, query_down, preferred_element_type=jnp.float32).astype(jnp.bfloat16)
    latent_memory = jnp.dot(normed, memory_down, preferred_element_type=jnp.float32).astype(jnp.bfloat16)
    rope_rows = jnp.dot(normed, rope_weight, preferred_element_type=jnp.float32).astype(jnp.bfloat16)
    value_part = jnp.dot(normed, conv_value, preferred_element_type=jnp.float32)
    gate_part = jnp.dot(normed, conv_gate, preferred_element_type=jnp.float32)
    gated = (value_part * jax.nn.sigmoid(gate_part)).astype(jnp.bfloat16)
    query_normed = norm_rows(latent_query.astype(jnp.float32), latent_gain).astype(jnp.bfloat16)
    memory_normed = norm_rows(latent_memory.astype(jnp.float32), memory_gain).astype(jnp.bfloat16)
    positions = jnp.arange(SEQ, dtype=jnp.int32)
    cosine_table, sine_table = rope_tables(positions)
    queries = heads_query(query_normed, query_up, query_gain, cosine_table, sine_table)
    key_rows = heads_key(memory_normed, rope_rows, key_up, key_gain, cosine_table, sine_table)
    value_rows = jnp.dot(memory_normed, value_up, preferred_element_type=jnp.float32).astype(jnp.bfloat16).reshape(SEQ, HEADS, V_DIM)
    query_blocks = queries.reshape(SEQ // TOK_DEV, TOK_DEV, HEADS, QK_DIM)
    block_pos = positions.reshape(SEQ // TOK_DEV, TOK_DEV)

    def per_block(pair):
        return attention_block(pair[0], key_rows, value_rows, pair[1])
    attention = lax.map(per_block, (query_blocks, block_pos)).reshape(SEQ, HEADS * V_DIM)
    extended = jnp.concatenate([jnp.zeros((CONV_K - 1, CONV_W), jnp.bfloat16), gated], axis=0)
    conv_sum = depthwise(extended, conv_kernel, SEQ)
    row_mean = lax.optimization_barrier(jnp.mean(conv_sum, axis=1, keepdims=True))
    centered = conv_sum - row_mean
    spread = lax.optimization_barrier(jnp.mean(centered * centered, axis=1, keepdims=True))
    conv_result = jax.nn.silu(centered * lax.rsqrt(spread + epsilon) * channel_gain.astype(jnp.float32) + channel_shift.astype(jnp.float32)).astype(jnp.bfloat16)
    attn_width = HEADS * V_DIM // N_TP
    conv_width = CONV_W // N_TP
    mixed = jnp.zeros((SEQ, D), jnp.float32)
    for group_index in range(N_TP):
        head_cols = slice(group_index * attn_width, (group_index + 1) * attn_width)
        conv_cols = slice(group_index * conv_width, (group_index + 1) * conv_width)
        partial_sum = jnp.dot(attention[:, head_cols], heads_out[head_cols], preferred_element_type=jnp.float32)
        partial_sum = partial_sum + jnp.dot(conv_result[:, conv_cols], conv_out[conv_cols], preferred_element_type=jnp.float32)
        mixed = mixed + lax.optimization_barrier(partial_sum.astype(jnp.bfloat16)).astype(jnp.float32)
    return mixed.astype(jnp.bfloat16)

def reference(tokens, mix_gain, query_down, memory_down, rope_weight, query_up, key_up, value_up, latent_gain, memory_gain, query_gain, key_gain, conv_value, conv_gate, conv_kernel, channel_gain, channel_shift, heads_out, conv_out):

    def per_sequence(sequence):
        return one_sequence(sequence, mix_gain, query_down, memory_down, rope_weight, query_up, key_up, value_up, latent_gain, memory_gain, query_gain, key_gain, conv_value, conv_gate, conv_kernel, channel_gain, channel_shift, heads_out, conv_out)
    return lax.map(per_sequence, tokens)
```

```python
import jax
import jax.numpy as jnp
from jax import lax
from jax.experimental import pallas as pl
from jax.experimental.pallas import tpu as pltpu
from jax.sharding import PartitionSpec as P

QK_NOPE = 64
QK_ROPE = 32
V_DIM = 64
CONV_W = 1024
SEG = 64
QK_DIM = 96
Q_LAT = 768
KV_LAT = 512
ROWS = 256
TAPS = 31
HALO = 32
LANES = 128
N_FS = 4
N_TP = 8
N_SP = 16
CHUNK = 512

epsilon = 1e-06
rope_base = 10000.0
masked_score = -1e30
log2_e = 1.4426950408889634
bf16 = jnp.bfloat16
f32 = jnp.float32

SAME_CORE = [[0, 2, 4, 6], [1, 3, 5, 7]]
CORE_PAIRS = [(i, i ^ 1) for i in range(N_TP)]


def call(kernel, out_shape, scratch=(), scalars=0, arrays=0):
    specs = {}
    if scalars:
        smem = pl.BlockSpec(memory_space=pltpu.SMEM)
        specs["in_specs"] = [smem] * scalars + [pl.BlockSpec(memory_space=pltpu.VMEM)] * arrays
    return pl.pallas_call(
        kernel,
        out_shape=out_shape,
        **specs,
        scratch_shapes=list(scratch),
        compiler_params=pltpu.CompilerParams(vmem_limit_bytes=48 * 1024 * 1024),
    )


def norm_rows(matrix, scale_vector):
    return (
        matrix
        * lax.rsqrt(jnp.mean(matrix * matrix, axis=-1, keepdims=True) + epsilon)
        * scale_vector
    )


def head_tile(tile, gain, cosine, sine_up, sine_down):
    scale = lax.rsqrt(jnp.sum(tile * tile, axis=-1, keepdims=True) * (1.0 / QK_DIM) + epsilon)
    tile = tile * scale * gain
    half = QK_ROPE // 2
    return (
        tile * cosine
        + pltpu.roll(tile, LANES - half, 1) * sine_up
        + pltpu.roll(tile, half, 1) * sine_down
    )


def keys_values_kernel(lat_ref, rope_ref, w_ref, mgain_ref, kgain_ref, cos_ref, up_ref, down_ref, out_ref, m_scr, w_scr):
    total = jnp.zeros((ROWS, 1), f32)
    for g in range(N_TP):
        piece = lat_ref[g, :, :64].astype(f32)
        total = total + jnp.sum(piece * piece, axis=-1, keepdims=True)
    scale = lax.rsqrt(total * (1.0 / KV_LAT) + epsilon)
    for g in range(N_TP):
        piece = lat_ref[g, :, :64].astype(f32)
        cols = slice(g * 64, (g + 1) * 64)
        m_scr[:, cols] = (piece * scale * mgain_ref[:, cols]).astype(bf16)
    for f in range(N_FS):
        for b in range(4):
            w_scr[f * 128 : (f + 1) * 128, b * 64 : (b + 1) * 64] = w_ref[
                f, b * 128 : (b + 1) * 128, :64
            ]
    both = jnp.dot(m_scr[...], w_scr[...], preferred_element_type=f32)
    nope = both[:, :LANES]
    lane = lax.broadcasted_iota(jnp.int32, (ROWS, LANES), 1)
    rope = rope_ref[...].astype(f32)
    for h in range(2):
        part = nope if h == 0 else pltpu.roll(nope, 64, 1)
        tile = jnp.where(lane < QK_NOPE, part, rope)
        out_ref[:, h * LANES : (h + 1) * LANES] = head_tile(
            tile, kgain_ref[...], cos_ref[...], up_ref[...], down_ref[...]
        ).astype(bf16)
    out_ref[:, 2 * LANES :] = both[:, LANES:].astype(bf16)


def queries_kernel(lat_ref, w_ref, lgain_ref, qgain_ref, cos_ref, up_ref, down_ref, out_ref, q_scr):
    total = jnp.zeros((ROWS, 1), f32)
    for g in range(N_TP):
        piece = lat_ref[g, :, 64:].astype(f32)
        total = total + jnp.sum(piece * piece, axis=-1, keepdims=True)
    scale = lax.rsqrt(total * (1.0 / Q_LAT) + epsilon)
    for g in range(N_TP):
        piece = lat_ref[g, :, 64:].astype(f32)
        cols = slice(g * 96, (g + 1) * 96)
        q_scr[:, cols] = (piece * scale * lgain_ref[:, cols]).astype(bf16)
    both = jnp.zeros((ROWS, 2 * LANES), f32)
    for f in range(N_FS):
        both = both + jnp.dot(
            q_scr[:, f * 192 : (f + 1) * 192], w_ref[f, 512:704, :], preferred_element_type=f32
        )
    for h in range(2):
        out_ref[:, h * LANES : (h + 1) * LANES] = head_tile(
            both[:, h * LANES : (h + 1) * LANES],
            qgain_ref[...],
            cos_ref[...],
            up_ref[...],
            down_ref[...],
        ).astype(bf16)


def gated_kernel(normed_ref, w_ref, out_ref):
    both = jnp.zeros((ROWS, 2 * LANES), f32)
    for f in range(N_FS):
        both = both + jnp.dot(
            normed_ref[:, f * 512 : (f + 1) * 512], w_ref[f, :512, :], preferred_element_type=f32
        )
    out_ref[...] = (both[:, :LANES] * jax.nn.sigmoid(both[:, LANES:])).astype(bf16)


def conv_kernel_body(halo_ref, gated_ref, taps_ref, sum_ref, first_ref, second_ref, ext_scr):
    ext_scr[:HALO, :] = halo_ref[...].astype(f32)
    ext_scr[HALO:, :] = gated_ref[...].astype(f32)
    start = HALO - (TAPS - 1)
    block = 64
    for r in range(0, ROWS, block):
        running = jnp.zeros((block, LANES), f32)
        for j in range(TAPS):
            running = running + ext_scr[pl.ds(r + start + j, block), :] * taps_ref[j : j + 1, :]
        sum_ref[r : r + block, :] = running
        total = jnp.sum(running, axis=-1, keepdims=True)
        off = running - total * (1.0 / LANES)
        first_ref[r : r + block, :] = total
        second_ref[r : r + block, :] = jnp.sum(off * off, axis=-1, keepdims=True)


def attention_kernel(at_ref, q_ref, kv_ref, conv_ref, heads_ref, conv_w_ref, out_ref):
    at = at_ref[0]
    rate = QK_DIM ** (-0.5) * log2_e
    heads = [q_ref[:, h * LANES : (h + 1) * LANES] for h in range(2)]

    def part(state, chunk, mask):
        block = pl.multiple_of(chunk * CHUNK, CHUNK)
        values = kv_ref[pl.ds(block, CHUNK), 2 * LANES :]
        fresh = []
        for h in range(2):
            top, total, weighted = state[h]
            keys = kv_ref[pl.ds(block, CHUNK), h * LANES : (h + 1) * LANES]
            scores = lax.dot_general(
                heads[h], keys, (((1,), (1,)), ((), ())), preferred_element_type=f32
            ) * rate
            if mask is not None:
                scores = jnp.where(mask, scores, masked_score)
            new_top = jnp.maximum(top, jnp.max(scores, axis=-1, keepdims=True))
            weights = jnp.exp2(scores - new_top)
            factor = jnp.exp2(top - new_top)
            total = total * factor + jnp.sum(weights, axis=-1, keepdims=True)
            weighted = weighted * factor + jnp.dot(
                weights.astype(bf16), values, preferred_element_type=f32
            )
            fresh.append((new_top, total, weighted))
        return tuple(fresh)

    last = at // (CHUNK // ROWS)
    row = lax.broadcasted_iota(jnp.int32, (ROWS, CHUNK), 0) + at * ROWS
    col = lax.broadcasted_iota(jnp.int32, (ROWS, CHUNK), 1) + last * CHUNK
    mask = jnp.right_shift(col, 6) <= jnp.right_shift(row, 6)
    empty = (
        jnp.full((ROWS, 1), masked_score, f32),
        jnp.zeros((ROWS, 1), f32),
        jnp.zeros((ROWS, LANES), f32),
    )
    state = part((empty, empty), last, mask)
    state = lax.fori_loop(0, last, lambda c, s: part(s, c, None), state)
    lane = lax.broadcasted_iota(jnp.int32, (ROWS, LANES), 1)
    result = jnp.where(
        lane < V_DIM, state[0][2] / state[0][1], state[1][2] / state[1][1]
    ).astype(bf16)
    conv = conv_ref[...]
    for f in range(N_FS):
        out_ref[:, f * 512 : (f + 1) * 512] = (
            jnp.dot(result, heads_ref[f], preferred_element_type=f32)
            + jnp.dot(conv, conv_w_ref[f], preferred_element_type=f32)
        ).astype(bf16)


def rotation_tables(positions):
    inverse_freq = 1.0 / rope_base ** (jnp.arange(0, QK_ROPE, 2, dtype=f32) / QK_ROPE)
    angles = positions.astype(f32)[:, None] * inverse_freq[None, :]
    cosine, sine = jnp.cos(angles), jnp.sin(angles)
    rows = positions.shape[0]
    ones = jnp.ones((rows, QK_NOPE), f32)
    zeros = jnp.zeros((rows, QK_NOPE), f32)
    pad = jnp.zeros((rows, LANES - QK_DIM), f32)
    none = jnp.zeros_like(sine)
    return (
        jnp.concatenate([ones, cosine, cosine, pad], axis=1),
        jnp.concatenate([zeros, -sine, none, pad], axis=1),
        jnp.concatenate([zeros, none, sine, pad], axis=1),
    )


def local(
    tokens,
    mix_gain,
    query_down,
    memory_down,
    rope_weight,
    query_up,
    key_up,
    value_up,
    latent_gain,
    memory_gain,
    query_gain,
    key_gain,
    conv_value,
    conv_gate,
    conv_kernel,
    channel_gain,
    channel_shift,
    heads_out,
    conv_out,
):
    at = lax.axis_index("sp")
    query_pad = jnp.pad(query_up.reshape(192, 2, QK_DIM), ((0, 0), (0, 0), (0, 32))).reshape(192, 256)
    wide = jnp.concatenate([jnp.concatenate([conv_value, conv_gate], axis=1), query_pad], axis=0)
    wide_all = lax.all_gather(wide, "fs")
    up = jnp.concatenate(
        [key_up[:, :64], key_up[:, 64:], value_up[:, :64], value_up[:, 64:]], axis=0
    )
    narrow = jnp.concatenate([up, memory_down, query_down], axis=1)
    normed = norm_rows(tokens[0].astype(f32), mix_gain).astype(bf16)
    rope_pad = jnp.pad(rope_weight, ((0, 0), (QK_NOPE, LANES - QK_DIM)))
    rope_rows = jnp.dot(normed, rope_pad, preferred_element_type=f32).astype(bf16)
    narrow_all = lax.all_gather(narrow, "fs")
    projected = jnp.dot(
        normed, narrow_all.reshape(2048, 224), preferred_element_type=f32
    ).astype(bf16)
    latents = lax.all_gather(projected[:, 64:], "tp")
    positions = at * ROWS + jnp.arange(ROWS, dtype=jnp.int32)
    cosine, sine_up, sine_down = rotation_tables(positions)

    def row(vector, width):
        return jnp.pad(vector, (0, width - vector.shape[0]))[None, :]

    own = call(
        keys_values_kernel,
        jax.ShapeDtypeStruct((ROWS, 3 * LANES), bf16),
        [pltpu.VMEM((ROWS, KV_LAT), bf16), pltpu.VMEM((KV_LAT, 256), bf16)],
    )(
        latents, rope_rows, narrow_all, memory_gain[None, :], row(key_gain, LANES),
        cosine, sine_up, sine_down,
    )
    pieces = lax.all_gather(own, "sp", axis=0, tiled=True)
    queries = call(
        queries_kernel,
        jax.ShapeDtypeStruct((ROWS, 2 * LANES), bf16),
        [pltpu.VMEM((ROWS, Q_LAT), bf16)],
    )(
        latents, wide_all, latent_gain[None, :], row(query_gain, LANES),
        cosine, sine_up, sine_down,
    )
    gated = call(gated_kernel, jax.ShapeDtypeStruct((ROWS, LANES), bf16))(normed, wide_all)
    halo = lax.ppermute(gated[ROWS - HALO :], "sp", [(i, i + 1) for i in range(N_SP - 1)])
    taps = jnp.pad(conv_kernel.astype(f32), ((0, 1), (0, 0)))
    column = jax.ShapeDtypeStruct((ROWS, 1), f32)
    conv_sum, first, second = call(
        conv_kernel_body,
        (jax.ShapeDtypeStruct((ROWS, LANES), f32), column, column),
        [pltpu.VMEM((ROWS + HALO, LANES), f32)],
    )(halo, gated, taps)
    stats = jnp.concatenate([first[:, 0], second[:, 0]])
    stats = jnp.broadcast_to(stats, (N_TP, 1, 2 * ROWS))
    stats = lax.all_to_all(stats, "tp", split_axis=0, concat_axis=0, tiled=True)[:, 0]
    sums, squares = stats[:, :ROWS], stats[:, ROWS:]
    row_mean = jnp.sum(sums, axis=0) * (1.0 / CONV_W)
    apart = sums * (1.0 / LANES) - row_mean[None, :]
    spread = jnp.sum(squares + LANES * apart * apart, axis=0) * (1.0 / CONV_W)
    conv_result = jax.nn.silu(
        (conv_sum - row_mean[:, None]) * lax.rsqrt(spread + epsilon)[:, None] * channel_gain
        + channel_shift
    ).astype(bf16)
    heads_all = lax.all_gather(heads_out, "fs")
    conv_all = lax.all_gather(conv_out, "fs")
    partial = call(
        attention_kernel, jax.ShapeDtypeStruct((ROWS, 2048), bf16), scalars=1, arrays=5
    )(at[None], queries, pieces, conv_result, heads_all, conv_all)
    share = lax.all_to_all(
        partial.reshape(N_TP, ROWS // N_TP, 2048), "tp", split_axis=0, concat_axis=0, tiled=True
    )
    share = jnp.sum(share.astype(f32), axis=0).astype(bf16)
    mine = lax.all_gather(share, "tp", axis_index_groups=SAME_CORE)
    other = lax.ppermute(mine, "tp", CORE_PAIRS)
    even = lax.axis_index("tp") % 2 == 0
    mixed = jnp.stack([jnp.where(even, mine, other), jnp.where(even, other, mine)], axis=1)
    return mixed.reshape(1, ROWS, 2048)


def solution(mesh):
    in_specs = (
        P("fs", "sp", None),
        P(),
        P("fs", "tp"),
        P("fs", "tp"),
        P(),
        P("fs", "tp"),
        P("fs", "tp"),
        P("fs", "tp"),
        P(),
        P(),
        P(),
        P(),
        P("fs", "tp"),
        P("fs", "tp"),
        P(None, "tp"),
        P("tp"),
        P("tp"),
        P("tp", "fs"),
        P("tp", "fs"),
    )
    out_specs = P("fs", "sp", None)
    return jax.shard_map(local, mesh=mesh, in_specs=in_specs, out_specs=out_specs, check_vma=False)
```

```python
import jax
import jax.numpy as jnp
from jax import lax
from jax.experimental import pallas as pl
from jax.experimental.pallas import tpu as pltpu
from jax.sharding import PartitionSpec as P

QK_NOPE = 64
QK_ROPE = 32
V_DIM = 64
CONV_W = 1024
SEG = 64
QK_DIM = 96
Q_LAT = 768
KV_LAT = 512
ROWS = 256
TAPS = 31
HALO = 32
LANES = 128
N_FS = 4
N_TP = 8
N_SP = 16

epsilon = 1e-06
rope_base = 10000.0
masked_score = -1e30
log2_e = 1.4426950408889634
bf16 = jnp.bfloat16
f32 = jnp.float32

SAME_CORE = [[0, 2, 4, 6], [1, 3, 5, 7]]
CORE_PAIRS = [(i, i ^ 1) for i in range(N_TP)]


def call(kernel, out_shape, scratch=(), scalars=0, arrays=0):
    specs = {}
    if scalars:
        smem = pl.BlockSpec(memory_space=pltpu.SMEM)
        specs["in_specs"] = [smem] * scalars + [pl.BlockSpec(memory_space=pltpu.VMEM)] * arrays
    return pl.pallas_call(
        kernel,
        out_shape=out_shape,
        **specs,
        scratch_shapes=list(scratch),
        compiler_params=pltpu.CompilerParams(vmem_limit_bytes=8 * 1024 * 1024),
    )


def norm_rows(matrix, scale_vector):
    return (
        matrix
        * lax.rsqrt(jnp.mean(matrix * matrix, axis=-1, keepdims=True) + epsilon)
        * scale_vector
    )


def head_tile(tile, gain, cosine, sine_up, sine_down):
    scale = lax.rsqrt(jnp.sum(tile * tile, axis=-1, keepdims=True) * (1.0 / QK_DIM) + epsilon)
    tile = tile * scale * gain
    half = QK_ROPE // 2
    return (
        tile * cosine
        + pltpu.roll(tile, LANES - half, 1) * sine_up
        + pltpu.roll(tile, half, 1) * sine_down
    )


def keys_values_kernel(lat_ref, rope_ref, w_ref, mgain_ref, kgain_ref, cos_ref, up_ref, down_ref, out_ref, m_scr, w_scr):
    total = jnp.zeros((ROWS, 1), f32)
    for g in range(N_TP):
        piece = lat_ref[g, :, :64].astype(f32)
        total = total + jnp.sum(piece * piece, axis=-1, keepdims=True)
    scale = lax.rsqrt(total * (1.0 / KV_LAT) + epsilon)
    for g in range(N_TP):
        piece = lat_ref[g, :, :64].astype(f32)
        cols = slice(g * 64, (g + 1) * 64)
        m_scr[:, cols] = (piece * scale * mgain_ref[:, cols]).astype(bf16)
    for f in range(N_FS):
        for b in range(4):
            w_scr[f * 128 : (f + 1) * 128, b * 64 : (b + 1) * 64] = w_ref[
                f, b * 128 : (b + 1) * 128, :64
            ]
    both = jnp.dot(m_scr[...], w_scr[...], preferred_element_type=f32)
    nope = both[:, :LANES]
    lane = lax.broadcasted_iota(jnp.int32, (ROWS, LANES), 1)
    rope = rope_ref[...].astype(f32)
    tiles = []
    for h in range(2):
        part = nope if h == 0 else pltpu.roll(nope, 64, 1)
        tile = jnp.where(lane < QK_NOPE, part, rope)
        tiles.append(head_tile(tile, kgain_ref[...], cos_ref[...], up_ref[...], down_ref[...]))
    moved = pltpu.roll(tiles[1], QK_DIM, 1)
    values = both[:, LANES:]
    swapped = pltpu.roll(values, V_DIM, 1)
    half = ROWS // 2
    out_ref[:ROWS, :] = jnp.where(lane < QK_DIM, tiles[0], moved).astype(bf16)
    out_ref[ROWS : 2 * ROWS, :] = jnp.where(lane < V_DIM, moved, swapped).astype(bf16)
    out_ref[2 * ROWS :, :] = jnp.where(lane[:half] < V_DIM, swapped[:half], values[half:]).astype(
        bf16
    )


def queries_kernel(fs_ref, lat_ref, w0, w1, w2, w3, lgain_ref, qgain_ref, cos_ref, up_ref, down_ref, out_ref, q_scr):
    total = jnp.zeros((ROWS, 1), f32)
    for g in range(N_TP):
        piece = lat_ref[g, :, 64:].astype(f32)
        total = total + jnp.sum(piece * piece, axis=-1, keepdims=True)
    scale = lax.rsqrt(total * (1.0 / Q_LAT) + epsilon)
    for g in range(N_TP):
        piece = lat_ref[g, :, 64:].astype(f32)
        cols = slice(g * 96, (g + 1) * 96)
        inner = slice((g % 2) * 96, (g % 2 + 1) * 96)
        q_scr[g // 2, :, inner] = (piece * scale * lgain_ref[:, cols]).astype(bf16)
    both = jnp.zeros((ROWS, 2 * LANES), f32)
    for s, w in enumerate((w0, w1, w2, w3)):
        f = lax.rem(fs_ref[0] + (N_FS - s), N_FS)
        part = q_scr[f]
        both = both + jnp.dot(part[:, :96], w[512:608, :256], preferred_element_type=f32)
        both = both + jnp.dot(part[:, 96:], w[512:608, 256:], preferred_element_type=f32)
    lane = lax.broadcasted_iota(jnp.int32, (ROWS, LANES), 1)
    tiles = [
        head_tile(
            both[:, h * LANES : (h + 1) * LANES],
            qgain_ref[...],
            cos_ref[...],
            up_ref[...],
            down_ref[...],
        )
        for h in range(2)
    ]
    moved = pltpu.roll(tiles[1], QK_DIM, 1)
    out_ref[:, :LANES] = tiles[0].astype(bf16)
    out_ref[:, LANES : 2 * LANES] = jnp.where(lane < QK_DIM, 0.0, moved).astype(bf16)
    out_ref[:, 2 * LANES :] = jnp.where(lane < V_DIM, moved, 0.0).astype(bf16)


def gated_kernel(fs_ref, normed_ref, w0, w1, w2, w3, out_ref):
    value = jnp.zeros((ROWS, LANES), f32)
    gate = jnp.zeros((ROWS, LANES), f32)
    for s, w in enumerate((w0, w1, w2, w3)):
        f = lax.rem(fs_ref[0] + (N_FS - s), N_FS)
        for b in range(4):
            rows = normed_ref[:, pl.ds(pl.multiple_of(f * 512, 512) + b * LANES, LANES)]
            cols = slice(b * LANES, (b + 1) * LANES)
            value = value + jnp.dot(rows, w[256:384, cols], preferred_element_type=f32)
            gate = gate + jnp.dot(rows, w[384:512, cols], preferred_element_type=f32)
    out_ref[...] = (value * jax.nn.sigmoid(gate)).astype(bf16)


def conv_kernel_body(halo_ref, gated_ref, taps_ref, sum_ref, stat_ref, ext_scr):
    ext_scr[:HALO, :] = halo_ref[...].astype(f32)
    ext_scr[HALO:, :] = gated_ref[...].astype(f32)
    start = HALO - (TAPS - 1)
    block = LANES
    stat_ref[4:, :] = jnp.zeros((4, LANES), f32)
    for n in range(ROWS // block):
        r = n * block
        running = jnp.zeros((block, LANES), f32)
        for j in range(TAPS):
            running = running + ext_scr[pl.ds(r + start + j, block), :] * taps_ref[j : j + 1, :]
        sum_ref[r : r + block, :] = running
        flat = running.T
        total = jnp.sum(flat, axis=0, keepdims=True)
        off = flat - total * (1.0 / LANES)
        stat_ref[n : n + 1, :] = total
        stat_ref[2 + n : 3 + n, :] = jnp.sum(off * off, axis=0, keepdims=True)


def channel_kernel(sum_ref, stat_ref, gain_ref, shift_ref, out_ref):
    for n in range(ROWS // LANES):
        total = stat_ref[0, n : n + 1, :]
        for g in range(1, N_TP):
            total = total + stat_ref[g, n : n + 1, :]
        mean = total * (1.0 / CONV_W)
        spread = jnp.zeros((1, LANES), f32)
        for g in range(N_TP):
            apart = stat_ref[g, n : n + 1, :] * (1.0 / LANES) - mean
            spread = spread + stat_ref[g, 2 + n : 3 + n, :] + LANES * apart * apart
        scale = lax.rsqrt(spread * (1.0 / CONV_W) + epsilon)
        mean = jnp.broadcast_to(mean, (LANES, LANES)).T
        scale = jnp.broadcast_to(scale, (LANES, LANES)).T
        rows = slice(n * LANES, (n + 1) * LANES)
        value = (sum_ref[rows, :] - mean) * scale * gain_ref[...] + shift_ref[...]
        out_ref[rows, :] = (value / (1.0 + jnp.exp(-value))).astype(bf16)


def attend(q_ref, blocks, stat, acc, mask=None):
    rate = QK_DIM ** (-0.5) * log2_e
    firsts = [b[:ROWS, :] for b in blocks]
    seconds = [b[ROWS : 2 * ROWS, :] for b in blocks]
    thirds = [b[2 * ROWS :, :] for b in blocks]
    turned = (((1,), (1,)), ((), ()))
    keys_a = jnp.concatenate(firsts, axis=0)
    keys_b = jnp.concatenate(seconds, axis=0)
    score_a = lax.dot_general(q_ref[:, :LANES], keys_a, turned, preferred_element_type=f32)
    score_b = lax.dot_general(
        q_ref[:, LANES:],
        jnp.concatenate([keys_a, keys_b], axis=1),
        turned,
        preferred_element_type=f32,
    )
    for h, scores in enumerate((score_a, score_b)):
        scores = scores * rate
        if mask is not None:
            scores = jnp.where(mask, scores, masked_score)
        top = stat[2 * h]
        new_top = jnp.maximum(top, jnp.max(scores, axis=-1, keepdims=True))
        weights = jnp.exp2(scores - new_top)
        factor = jnp.exp2(top - new_top)
        stat[2 * h] = new_top
        stat[2 * h + 1] = stat[2 * h + 1] * factor + jnp.sum(weights, axis=-1, keepdims=True)
        weights = weights.astype(bf16)
        if h == 0:
            acc[0] = acc[0] * factor + jnp.dot(weights, keys_b, preferred_element_type=f32)
        else:
            left = acc[1] * factor
            right = acc[2] * factor
            for n, third in enumerate(thirds):
                at = n * ROWS
                half = ROWS // 2
                left = left + jnp.dot(
                    weights[:, at : at + half], third, preferred_element_type=f32
                )
                right = right + jnp.dot(
                    weights[:, at + half : at + ROWS], third, preferred_element_type=f32
                )
            acc[1] = left
            acc[2] = right


def attend_pair(at, step, q_ref, up, down, stat, acc):
    if down is None:
        pl.when(at >= step)(lambda: attend(q_ref, [up], stat, acc))
        return
    both = at >= N_SP - step
    pl.when(both)(lambda: attend(q_ref, [up, down], stat, acc))
    pl.when(jnp.logical_and(at >= step, jnp.logical_not(both)))(
        lambda: attend(q_ref, [up], stat, acc)
    )


def early_kernel(at_ref, q_ref, own_ref, *rest):
    pairs, (stat_ref, acc_ref) = rest[:-2], rest[-2:]
    at = at_ref[0]
    for h in range(2):
        stat_ref[2 * h] = jnp.full((ROWS, 1), masked_score, f32)
        stat_ref[2 * h + 1] = jnp.zeros((ROWS, 1), f32)
    acc_ref[...] = jnp.zeros(acc_ref.shape, f32)
    row = lax.broadcasted_iota(jnp.int32, (ROWS, ROWS), 0)
    col = lax.broadcasted_iota(jnp.int32, (ROWS, ROWS), 1)
    mask = jnp.right_shift(col, 6) <= jnp.right_shift(row, 6)
    attend(q_ref, [own_ref], stat_ref, acc_ref, mask)
    for n in range(0, len(pairs), 2):
        attend_pair(at, n // 2 + 1, q_ref, pairs[n], pairs[n + 1], stat_ref, acc_ref)


def late_kernel(at_ref, fs_ref, q_ref, stat_in, acc_in, conv_ref, w0, w1, w2, w3, *rest):
    blocks, (out_ref, stat, acc) = rest[:-3], rest[-3:]
    at = at_ref[0]
    stat[...] = stat_in[...]
    acc[...] = acc_in[...]
    first = N_SP // 2 - len(blocks) // 2
    for n in range(0, len(blocks), 2):
        down = blocks[n + 1] if n + 1 < len(blocks) else None
        attend_pair(at, first + n // 2, q_ref, blocks[n], down, stat, acc)
    lane = lax.broadcasted_iota(jnp.int32, (ROWS, LANES), 1)
    result = jnp.where(
        lane < V_DIM,
        pltpu.roll(acc[0], V_DIM, 1) / stat[1],
        (pltpu.roll(acc[1], V_DIM, 1) + acc[2]) / stat[3],
    ).astype(bf16)
    conv = conv_ref[...]
    share = ROWS // N_TP
    for s, w in enumerate((w0, w1, w2, w3)):
        f = lax.rem(fs_ref[0] + (N_FS - s), N_FS)
        part = (
            jnp.dot(result, w[:128, :], preferred_element_type=f32)
            + jnp.dot(conv, w[128:256, :], preferred_element_type=f32)
        ).astype(bf16)
        for r in range(N_TP):
            out_ref[r, f] = part[r * share : (r + 1) * share]


def total_kernel(in_ref, out_ref):
    for f in range(N_FS):
        total = in_ref[0, f].astype(f32)
        for g in range(1, N_TP):
            total = total + in_ref[g, f].astype(f32)
        out_ref[:, f * 512 : (f + 1) * 512] = total.astype(bf16)


def assemble_kernel(core_ref, mine_ref, other_ref, out_ref):
    share = ROWS // N_TP

    def place(first, second):
        for x in range(N_TP // 2):
            out_ref[2 * x * share : (2 * x + 1) * share, :] = first[x]
            out_ref[(2 * x + 1) * share : (2 * x + 2) * share, :] = second[x]

    pl.when(core_ref[0] == 0)(lambda: place(mine_ref, other_ref))
    pl.when(core_ref[0] == 1)(lambda: place(other_ref, mine_ref))


def rotation_tables(positions):
    inverse_freq = 1.0 / rope_base ** (jnp.arange(0, QK_ROPE, 2, dtype=f32) / QK_ROPE)
    angles = positions.astype(f32)[:, None] * inverse_freq[None, :]
    cosine, sine = jnp.cos(angles), jnp.sin(angles)
    rows = positions.shape[0]
    ones = jnp.ones((rows, QK_NOPE), f32)
    zeros = jnp.zeros((rows, QK_NOPE), f32)
    pad = jnp.zeros((rows, LANES - QK_DIM), f32)
    none = jnp.zeros_like(sine)
    return (
        jnp.concatenate([ones, cosine, cosine, pad], axis=1),
        jnp.concatenate([zeros, -sine, none, pad], axis=1),
        jnp.concatenate([zeros, none, sine, pad], axis=1),
    )


def local(
    tokens,
    mix_gain,
    query_down,
    memory_down,
    rope_weight,
    query_up,
    key_up,
    value_up,
    latent_gain,
    memory_gain,
    query_gain,
    key_gain,
    conv_value,
    conv_gate,
    conv_kernel,
    channel_gain,
    channel_shift,
    heads_out,
    conv_out,
):
    at = lax.axis_index("sp")
    fs = lax.axis_index("fs")
    up = jnp.concatenate(
        [key_up[:, :64], key_up[:, 64:], value_up[:, :64], value_up[:, 64:]], axis=0
    )
    narrow = jnp.concatenate([up, memory_down, query_down], axis=1)
    normed = norm_rows(tokens[0].astype(f32), mix_gain).astype(bf16)
    rope_pad = jnp.pad(rope_weight, ((0, 0), (QK_NOPE, LANES - QK_DIM)))
    rope_rows = jnp.dot(normed, rope_pad, preferred_element_type=f32).astype(bf16)
    narrow_all = lax.all_gather(narrow, "fs")
    projected = jnp.dot(
        normed, narrow_all.reshape(2048, 224), preferred_element_type=f32
    ).astype(bf16)
    latents = lax.all_gather(projected[:, 64:], "tp")
    positions = at * ROWS + jnp.arange(ROWS, dtype=jnp.int32)
    cosine, sine_up, sine_down = rotation_tables(positions)

    def row(vector, width):
        return jnp.pad(vector, (0, width - vector.shape[0]))[None, :]

    def beside(matrix):
        return jnp.concatenate([matrix[b * 128 : (b + 1) * 128] for b in range(4)], axis=1)

    query_pad = jnp.pad(query_up.reshape(192, 2, QK_DIM), ((0, 0), (0, 0), (0, 32))).reshape(192, 256)
    package = jnp.concatenate(
        [
            heads_out,
            conv_out,
            beside(conv_value),
            beside(conv_gate),
            jnp.concatenate([query_pad[:96], query_pad[96:]], axis=1),
        ],
        axis=0,
    )
    own = call(
        keys_values_kernel,
        jax.ShapeDtypeStruct((5 * LANES, LANES), bf16),
        [pltpu.VMEM((ROWS, KV_LAT), bf16), pltpu.VMEM((KV_LAT, 256), bf16)],
    )(
        latents, rope_rows, narrow_all, memory_gain[None, :], row(key_gain, LANES),
        cosine, sine_up, sine_down,
    )

    def along(value, axis, by):
        count = lax.axis_size(axis)
        return lax.ppermute(value, axis, [(i, (i + by) % count) for i in range(count)])

    at, fs, core = at[None], fs[None], jnp.bitwise_and(lax.axis_index("tp"), 1)[None]
    own, package, normed, at, fs, core = lax.optimization_barrier(
        (own, package, normed, at, fs, core)
    )
    ups, downs = [own], [own]
    for step in range(1, 9):
        ups.append(along(ups[-1], "sp", 1))
        if step < 8:
            downs.append(along(downs[-1], "sp", -1))
        if step == 1:
            weights = [package] + [along(package, "fs", s) for s in (1, 2, 3)]
        if step == 5:
            ups[-1], downs[-1], *weights = lax.optimization_barrier((ups[-1], downs[-1], *weights))
            gated = call(
                gated_kernel, jax.ShapeDtypeStruct((ROWS, LANES), bf16), scalars=1, arrays=5
            )(fs, normed, *weights)
            halo = lax.ppermute(gated[ROWS - HALO :], "sp", [(i, i + 1) for i in range(N_SP - 1)])
            queries = call(
                queries_kernel,
                jax.ShapeDtypeStruct((ROWS, 3 * LANES), bf16),
                [pltpu.VMEM((N_FS, ROWS, 192), bf16)],
                scalars=1,
                arrays=10,
            )(
                fs, latents, *weights, latent_gain[None, :], row(query_gain, LANES),
                cosine, sine_up, sine_down,
            )
        if step == 6:
            ups[-1], downs[-1], halo = lax.optimization_barrier((ups[-1], downs[-1], halo))
            taps = jnp.pad(conv_kernel.astype(f32), ((0, 1), (0, 0)))
            conv_sum, stats = call(
                conv_kernel_body,
                (
                    jax.ShapeDtypeStruct((ROWS, LANES), f32),
                    jax.ShapeDtypeStruct((8, LANES), f32),
                ),
                [pltpu.VMEM((ROWS + HALO, LANES), f32)],
            )(halo, gated, taps)
            stats = lax.all_gather(stats, "tp")
        if step == 7:
            ups[-1], downs[-1], stats, queries = lax.optimization_barrier(
                (ups[-1], downs[-1], stats, queries)
            )
    conv_result = call(channel_kernel, jax.ShapeDtypeStruct((ROWS, LANES), bf16))(
        conv_sum, stats, channel_gain[None, :], channel_shift[None, :]
    )
    pairs = [b for step in range(1, 8) for b in (ups[step], downs[step])] + [ups[8]]
    split = 10
    stat, acc = call(
        early_kernel,
        (
            jax.ShapeDtypeStruct((4, ROWS, 1), f32),
            jax.ShapeDtypeStruct((3, ROWS, LANES), f32),
        ),
        scalars=1,
        arrays=2 + split,
    )(at, queries, own, *pairs[:split])
    late = pairs[split:]
    partial = call(
        late_kernel,
        jax.ShapeDtypeStruct((N_TP, N_FS, ROWS // N_TP, 512), bf16),
        [pltpu.VMEM((4, ROWS, 1), f32), pltpu.VMEM((3, ROWS, LANES), f32)],
        scalars=2,
        arrays=8 + len(late),
    )(at, fs, queries, stat, acc, conv_result, *weights, *late)
    share = lax.all_to_all(partial, "tp", split_axis=0, concat_axis=0, tiled=True)
    share = call(total_kernel, jax.ShapeDtypeStruct((ROWS // N_TP, 2048), bf16))(share)
    mine = lax.all_gather(share, "tp", axis_index_groups=SAME_CORE)
    other = lax.ppermute(mine, "tp", CORE_PAIRS)
    mixed = call(
        assemble_kernel, jax.ShapeDtypeStruct((ROWS, 2048), bf16), scalars=1, arrays=2
    )(core, mine, other)
    return mixed[None]


def solution(mesh):
    in_specs = (
        P("fs", "sp", None),
        P(),
        P("fs", "tp"),
        P("fs", "tp"),
        P(),
        P("fs", "tp"),
        P("fs", "tp"),
        P("fs", "tp"),
        P(),
        P(),
        P(),
        P(),
        P("fs", "tp"),
        P("fs", "tp"),
        P(None, "tp"),
        P("tp"),
        P("tp"),
        P("tp", "fs"),
        P("tp", "fs"),
    )
    out_specs = P("fs", "sp", None)
    return jax.shard_map(local, mesh=mesh, in_specs=in_specs, out_specs=out_specs, check_vma=False)
```

```python
import jax
import jax.numpy as jnp
from jax import lax
from jax.experimental import pallas as pl
from jax.experimental.pallas import tpu as pltpu
from jax.sharding import PartitionSpec as P

QK_NOPE = 64
QK_ROPE = 32
V_DIM = 64
CONV_W = 1024
SEG = 64
QK_DIM = 96
Q_LAT = 768
KV_LAT = 512
ROWS = 256
TAPS = 31
HALO = 32
LANES = 128
N_FS = 4
N_TP = 8
N_SP = 16
BUNDLE = 2

epsilon = 1e-06
rope_base = 10000.0
masked_score = -1e30
log2_e = 1.4426950408889634
bf16 = jnp.bfloat16
f32 = jnp.float32

SAME_CORE = [[0, 2, 4, 6], [1, 3, 5, 7]]
CORE_PAIRS = [(i, i ^ 1) for i in range(N_TP)]


def call(kernel, out_shape, scratch=(), scalars=0, arrays=0, specs=None):
    extra = {}
    if scalars:
        smem = pl.BlockSpec(memory_space=pltpu.SMEM)
        specs = [smem] * scalars + [pl.BlockSpec(memory_space=pltpu.VMEM)] * arrays
    if specs:
        extra["in_specs"] = specs
    return pl.pallas_call(
        kernel,
        out_shape=out_shape,
        scratch_shapes=list(scratch),
        compiler_params=pltpu.CompilerParams(vmem_limit_bytes=16 * 1024 * 1024),
        **extra,
    )


def head_tile(tile, gain, cosine, sine_up, sine_down):
    scale = lax.rsqrt(jnp.sum(tile * tile, axis=-1, keepdims=True) * (1.0 / QK_DIM) + epsilon)
    tile = tile * scale * gain
    half = QK_ROPE // 2
    return (
        tile * cosine
        + pltpu.roll(tile, LANES - half, 1) * sine_up
        + pltpu.roll(tile, half, 1) * sine_down
    )


def pack_kernel(qd_ref, md_ref, qu_ref, ku_ref, vu_ref, cv_ref, cg_ref, narrow_ref, wide_ref, qu_scr, sems):
    pairs = [
        (qd_ref, narrow_ref.at[:96, :]),
        (md_ref, narrow_ref.at[96:160, :]),
        (qu_ref, qu_scr),
        (cv_ref, wide_ref.at[:512, :LANES]),
        (cg_ref, wide_ref.at[:512, LANES:]),
    ]
    for n, ref in enumerate((ku_ref, vu_ref)):
        for b in range(2):
            at = (2 * n + b) * LANES
            pairs.append((ref.at[b * 64 : (b + 1) * 64, :], narrow_ref.at[160:, at : at + LANES]))
    copies = [
        pltpu.make_async_copy(source, target, sems.at[n]) for n, (source, target) in enumerate(pairs)
    ]
    for copy in copies:
        copy.start()
    for copy in copies:
        copy.wait()
    wide_ref[512:, :] = jnp.zeros((192, 256), bf16)
    wide_ref[512:, :QK_DIM] = qu_scr[:, :QK_DIM]
    wide_ref[512:, LANES : LANES + QK_DIM] = qu_scr[:, QK_DIM:]


def project_kernel(tok_ref, gain_ref, rope_w_ref, cos_ref, sin_ref, w_ref, lat_ref, rope_ref, normed_ref, cosine_ref, up_ref, down_ref):
    block = 64
    turned = (((1,), (1,)), ((), ()))
    for r in range(0, ROWS, block):
        rows = tok_ref[r : r + block, :].astype(f32)
        scale = lax.rsqrt(jnp.mean(rows * rows, axis=-1, keepdims=True) + epsilon)
        normed_ref[r : r + block, :] = (rows * scale * gain_ref[...]).astype(bf16)
    both = jnp.zeros((ROWS, 160), f32)
    for f in range(N_FS):
        both = both + lax.dot_general(
            normed_ref[:, f * 512 : (f + 1) * 512],
            w_ref[f, :160, :],
            turned,
            preferred_element_type=f32,
        )
    both = both.astype(bf16)
    lat_ref[:ROWS, :] = both[:, :LANES]
    for r in range(4):
        lat_ref[ROWS:, r * 32 : (r + 1) * 32] = both[r * 64 : (r + 1) * 64, LANES:]
    rope = lax.dot_general(normed_ref[...], rope_w_ref[...], turned, preferred_element_type=f32)
    rope_ref[...] = jnp.zeros((ROWS, LANES), bf16)
    rope_ref[:, QK_NOPE:QK_DIM] = rope.astype(bf16)
    half = QK_ROPE // 2
    empty = jnp.zeros((ROWS, LANES - half), f32)
    cosine = jnp.concatenate([cos_ref[...].T, empty], axis=1)
    sine = jnp.concatenate([sin_ref[...].T, empty], axis=1)
    lane = lax.broadcasted_iota(jnp.int32, (ROWS, LANES), 1)
    cosine = pltpu.roll(cosine, QK_NOPE, 1) + pltpu.roll(cosine, QK_NOPE + half, 1)
    cosine_ref[...] = jnp.where(lane < QK_NOPE, 1.0, cosine)
    up_ref[...] = -pltpu.roll(sine, QK_NOPE, 1)
    down_ref[...] = pltpu.roll(sine, QK_NOPE + half, 1)


def keys_values_kernel(lat_ref, rope_ref, w_ref, mgain_ref, kgain_ref, cos_ref, up_ref, down_ref, out_ref, m_scr, w_scr):
    for g in range(N_TP):
        at = g * 64
        m_scr[:, at : at + 32] = lat_ref[g, :ROWS, 96:]
        for r in range(4):
            m_scr[r * 64 : (r + 1) * 64, at + 32 : at + 64] = lat_ref[
                g, ROWS:, r * 32 : (r + 1) * 32
            ]
    raw = m_scr[...].astype(f32)
    scale = lax.rsqrt(jnp.mean(raw * raw, axis=-1, keepdims=True) + epsilon)
    m_scr[...] = (raw * scale * mgain_ref[...]).astype(bf16)
    for f in range(N_FS):
        for n in range(2):
            for b in range(2):
                lanes = (2 * n + b) * LANES
                row = f * 128 + b * 64
                w_scr[row : row + 64, n * LANES : (n + 1) * LANES] = w_ref[
                    f, 160:, lanes : lanes + LANES
                ]
    both = jnp.dot(m_scr[...], w_scr[...], preferred_element_type=f32)
    nope = both[:, :LANES]
    lane = lax.broadcasted_iota(jnp.int32, (ROWS, LANES), 1)
    rope = rope_ref[...].astype(f32)
    tiles = []
    for h in range(2):
        part = nope if h == 0 else pltpu.roll(nope, 64, 1)
        tile = jnp.where(lane < QK_NOPE, part, rope)
        tiles.append(head_tile(tile, kgain_ref[...], cos_ref[...], up_ref[...], down_ref[...]))
    moved = pltpu.roll(tiles[1], QK_DIM, 1)
    values = both[:, LANES:]
    swapped = pltpu.roll(values, V_DIM, 1)
    half = ROWS // 2
    out_ref[:ROWS, :] = jnp.where(lane < QK_DIM, tiles[0], moved).astype(bf16)
    out_ref[ROWS : 2 * ROWS, :] = jnp.where(lane < V_DIM, moved, swapped).astype(bf16)
    out_ref[2 * ROWS :, :] = jnp.where(lane[:half] < V_DIM, swapped[:half], values[half:]).astype(
        bf16
    )


def queries_kernel(lat_ref, w_ref, lgain_ref, qgain_ref, cos_ref, up_ref, down_ref, out_ref, q_scr):
    for g in range(N_TP):
        q_scr[:, g * 96 : (g + 1) * 96] = lat_ref[g, :ROWS, :96]
    raw = q_scr[...].astype(f32)
    scale = lax.rsqrt(jnp.mean(raw * raw, axis=-1, keepdims=True) + epsilon)
    q_scr[...] = (raw * scale * lgain_ref[...]).astype(bf16)
    both = jnp.zeros((ROWS, 2 * LANES), f32)
    for f in range(N_FS):
        both = both + jnp.dot(
            q_scr[:, f * 192 : (f + 1) * 192], w_ref[f, 512:704, :], preferred_element_type=f32
        )
    lane = lax.broadcasted_iota(jnp.int32, (ROWS, LANES), 1)
    tiles = [
        head_tile(
            both[:, h * LANES : (h + 1) * LANES],
            qgain_ref[...],
            cos_ref[...],
            up_ref[...],
            down_ref[...],
        )
        for h in range(2)
    ]
    moved = pltpu.roll(tiles[1], QK_DIM, 1)
    out_ref[:, :LANES] = tiles[0].astype(bf16)
    out_ref[:, LANES : 2 * LANES] = jnp.where(lane < QK_DIM, 0.0, moved).astype(bf16)
    out_ref[:, 2 * LANES :] = jnp.where(lane < V_DIM, moved, 0.0).astype(bf16)


def gated_kernel(normed_ref, w_ref, out_ref):
    both = jnp.zeros((ROWS, 2 * LANES), f32)
    for f in range(N_FS):
        both = both + jnp.dot(
            normed_ref[:, f * 512 : (f + 1) * 512], w_ref[f, :512, :], preferred_element_type=f32
        )
    out_ref[...] = (both[:, :LANES] * jax.nn.sigmoid(both[:, LANES:])).astype(bf16)


def conv_kernel_body(halo_ref, gated_ref, taps_ref, sum_ref, stat_ref, ext_scr):
    ext_scr[:HALO, :] = halo_ref[...].astype(f32)
    ext_scr[HALO:, :] = gated_ref[...].astype(f32)
    start = HALO - (TAPS - 1)
    block = LANES
    stat_ref[4:, :] = jnp.zeros((4, LANES), f32)
    for n in range(ROWS // block):
        r = n * block
        running = jnp.zeros((block, LANES), f32)
        for j in range(TAPS):
            running = running + ext_scr[pl.ds(r + start + j, block), :] * taps_ref[j : j + 1, :]
        sum_ref[r : r + block, :] = running
        flat = running.T
        total = jnp.sum(flat, axis=0, keepdims=True)
        off = flat - total * (1.0 / LANES)
        stat_ref[n : n + 1, :] = total
        stat_ref[2 + n : 3 + n, :] = jnp.sum(off * off, axis=0, keepdims=True)


def channel_kernel(sum_ref, stat_ref, gain_ref, shift_ref, out_ref):
    for n in range(ROWS // LANES):
        total = stat_ref[0, n : n + 1, :]
        for g in range(1, N_TP):
            total = total + stat_ref[g, n : n + 1, :]
        mean = total * (1.0 / CONV_W)
        spread = jnp.zeros((1, LANES), f32)
        for g in range(N_TP):
            apart = stat_ref[g, n : n + 1, :] * (1.0 / LANES) - mean
            spread = spread + stat_ref[g, 2 + n : 3 + n, :] + LANES * apart * apart
        scale = lax.rsqrt(spread * (1.0 / CONV_W) + epsilon)
        mean = jnp.broadcast_to(mean, (LANES, LANES)).T
        scale = jnp.broadcast_to(scale, (LANES, LANES)).T
        rows = slice(n * LANES, (n + 1) * LANES)
        value = (sum_ref[rows, :] - mean) * scale * gain_ref[...] + shift_ref[...]
        out_ref[rows, :] = (value / (1.0 + jnp.exp(-value))).astype(bf16)


def attend(q_ref, blocks, stat, acc, mask=None):
    rate = QK_DIM ** (-0.5) * log2_e
    firsts = [b[:ROWS, :] for b in blocks]
    seconds = [b[ROWS : 2 * ROWS, :] for b in blocks]
    thirds = [b[2 * ROWS :, :] for b in blocks]
    turned = (((1,), (1,)), ((), ()))
    keys_a = jnp.concatenate(firsts, axis=0)
    keys_b = jnp.concatenate(seconds, axis=0)
    score_a = lax.dot_general(q_ref[:, :LANES], keys_a, turned, preferred_element_type=f32)
    score_b = lax.dot_general(
        q_ref[:, LANES:],
        jnp.concatenate([keys_a, keys_b], axis=1),
        turned,
        preferred_element_type=f32,
    )
    for h, scores in enumerate((score_a, score_b)):
        scores = scores * rate
        if mask is not None:
            scores = jnp.where(mask, scores, masked_score)
        top = stat[2 * h]
        new_top = jnp.maximum(top, jnp.max(scores, axis=-1, keepdims=True))
        weights = jnp.exp2(scores - new_top)
        factor = jnp.exp2(top - new_top)
        stat[2 * h] = new_top
        stat[2 * h + 1] = stat[2 * h + 1] * factor + jnp.sum(weights, axis=-1, keepdims=True)
        weights = weights.astype(bf16)
        if h == 0:
            acc[0] = acc[0] * factor + jnp.dot(weights, keys_b, preferred_element_type=f32)
        else:
            left = acc[1] * factor
            right = acc[2] * factor
            for n, third in enumerate(thirds):
                at = n * ROWS
                half = ROWS // 2
                left = left + jnp.dot(
                    weights[:, at : at + half], third, preferred_element_type=f32
                )
                right = right + jnp.dot(
                    weights[:, at + half : at + ROWS], third, preferred_element_type=f32
                )
            acc[1] = left
            acc[2] = right


def attention_kernel(at_ref, q_ref, kv_ref, conv_ref, heads_ref, conv_w_ref, out_ref, kv, stat, acc, sems):
    at = at_ref[0]
    copies = [
        pltpu.make_async_copy(kv_ref.at[n], kv.at[n], sems.at[n]) for n in range(N_SP // BUNDLE)
    ]
    for copy in copies:
        copy.start()
    for h in range(2):
        stat[2 * h] = jnp.full((ROWS, 1), masked_score, f32)
        stat[2 * h + 1] = jnp.zeros((ROWS, 1), f32)
    acc[...] = jnp.zeros(acc.shape, f32)
    wide = BUNDLE * ROWS
    for n, copy in enumerate(copies):
        copy.wait()
        blocks = [kv.at[n, i] for i in range(BUNDLE)]

        def whole(blocks=blocks):
            attend(q_ref, blocks, stat, acc)

        def cut(blocks=blocks, n=n):
            row = lax.broadcasted_iota(jnp.int32, (ROWS, wide), 0) + at * ROWS
            col = lax.broadcasted_iota(jnp.int32, (ROWS, wide), 1) + n * wide
            mask = jnp.right_shift(col, 6) <= jnp.right_shift(row, 6)
            attend(q_ref, blocks, stat, acc, mask)

        pl.when(at >= (n + 1) * BUNDLE)(whole)
        pl.when(jnp.logical_and(at >= n * BUNDLE, at < (n + 1) * BUNDLE))(cut)
    lane = lax.broadcasted_iota(jnp.int32, (ROWS, LANES), 1)
    result = jnp.where(
        lane < V_DIM,
        pltpu.roll(acc[0], V_DIM, 1) / stat[1],
        (pltpu.roll(acc[1], V_DIM, 1) + acc[2]) / stat[3],
    ).astype(bf16)
    conv = conv_ref[...]
    share = ROWS // N_TP
    for f in range(N_FS):
        part = (
            jnp.dot(result, heads_ref[f], preferred_element_type=f32)
            + jnp.dot(conv, conv_w_ref[f], preferred_element_type=f32)
        ).astype(bf16)
        for r in range(N_TP):
            out_ref[r, :, f * 512 : (f + 1) * 512] = part[r * share : (r + 1) * share]


def total_kernel(in_ref, out_ref):
    total = in_ref[0].astype(f32)
    for g in range(1, N_TP):
        total = total + in_ref[g].astype(f32)
    out_ref[...] = total.astype(bf16)


def assemble_kernel(core_ref, mine_ref, other_ref, out_ref):
    share = ROWS // N_TP

    def place(first, second):
        for x in range(N_TP // 2):
            out_ref[2 * x * share : (2 * x + 1) * share, :] = first[x]
            out_ref[(2 * x + 1) * share : (2 * x + 2) * share, :] = second[x]

    pl.when(core_ref[0] == 0)(lambda: place(mine_ref, other_ref))
    pl.when(core_ref[0] == 1)(lambda: place(other_ref, mine_ref))


def rotation_tables(positions):
    inverse_freq = 1.0 / rope_base ** (jnp.arange(0, QK_ROPE, 2, dtype=f32) / QK_ROPE)
    angles = positions.astype(f32)[None, :] * inverse_freq[:, None]
    return jnp.cos(angles), jnp.sin(angles)


def local(
    tokens,
    mix_gain,
    query_down,
    memory_down,
    rope_weight,
    query_up,
    key_up,
    value_up,
    latent_gain,
    memory_gain,
    query_gain,
    key_gain,
    conv_value,
    conv_gate,
    conv_kernel,
    channel_gain,
    channel_shift,
    heads_out,
    conv_out,
):
    at = lax.axis_index("sp")
    hbm = pl.BlockSpec(memory_space=pltpu.HBM)
    vmem = pl.BlockSpec(memory_space=pltpu.VMEM)
    narrow, wide = call(
        pack_kernel,
        (jax.ShapeDtypeStruct((224, 512), bf16), jax.ShapeDtypeStruct((704, 256), bf16)),
        [pltpu.VMEM((192, 192), bf16), pltpu.SemaphoreType.DMA((9,))],
        specs=[hbm] * 7,
    )(
        *(
            pltpu.with_memory_space_constraint(a, pltpu.HBM)
            for a in (
                query_down.T, memory_down.T, query_up, key_up, value_up, conv_value, conv_gate
            )
        )
    )
    wide_all = lax.all_gather(wide, "fs")
    narrow_all = lax.all_gather(narrow, "fs")
    positions = at * ROWS + jnp.arange(ROWS, dtype=jnp.int32)
    cosine, sine = rotation_tables(positions)
    table = jax.ShapeDtypeStruct((ROWS, LANES), f32)
    latents, rope_rows, normed, cosine, sine_up, sine_down = call(
        project_kernel,
        (
            jax.ShapeDtypeStruct((320, LANES), bf16),
            jax.ShapeDtypeStruct((ROWS, LANES), bf16),
            jax.ShapeDtypeStruct((ROWS, 2048), bf16),
            table,
            table,
            table,
        ),
    )(tokens[0], mix_gain[None, :], rope_weight.T, cosine, sine, narrow_all)
    latents = lax.all_gather(latents, "tp")

    def row(vector, width):
        return jnp.pad(vector, (0, width - vector.shape[0]))[None, :]

    own = call(
        keys_values_kernel,
        jax.ShapeDtypeStruct((5 * LANES, LANES), bf16),
        [pltpu.VMEM((ROWS, KV_LAT), bf16), pltpu.VMEM((KV_LAT, 256), bf16)],
    )(
        latents, rope_rows, narrow_all, memory_gain[None, :], row(key_gain, LANES),
        cosine, sine_up, sine_down,
    )
    pieces = lax.all_gather(own, "sp")
    queries = call(
        queries_kernel,
        jax.ShapeDtypeStruct((ROWS, 3 * LANES), bf16),
        [pltpu.VMEM((ROWS, Q_LAT), bf16)],
    )(
        latents, wide_all, latent_gain[None, :], row(query_gain, LANES),
        cosine, sine_up, sine_down,
    )
    gated = call(gated_kernel, jax.ShapeDtypeStruct((ROWS, LANES), bf16))(normed, wide_all)
    halo = lax.ppermute(gated[ROWS - HALO :], "sp", [(i, i + 1) for i in range(N_SP - 1)])
    taps = jnp.pad(conv_kernel.astype(f32), ((0, 1), (0, 0)))
    conv_sum, stats = call(
        conv_kernel_body,
        (jax.ShapeDtypeStruct((ROWS, LANES), f32), jax.ShapeDtypeStruct((8, LANES), f32)),
        [pltpu.VMEM((ROWS + HALO, LANES), f32)],
    )(halo, gated, taps)
    stats = lax.all_gather(stats, "tp")
    conv_result = call(channel_kernel, jax.ShapeDtypeStruct((ROWS, LANES), bf16))(
        conv_sum, stats, channel_gain[None, :], channel_shift[None, :]
    )
    heads_all = lax.all_gather(heads_out, "fs")
    conv_all = lax.all_gather(conv_out, "fs")
    core = jnp.bitwise_and(lax.axis_index("tp"), 1)[None]
    pieces = pltpu.with_memory_space_constraint(
        pieces.reshape(N_SP // BUNDLE, BUNDLE, 5 * LANES, LANES), pltpu.HBM
    )
    partial = call(
        attention_kernel,
        jax.ShapeDtypeStruct((N_TP, ROWS // N_TP, 2048), bf16),
        [
            pltpu.VMEM((N_SP // BUNDLE, BUNDLE, 5 * LANES, LANES), bf16),
            pltpu.VMEM((4, ROWS, 1), f32),
            pltpu.VMEM((3, ROWS, LANES), f32),
            pltpu.SemaphoreType.DMA((N_SP // BUNDLE,)),
        ],
        specs=[
            pl.BlockSpec(memory_space=pltpu.SMEM), vmem, hbm, vmem, vmem, vmem,
        ],
    )(at[None], queries, pieces, conv_result, heads_all, conv_all)
    share = lax.all_to_all(partial, "tp", split_axis=0, concat_axis=0, tiled=True)
    share = call(total_kernel, jax.ShapeDtypeStruct((ROWS // N_TP, 2048), bf16))(share)
    mine = lax.all_gather(share, "tp", axis_index_groups=SAME_CORE)
    other = lax.ppermute(mine, "tp", CORE_PAIRS)
    mixed = call(
        assemble_kernel, jax.ShapeDtypeStruct((ROWS, 2048), bf16), scalars=1, arrays=2
    )(core, mine, other)
    return mixed[None]


def solution(mesh):
    in_specs = (
        P("fs", "sp", None),
        P(),
        P("fs", "tp"),
        P("fs", "tp"),
        P(),
        P("fs", "tp"),
        P("fs", "tp"),
        P("fs", "tp"),
        P(),
        P(),
        P(),
        P(),
        P("fs", "tp"),
        P("fs", "tp"),
        P(None, "tp"),
        P("tp"),
        P("tp"),
        P("tp", "fs"),
        P("tp", "fs"),
    )
    out_specs = P("fs", "sp", None)
    return jax.shard_map(local, mesh=mesh, in_specs=in_specs, out_specs=out_specs, check_vma=False)
```

```python
import jax
import jax.numpy as jnp
from jax import lax
from jax.experimental import pallas as pl
from jax.experimental.pallas import tpu as pltpu
from jax.sharding import PartitionSpec as P

QK_NOPE = 64
QK_ROPE = 32
V_DIM = 64
CONV_W = 1024
SEG = 64
QK_DIM = 96
Q_LAT = 768
KV_LAT = 512
ROWS = 256
TAPS = 31
HALO = 32
LANES = 128
N_FS = 4
N_TP = 8
N_SP = 16
BUNDLE = 4

epsilon = 1e-06
rope_base = 10000.0
masked_score = -1e30
log2_e = 1.4426950408889634
bf16 = jnp.bfloat16
f32 = jnp.float32

SAME_CORE = [[0, 2, 4, 6], [1, 3, 5, 7]]
CORE_PAIRS = [(i, i ^ 1) for i in range(N_TP)]


def call(kernel, out_shape, scratch=(), scalars=0, arrays=0, specs=None):
    extra = {}
    if scalars:
        smem = pl.BlockSpec(memory_space=pltpu.SMEM)
        specs = [smem] * scalars + [pl.BlockSpec(memory_space=pltpu.VMEM)] * arrays
    if specs:
        extra["in_specs"] = specs
    return pl.pallas_call(
        kernel,
        out_shape=out_shape,
        scratch_shapes=list(scratch),
        compiler_params=pltpu.CompilerParams(vmem_limit_bytes=16 * 1024 * 1024),
        **extra,
    )


def head_tile(tile, gain, cosine, sine_up, sine_down):
    scale = lax.rsqrt(jnp.sum(tile * tile, axis=-1, keepdims=True) * (1.0 / QK_DIM) + epsilon)
    tile = tile * scale * gain
    half = QK_ROPE // 2
    return (
        tile * cosine
        + pltpu.roll(tile, LANES - half, 1) * sine_up
        + pltpu.roll(tile, half, 1) * sine_down
    )


def pack_kernel(qd_ref, md_ref, qu_ref, ku_ref, vu_ref, cv_ref, cg_ref, rope_ref, gain_ref, narrow_ref, wide_ref, rope_out, gain_out, qu_scr, sems):
    pairs = [
        (qd_ref, narrow_ref.at[:96, :]),
        (md_ref, narrow_ref.at[96:160, :]),
        (qu_ref, qu_scr),
        (cv_ref, wide_ref.at[:512, :LANES]),
        (cg_ref, wide_ref.at[:512, LANES:]),
        (rope_ref, rope_out),
        (gain_ref, gain_out),
    ]
    for n, ref in enumerate((ku_ref, vu_ref)):
        for b in range(2):
            at = (2 * n + b) * LANES
            pairs.append((ref.at[b * 64 : (b + 1) * 64, :], narrow_ref.at[160:, at : at + LANES]))
    copies = [
        pltpu.make_async_copy(source, target, sems.at[n]) for n, (source, target) in enumerate(pairs)
    ]
    for copy in copies:
        copy.start()
    for copy in copies:
        copy.wait()
    wide_ref[512:, :] = jnp.zeros((192, 256), bf16)
    wide_ref[512:, :QK_DIM] = qu_scr[:, :QK_DIM]
    wide_ref[512:, LANES : LANES + QK_DIM] = qu_scr[:, QK_DIM:]


def project_kernel(tok_ref, gain_ref, rope_w_ref, cos_ref, sin_ref, w_ref, lat_ref, rope_ref, normed_ref, cosine_ref, up_ref, down_ref, tok_scr, sems):
    block = 64
    copies = []
    for n in range(ROWS // block):
        rows = slice(n * block, (n + 1) * block)
        copies.append(
            pltpu.make_async_copy(tok_ref.at[rows, :], tok_scr.at[rows, :], sems.at[n])
        )
        copies[-1].start()
    turned = (((1,), (1,)), ((), ()))
    for r in range(0, ROWS, block):
        copies[r // block].wait()
        rows = tok_scr[r : r + block, :].astype(f32)
        scale = lax.rsqrt(jnp.mean(rows * rows, axis=-1, keepdims=True) + epsilon)
        normed_ref[r : r + block, :] = (rows * scale * gain_ref[...]).astype(bf16)
    both = jnp.zeros((ROWS, 160), f32)
    for f in range(N_FS):
        both = both + lax.dot_general(
            normed_ref[:, f * 512 : (f + 1) * 512],
            w_ref[f, :160, :],
            turned,
            preferred_element_type=f32,
        )
    both = both.astype(bf16)
    lat_ref[:ROWS, :] = both[:, :LANES]
    for r in range(4):
        lat_ref[ROWS:, r * 32 : (r + 1) * 32] = both[r * 64 : (r + 1) * 64, LANES:]
    rope = lax.dot_general(normed_ref[...], rope_w_ref[...], turned, preferred_element_type=f32)
    rope_ref[...] = jnp.zeros((ROWS, LANES), bf16)
    rope_ref[:, QK_NOPE:QK_DIM] = rope.astype(bf16)
    half = QK_ROPE // 2
    empty = jnp.zeros((ROWS, LANES - half), f32)
    cosine = jnp.concatenate([cos_ref[...].T, empty], axis=1)
    sine = jnp.concatenate([sin_ref[...].T, empty], axis=1)
    lane = lax.broadcasted_iota(jnp.int32, (ROWS, LANES), 1)
    cosine = pltpu.roll(cosine, QK_NOPE, 1) + pltpu.roll(cosine, QK_NOPE + half, 1)
    cosine_ref[...] = jnp.where(lane < QK_NOPE, 1.0, cosine)
    up_ref[...] = -pltpu.roll(sine, QK_NOPE, 1)
    down_ref[...] = pltpu.roll(sine, QK_NOPE + half, 1)


def keys_values_kernel(lat_ref, rope_ref, w_ref, mgain_ref, kgain_ref, cos_ref, up_ref, down_ref, out_ref, m_scr, w_scr):
    for g in range(N_TP):
        at = g * 64
        m_scr[:, at : at + 32] = lat_ref[g, :ROWS, 96:]
        for r in range(4):
            m_scr[r * 64 : (r + 1) * 64, at + 32 : at + 64] = lat_ref[
                g, ROWS:, r * 32 : (r + 1) * 32
            ]
    raw = m_scr[...].astype(f32)
    scale = lax.rsqrt(jnp.mean(raw * raw, axis=-1, keepdims=True) + epsilon)
    m_scr[...] = (raw * scale * mgain_ref[...]).astype(bf16)
    for f in range(N_FS):
        for n in range(2):
            for b in range(2):
                lanes = (2 * n + b) * LANES
                row = f * 128 + b * 64
                w_scr[row : row + 64, n * LANES : (n + 1) * LANES] = w_ref[
                    f, 160:, lanes : lanes + LANES
                ]
    both = jnp.dot(m_scr[...], w_scr[...], preferred_element_type=f32)
    nope = both[:, :LANES]
    lane = lax.broadcasted_iota(jnp.int32, (ROWS, LANES), 1)
    rope = rope_ref[...].astype(f32)
    tiles = []
    for h in range(2):
        part = nope if h == 0 else pltpu.roll(nope, 64, 1)
        tile = jnp.where(lane < QK_NOPE, part, rope)
        tiles.append(head_tile(tile, kgain_ref[...], cos_ref[...], up_ref[...], down_ref[...]))
    for h in range(2):
        out_ref[h * ROWS : (h + 1) * ROWS, :] = tiles[h].astype(bf16)
    values = both[:, LANES:].T.astype(bf16)
    for half in range(2):
        at = 2 * ROWS + half * LANES
        out_ref[at : at + LANES, :] = values[:, half * LANES : (half + 1) * LANES]


def queries_kernel(lat_ref, w_ref, lgain_ref, qgain_ref, cos_ref, up_ref, down_ref, out_ref, q_scr):
    for g in range(N_TP):
        q_scr[:, g * 96 : (g + 1) * 96] = lat_ref[g, :ROWS, :96]
    raw = q_scr[...].astype(f32)
    scale = lax.rsqrt(jnp.mean(raw * raw, axis=-1, keepdims=True) + epsilon)
    q_scr[...] = (raw * scale * lgain_ref[...]).astype(bf16)
    both = jnp.zeros((ROWS, 2 * LANES), f32)
    for f in range(N_FS):
        both = both + jnp.dot(
            q_scr[:, f * 192 : (f + 1) * 192], w_ref[f, 512:704, :], preferred_element_type=f32
        )
    lane = lax.broadcasted_iota(jnp.int32, (ROWS, LANES), 1)
    tiles = [
        head_tile(
            both[:, h * LANES : (h + 1) * LANES],
            qgain_ref[...],
            cos_ref[...],
            up_ref[...],
            down_ref[...],
        )
        for h in range(2)
    ]
    for h in range(2):
        out_ref[:, h * LANES : (h + 1) * LANES] = tiles[h].astype(bf16)


def gated_kernel(normed_ref, w_ref, out_ref):
    both = jnp.zeros((ROWS, 2 * LANES), f32)
    for f in range(N_FS):
        both = both + jnp.dot(
            normed_ref[:, f * 512 : (f + 1) * 512], w_ref[f, :512, :], preferred_element_type=f32
        )
    out_ref[...] = (both[:, :LANES] * jax.nn.sigmoid(both[:, LANES:])).astype(bf16)


def conv_kernel_body(halo_ref, gated_ref, taps_ref, sum_ref, stat_ref, ext_scr):
    ext_scr[:HALO, :] = halo_ref[...].astype(f32)
    ext_scr[HALO:, :] = gated_ref[...].astype(f32)
    start = HALO - (TAPS - 1)
    block = LANES
    stat_ref[4:, :] = jnp.zeros((4, LANES), f32)
    for n in range(ROWS // block):
        r = n * block
        running = jnp.zeros((block, LANES), f32)
        for j in range(TAPS):
            running = running + ext_scr[pl.ds(r + start + j, block), :] * taps_ref[j : j + 1, :]
        sum_ref[r : r + block, :] = running
        flat = running.T
        total = jnp.sum(flat, axis=0, keepdims=True)
        off = flat - total * (1.0 / LANES)
        stat_ref[n : n + 1, :] = total
        stat_ref[2 + n : 3 + n, :] = jnp.sum(off * off, axis=0, keepdims=True)


def channel_kernel(sum_ref, stat_ref, gain_ref, shift_ref, out_ref):
    for n in range(ROWS // LANES):
        total = stat_ref[0, n : n + 1, :]
        for g in range(1, N_TP):
            total = total + stat_ref[g, n : n + 1, :]
        mean = total * (1.0 / CONV_W)
        spread = jnp.zeros((1, LANES), f32)
        for g in range(N_TP):
            apart = stat_ref[g, n : n + 1, :] * (1.0 / LANES) - mean
            spread = spread + stat_ref[g, 2 + n : 3 + n, :] + LANES * apart * apart
        scale = lax.rsqrt(spread * (1.0 / CONV_W) + epsilon)
        mean = jnp.broadcast_to(mean, (LANES, LANES)).T
        scale = jnp.broadcast_to(scale, (LANES, LANES)).T
        rows = slice(n * LANES, (n + 1) * LANES)
        value = (sum_ref[rows, :] - mean) * scale * gain_ref[...] + shift_ref[...]
        out_ref[rows, :] = (value / (1.0 + jnp.exp(-value))).astype(bf16)


def attend(q_ref, blocks, state, hidden, mask=None):
    rate = QK_DIM ** (-0.5) * log2_e
    fresh = []
    for h in range(2):
        top, total, weighted = state[h]
        keys = jnp.concatenate([b[h * ROWS : (h + 1) * ROWS, :] for b in blocks], axis=0)
        scores = lax.dot_general(
            keys,
            q_ref[:, h * LANES : (h + 1) * LANES],
            (((1,), (1,)), ((), ())),
            preferred_element_type=f32,
        )
        if mask is not None:
            scores = jnp.where(mask, scores, masked_score)
        new_top = top
        for n, off in enumerate(hidden):
            part = jnp.max(scores[n * ROWS : (n + 1) * ROWS], axis=0, keepdims=True)
            new_top = jnp.maximum(new_top, part - off)
        weights = jnp.concatenate(
            [
                jnp.exp2(scores[n * ROWS : (n + 1) * ROWS] * rate - (new_top * rate + off))
                for n, off in enumerate(hidden)
            ],
            axis=0,
        )
        factor = jnp.exp2((top - new_top) * rate)
        total = total * factor + jnp.sum(weights, axis=0, keepdims=True)
        at = 2 * ROWS + h * V_DIM
        values = jnp.concatenate(
            [b[at + i * LANES : at + i * LANES + V_DIM, :] for b in blocks for i in range(2)],
            axis=1,
        )
        weighted = weighted * factor + jnp.dot(
            values, weights.astype(bf16), preferred_element_type=f32
        )
        fresh.append((new_top, total, weighted))
    return fresh


def own_kernel(q_ref, own_ref, stat_ref, acc_ref):
    key = lax.broadcasted_iota(jnp.int32, (ROWS, ROWS), 0)
    query = lax.broadcasted_iota(jnp.int32, (ROWS, ROWS), 1)
    mask = jnp.right_shift(key, 6) <= jnp.right_shift(query, 6)
    empty = (
        jnp.full((1, ROWS), masked_score, f32),
        jnp.zeros((1, ROWS), f32),
        jnp.zeros((V_DIM, ROWS), f32),
    )
    state = attend(q_ref, [own_ref], [empty, empty], [0.0], mask)
    stat_ref[4:, :] = jnp.zeros((4, ROWS), f32)
    for h in range(2):
        stat_ref[2 * h : 2 * h + 1, :] = state[h][0]
        stat_ref[2 * h + 1 : 2 * h + 2, :] = state[h][1]
        acc_ref[h * V_DIM : (h + 1) * V_DIM, :] = state[h][2]


def attention_kernel(at_ref, q_ref, kv_ref, stat_ref, acc_ref, conv_ref, heads_ref, conv_w_ref, out_ref, kv, sems):
    at = at_ref[0]
    copies = [
        pltpu.make_async_copy(kv_ref.at[n], kv.at[n], sems.at[n]) for n in range(N_SP // BUNDLE)
    ]
    for copy in copies:
        copy.start()
    state = [
        (
            stat_ref[2 * h : 2 * h + 1, :],
            stat_ref[2 * h + 1 : 2 * h + 2, :],
            acc_ref[h * V_DIM : (h + 1) * V_DIM, :],
        )
        for h in range(2)
    ]
    for n, copy in enumerate(copies):
        copy.wait()
        hidden = [jnp.where(n * BUNDLE + i < at, 0.0, -masked_score) for i in range(BUNDLE)]
        state = attend(q_ref, [kv.at[n, i] for i in range(BUNDLE)], state, hidden)
    result = jnp.concatenate([state[h][2] / state[h][1] for h in range(2)], axis=0).T.astype(bf16)
    conv = conv_ref[...]
    share = ROWS // N_TP
    for f in range(N_FS):
        part = (
            jnp.dot(result, heads_ref[f], preferred_element_type=f32)
            + jnp.dot(conv, conv_w_ref[f], preferred_element_type=f32)
        ).astype(bf16)
        for r in range(N_TP):
            out_ref[r, :, f * 512 : (f + 1) * 512] = part[r * share : (r + 1) * share]


def total_kernel(in_ref, out_ref):
    total = in_ref[0].astype(f32)
    for g in range(1, N_TP):
        total = total + in_ref[g].astype(f32)
    out_ref[...] = total.astype(bf16)


def assemble_kernel(core_ref, mine_ref, other_ref, out_ref):
    share = ROWS // N_TP

    def place(first, second):
        for x in range(N_TP // 2):
            out_ref[2 * x * share : (2 * x + 1) * share, :] = first[x]
            out_ref[(2 * x + 1) * share : (2 * x + 2) * share, :] = second[x]

    pl.when(core_ref[0] == 0)(lambda: place(mine_ref, other_ref))
    pl.when(core_ref[0] == 1)(lambda: place(other_ref, mine_ref))


def rotation_tables(positions):
    inverse_freq = 1.0 / rope_base ** (jnp.arange(0, QK_ROPE, 2, dtype=f32) / QK_ROPE)
    angles = positions.astype(f32)[None, :] * inverse_freq[:, None]
    return jnp.cos(angles), jnp.sin(angles)


def local(
    tokens,
    mix_gain,
    query_down,
    memory_down,
    rope_weight,
    query_up,
    key_up,
    value_up,
    latent_gain,
    memory_gain,
    query_gain,
    key_gain,
    conv_value,
    conv_gate,
    conv_kernel,
    channel_gain,
    channel_shift,
    heads_out,
    conv_out,
):
    at = lax.axis_index("sp")
    hbm = pl.BlockSpec(memory_space=pltpu.HBM)
    vmem = pl.BlockSpec(memory_space=pltpu.VMEM)
    narrow, wide, rope_w, gain = call(
        pack_kernel,
        (
            jax.ShapeDtypeStruct((224, 512), bf16),
            jax.ShapeDtypeStruct((704, 256), bf16),
            jax.ShapeDtypeStruct((QK_ROPE, 2048), bf16),
            jax.ShapeDtypeStruct((1, 2048), f32),
        ),
        [pltpu.VMEM((192, 192), bf16), pltpu.SemaphoreType.DMA((11,))],
        specs=[hbm] * 9,
    )(
        *(
            pltpu.with_memory_space_constraint(a, pltpu.HBM)
            for a in (
                query_down.T, memory_down.T, query_up, key_up, value_up, conv_value, conv_gate,
                rope_weight.T, mix_gain[None, :],
            )
        )
    )
    wide_all = lax.all_gather(wide, "fs")
    narrow_all = lax.all_gather(narrow, "fs")
    positions = at * ROWS + jnp.arange(ROWS, dtype=jnp.int32)
    cosine, sine = rotation_tables(positions)
    table = jax.ShapeDtypeStruct((ROWS, LANES), f32)
    latents, rope_rows, normed, cosine, sine_up, sine_down = call(
        project_kernel,
        (
            jax.ShapeDtypeStruct((320, LANES), bf16),
            jax.ShapeDtypeStruct((ROWS, LANES), bf16),
            jax.ShapeDtypeStruct((ROWS, 2048), bf16),
            table,
            table,
            table,
        ),
        [pltpu.VMEM((ROWS, 2048), bf16), pltpu.SemaphoreType.DMA((4,))],
        specs=[hbm] + [vmem] * 5,
    )(pltpu.with_memory_space_constraint(tokens[0], pltpu.HBM), gain, rope_w, cosine, sine, narrow_all)
    latents = lax.all_gather(latents, "tp")

    def row(vector, width):
        return jnp.pad(vector, (0, width - vector.shape[0]))[None, :]

    own = call(
        keys_values_kernel,
        jax.ShapeDtypeStruct((6 * LANES, LANES), bf16),
        [pltpu.VMEM((ROWS, KV_LAT), bf16), pltpu.VMEM((KV_LAT, 256), bf16)],
    )(
        latents, rope_rows, narrow_all, memory_gain[None, :], row(key_gain, LANES),
        cosine, sine_up, sine_down,
    )
    pieces = lax.all_gather(own, "sp")
    queries = call(
        queries_kernel,
        jax.ShapeDtypeStruct((ROWS, 2 * LANES), bf16),
        [pltpu.VMEM((ROWS, Q_LAT), bf16)],
    )(
        latents, wide_all, latent_gain[None, :], row(query_gain, LANES),
        cosine, sine_up, sine_down,
    )
    gated = call(gated_kernel, jax.ShapeDtypeStruct((ROWS, LANES), bf16))(normed, wide_all)
    halo = lax.ppermute(gated[ROWS - HALO :], "sp", [(i, i + 1) for i in range(N_SP - 1)])
    taps = jnp.pad(conv_kernel.astype(f32), ((0, 1), (0, 0)))
    conv_sum, stats = call(
        conv_kernel_body,
        (jax.ShapeDtypeStruct((ROWS, LANES), f32), jax.ShapeDtypeStruct((8, LANES), f32)),
        [pltpu.VMEM((ROWS + HALO, LANES), f32)],
    )(halo, gated, taps)
    stats = lax.all_gather(stats, "tp")
    conv_result = call(channel_kernel, jax.ShapeDtypeStruct((ROWS, LANES), bf16))(
        conv_sum, stats, channel_gain[None, :], channel_shift[None, :]
    )
    stat, acc = call(
        own_kernel,
        (jax.ShapeDtypeStruct((8, ROWS), f32), jax.ShapeDtypeStruct((2 * V_DIM, ROWS), f32)),
    )(queries, own)
    heads_all = lax.all_gather(heads_out, "fs")
    conv_all = lax.all_gather(conv_out, "fs")
    core = jnp.bitwise_and(lax.axis_index("tp"), 1)[None]
    pieces = pltpu.with_memory_space_constraint(
        pieces.reshape(N_SP // BUNDLE, BUNDLE, 6 * LANES, LANES), pltpu.HBM
    )
    partial = call(
        attention_kernel,
        jax.ShapeDtypeStruct((N_TP, ROWS // N_TP, 2048), bf16),
        [
            pltpu.VMEM((N_SP // BUNDLE, BUNDLE, 6 * LANES, LANES), bf16),
            pltpu.SemaphoreType.DMA((N_SP // BUNDLE,)),
        ],
        specs=[
            pl.BlockSpec(memory_space=pltpu.SMEM), vmem, hbm, vmem, vmem, vmem, vmem, vmem,
        ],
    )(at[None], queries, pieces, stat, acc, conv_result, heads_all, conv_all)
    share = lax.all_to_all(partial, "tp", split_axis=0, concat_axis=0, tiled=True)
    share = call(total_kernel, jax.ShapeDtypeStruct((ROWS // N_TP, 2048), bf16))(share)
    mine = lax.all_gather(share, "tp", axis_index_groups=SAME_CORE)
    other = lax.ppermute(mine, "tp", CORE_PAIRS)
    mixed = call(
        assemble_kernel, jax.ShapeDtypeStruct((ROWS, 2048), bf16), scalars=1, arrays=2
    )(core, mine, other)
    return mixed[None]


def solution(mesh):
    in_specs = (
        P("fs", "sp", None),
        P(),
        P("fs", "tp"),
        P("fs", "tp"),
        P(),
        P("fs", "tp"),
        P("fs", "tp"),
        P("fs", "tp"),
        P(),
        P(),
        P(),
        P(),
        P("fs", "tp"),
        P("fs", "tp"),
        P(None, "tp"),
        P("tp"),
        P("tp"),
        P("tp", "fs"),
        P("tp", "fs"),
    )
    out_specs = P("fs", "sp", None)
    return jax.shard_map(local, mesh=mesh, in_specs=in_specs, out_specs=out_specs, check_vma=False)
```

```python
import jax
import jax.numpy as jnp
from jax import lax
from jax.experimental import pallas as pl
from jax.experimental.pallas import tpu as pltpu
from jax.sharding import PartitionSpec as P

QK_NOPE = 64
QK_ROPE = 32
V_DIM = 64
CONV_W = 1024
SEG = 64
QK_DIM = 96
Q_LAT = 768
KV_LAT = 512
ROWS = 256
TAPS = 31
HALO = 32
LANES = 128
N_FS = 4
N_TP = 8
N_SP = 16
BUNDLE = 4

epsilon = 1e-06
rope_base = 10000.0
masked_score = -1e30
log2_e = 1.4426950408889634
bf16 = jnp.bfloat16
f32 = jnp.float32

SAME_CORE = [[0, 2, 4, 6], [1, 3, 5, 7]]
CORE_PAIRS = [(i, i ^ 1) for i in range(N_TP)]


def call(kernel, out_shape, scratch=(), scalars=0, arrays=0, specs=None):
    extra = {}
    if scalars:
        smem = pl.BlockSpec(memory_space=pltpu.SMEM)
        specs = [smem] * scalars + [pl.BlockSpec(memory_space=pltpu.VMEM)] * arrays
    if specs:
        extra["in_specs"] = specs
    return pl.pallas_call(
        kernel,
        out_shape=out_shape,
        scratch_shapes=list(scratch),
        compiler_params=pltpu.CompilerParams(vmem_limit_bytes=16 * 1024 * 1024),
        **extra,
    )


def head_tile(tile, gain, cosine, sine_up, sine_down):
    scale = lax.rsqrt(jnp.sum(tile * tile, axis=-1, keepdims=True) * (1.0 / QK_DIM) + epsilon)
    tile = tile * scale * gain
    half = QK_ROPE // 2
    return (
        tile * cosine
        + pltpu.roll(tile, LANES - half, 1) * sine_up
        + pltpu.roll(tile, half, 1) * sine_down
    )


def copy_all(pairs, sems):
    copies = [
        pltpu.make_async_copy(source, target, sems.at[n]) for n, (source, target) in enumerate(pairs)
    ]
    for copy in copies:
        copy.start()
    for copy in copies:
        copy.wait()


def pack_kernel(qd_ref, md_ref, ku_ref, vu_ref, rope_ref, gain_ref, narrow_ref, rope_out, gain_out, sems):
    pairs = [
        (qd_ref, narrow_ref.at[:96, :]),
        (md_ref, narrow_ref.at[96:160, :]),
        (rope_ref, rope_out),
        (gain_ref, gain_out),
    ]
    for n, ref in enumerate((ku_ref, vu_ref)):
        for b in range(2):
            at = (2 * n + b) * LANES
            pairs.append((ref.at[b * 64 : (b + 1) * 64, :], narrow_ref.at[160:, at : at + LANES]))
    copy_all(pairs, sems)


def pack_rest_kernel(qu_ref, cv_ref, cg_ref, ho_ref, co_ref, first_ref, second_ref, third_ref, qu_scr, sems):
    pairs = [
        (qu_ref, qu_scr),
        (ho_ref.at[:64, :], second_ref.at[128:, :]),
        (ho_ref.at[64:, :], third_ref.at[:64, :]),
        (co_ref, third_ref.at[64:, :]),
    ]
    for ref, out in ((cv_ref, first_ref), (cg_ref, second_ref)):
        for b in range(4):
            rows = slice(b * 128, (b + 1) * 128)
            pairs.append((ref.at[rows, :], out.at[:128, rows]))
    copy_all(pairs, sems)
    first_ref[128:, :] = jnp.zeros((96, 512), bf16)
    for half in range(2):
        for h in range(2):
            at = half * 256 + h * LANES
            first_ref[128:, at : at + QK_DIM] = qu_scr[
                half * 96 : (half + 1) * 96, h * QK_DIM : (h + 1) * QK_DIM
            ]


def project_kernel(tok_ref, gain_ref, rope_w_ref, cos_ref, sin_ref, w_ref, lat_ref, rope_ref, normed_ref, cosine_ref, up_ref, down_ref, tok_scr, sems):
    block = 64
    copies = []
    for n in range(ROWS // block):
        rows = slice(n * block, (n + 1) * block)
        copies.append(
            pltpu.make_async_copy(tok_ref.at[rows, :], tok_scr.at[rows, :], sems.at[n])
        )
        copies[-1].start()
    turned = (((1,), (1,)), ((), ()))
    for r in range(0, ROWS, block):
        copies[r // block].wait()
        rows = tok_scr[r : r + block, :].astype(f32)
        scale = lax.rsqrt(jnp.mean(rows * rows, axis=-1, keepdims=True) + epsilon)
        normed_ref[r : r + block, :] = (rows * scale * gain_ref[...]).astype(bf16)
    both = jnp.zeros((ROWS, 160), f32)
    for f in range(N_FS):
        both = both + lax.dot_general(
            normed_ref[:, f * 512 : (f + 1) * 512],
            w_ref[f, :160, :],
            turned,
            preferred_element_type=f32,
        )
    both = both.astype(bf16)
    lat_ref[:ROWS, :] = both[:, :LANES]
    for r in range(4):
        lat_ref[ROWS:, r * 32 : (r + 1) * 32] = both[r * 64 : (r + 1) * 64, LANES:]
    rope = lax.dot_general(normed_ref[...], rope_w_ref[...], turned, preferred_element_type=f32)
    rope_ref[...] = jnp.zeros((ROWS, LANES), bf16)
    rope_ref[:, QK_NOPE:QK_DIM] = rope.astype(bf16)
    half = QK_ROPE // 2
    empty = jnp.zeros((ROWS, LANES - half), f32)
    cosine = jnp.concatenate([cos_ref[...].T, empty], axis=1)
    sine = jnp.concatenate([sin_ref[...].T, empty], axis=1)
    lane = lax.broadcasted_iota(jnp.int32, (ROWS, LANES), 1)
    cosine = pltpu.roll(cosine, QK_NOPE, 1) + pltpu.roll(cosine, QK_NOPE + half, 1)
    cosine_ref[...] = jnp.where(lane < QK_NOPE, 1.0, cosine)
    up_ref[...] = -pltpu.roll(sine, QK_NOPE, 1)
    down_ref[...] = pltpu.roll(sine, QK_NOPE + half, 1)


def keys_values_kernel(lat_ref, rope_ref, w_ref, mgain_ref, kgain_ref, cos_ref, up_ref, down_ref, out_ref, m_scr, w_scr):
    for g in range(N_TP):
        at = g * 64
        m_scr[:, at : at + 32] = lat_ref[g, :ROWS, 96:]
        for r in range(4):
            m_scr[r * 64 : (r + 1) * 64, at + 32 : at + 64] = lat_ref[
                g, ROWS:, r * 32 : (r + 1) * 32
            ]
    raw = m_scr[...].astype(f32)
    scale = lax.rsqrt(jnp.mean(raw * raw, axis=-1, keepdims=True) + epsilon)
    m_scr[...] = (raw * scale * mgain_ref[...]).astype(bf16)
    for f in range(N_FS):
        for n in range(2):
            for b in range(2):
                lanes = (2 * n + b) * LANES
                row = f * 128 + b * 64
                w_scr[row : row + 64, n * LANES : (n + 1) * LANES] = w_ref[
                    f, 160:, lanes : lanes + LANES
                ]
    both = jnp.dot(m_scr[...], w_scr[...], preferred_element_type=f32)
    nope = both[:, :LANES]
    lane = lax.broadcasted_iota(jnp.int32, (ROWS, LANES), 1)
    rope = rope_ref[...].astype(f32)
    tiles = []
    for h in range(2):
        part = nope if h == 0 else pltpu.roll(nope, 64, 1)
        tile = jnp.where(lane < QK_NOPE, part, rope)
        tiles.append(head_tile(tile, kgain_ref[...], cos_ref[...], up_ref[...], down_ref[...]))
    for h in range(2):
        out_ref[h * ROWS : (h + 1) * ROWS, :] = tiles[h].astype(bf16)
    values = both[:, LANES:].T.astype(bf16)
    for half in range(2):
        at = 2 * ROWS + half * LANES
        out_ref[at : at + LANES, :] = values[:, half * LANES : (half + 1) * LANES]


def queries_kernel(lat_ref, w_ref, lgain_ref, qgain_ref, cos_ref, up_ref, down_ref, out_ref, q_scr):
    for g in range(N_TP):
        q_scr[:, g * 96 : (g + 1) * 96] = lat_ref[g, :ROWS, :96]
    raw = q_scr[...].astype(f32)
    scale = lax.rsqrt(jnp.mean(raw * raw, axis=-1, keepdims=True) + epsilon)
    q_scr[...] = (raw * scale * lgain_ref[...]).astype(bf16)
    both = jnp.zeros((ROWS, 2 * LANES), f32)
    for f in range(N_FS):
        for half in range(2):
            at = f * 192 + half * 96
            both = both + jnp.dot(
                q_scr[:, at : at + 96],
                w_ref[f, 128:, half * 256 : (half + 1) * 256],
                preferred_element_type=f32,
            )
    lane = lax.broadcasted_iota(jnp.int32, (ROWS, LANES), 1)
    tiles = [
        head_tile(
            both[:, h * LANES : (h + 1) * LANES],
            qgain_ref[...],
            cos_ref[...],
            up_ref[...],
            down_ref[...],
        )
        for h in range(2)
    ]
    for h in range(2):
        out_ref[:, h * LANES : (h + 1) * LANES] = tiles[h].astype(bf16)


def gated_kernel(normed_ref, value_ref, gate_ref, out_ref):
    value = jnp.zeros((ROWS, LANES), f32)
    gate = jnp.zeros((ROWS, LANES), f32)
    for f in range(N_FS):
        for b in range(4):
            rows = normed_ref[:, f * 512 + b * LANES : f * 512 + (b + 1) * LANES]
            cols = slice(b * LANES, (b + 1) * LANES)
            value = value + jnp.dot(rows, value_ref[f, :128, cols], preferred_element_type=f32)
            gate = gate + jnp.dot(rows, gate_ref[f, :128, cols], preferred_element_type=f32)
    out_ref[...] = (value * jax.nn.sigmoid(gate)).astype(bf16)


def conv_kernel_body(halo_ref, gated_ref, taps_ref, sum_ref, stat_ref, ext_scr):
    ext_scr[:HALO, :] = halo_ref[...].astype(f32)
    ext_scr[HALO:, :] = gated_ref[...].astype(f32)
    start = HALO - (TAPS - 1)
    block = LANES
    stat_ref[4:, :] = jnp.zeros((4, LANES), f32)
    for n in range(ROWS // block):
        r = n * block
        running = jnp.zeros((block, LANES), f32)
        for j in range(TAPS):
            running = running + ext_scr[pl.ds(r + start + j, block), :] * taps_ref[j : j + 1, :]
        sum_ref[r : r + block, :] = running
        flat = running.T
        total = jnp.sum(flat, axis=0, keepdims=True)
        off = flat - total * (1.0 / LANES)
        stat_ref[n : n + 1, :] = total
        stat_ref[2 + n : 3 + n, :] = jnp.sum(off * off, axis=0, keepdims=True)


def channel_kernel(sum_ref, stat_ref, gain_ref, shift_ref, out_ref):
    for n in range(ROWS // LANES):
        total = stat_ref[0, n : n + 1, :]
        for g in range(1, N_TP):
            total = total + stat_ref[g, n : n + 1, :]
        mean = total * (1.0 / CONV_W)
        spread = jnp.zeros((1, LANES), f32)
        for g in range(N_TP):
            apart = stat_ref[g, n : n + 1, :] * (1.0 / LANES) - mean
            spread = spread + stat_ref[g, 2 + n : 3 + n, :] + LANES * apart * apart
        scale = lax.rsqrt(spread * (1.0 / CONV_W) + epsilon)
        mean = jnp.broadcast_to(mean, (LANES, LANES)).T
        scale = jnp.broadcast_to(scale, (LANES, LANES)).T
        rows = slice(n * LANES, (n + 1) * LANES)
        value = (sum_ref[rows, :] - mean) * scale * gain_ref[...] + shift_ref[...]
        out_ref[rows, :] = (value / (1.0 + jnp.exp(-value))).astype(bf16)


def attend(q_ref, blocks, state, hidden, mask=None):
    rate = QK_DIM ** (-0.5) * log2_e
    fresh = []
    for h in range(2):
        top, total, weighted = state[h]
        keys = jnp.concatenate([b[h * ROWS : (h + 1) * ROWS, :] for b in blocks], axis=0)
        scores = lax.dot_general(
            keys,
            q_ref[:, h * LANES : (h + 1) * LANES],
            (((1,), (1,)), ((), ())),
            preferred_element_type=f32,
        )
        if mask is not None:
            scores = jnp.where(mask, scores, masked_score)
        new_top = top
        for n, off in enumerate(hidden):
            part = jnp.max(scores[n * ROWS : (n + 1) * ROWS], axis=0, keepdims=True)
            new_top = jnp.maximum(new_top, part - off)
        weights = jnp.concatenate(
            [
                jnp.exp2(scores[n * ROWS : (n + 1) * ROWS] * rate - (new_top * rate + off))
                for n, off in enumerate(hidden)
            ],
            axis=0,
        )
        factor = jnp.exp2((top - new_top) * rate)
        total = total * factor + jnp.sum(weights, axis=0, keepdims=True)
        at = 2 * ROWS + h * V_DIM
        values = jnp.concatenate(
            [b[at + i * LANES : at + i * LANES + V_DIM, :] for b in blocks for i in range(2)],
            axis=1,
        )
        weighted = weighted * factor + jnp.dot(
            values, weights.astype(bf16), preferred_element_type=f32
        )
        fresh.append((new_top, total, weighted))
    return fresh


def own_kernel(q_ref, own_ref, stat_ref, acc_ref):
    key = lax.broadcasted_iota(jnp.int32, (ROWS, ROWS), 0)
    query = lax.broadcasted_iota(jnp.int32, (ROWS, ROWS), 1)
    mask = jnp.right_shift(key, 6) <= jnp.right_shift(query, 6)
    empty = (
        jnp.full((1, ROWS), masked_score, f32),
        jnp.zeros((1, ROWS), f32),
        jnp.zeros((V_DIM, ROWS), f32),
    )
    state = attend(q_ref, [own_ref], [empty, empty], [0.0], mask)
    stat_ref[4:, :] = jnp.zeros((4, ROWS), f32)
    for h in range(2):
        stat_ref[2 * h : 2 * h + 1, :] = state[h][0]
        stat_ref[2 * h + 1 : 2 * h + 2, :] = state[h][1]
        acc_ref[h * V_DIM : (h + 1) * V_DIM, :] = state[h][2]


def attention_kernel(at_ref, q_ref, kv_ref, stat_ref, acc_ref, conv_ref, second_ref, third_ref, out_ref, kv, sems):
    at = at_ref[0]
    copies = [
        pltpu.make_async_copy(kv_ref.at[n], kv.at[n], sems.at[n]) for n in range(N_SP // BUNDLE)
    ]
    for copy in copies:
        copy.start()
    state = [
        (
            stat_ref[2 * h : 2 * h + 1, :],
            stat_ref[2 * h + 1 : 2 * h + 2, :],
            acc_ref[h * V_DIM : (h + 1) * V_DIM, :],
        )
        for h in range(2)
    ]
    for n, copy in enumerate(copies):
        copy.wait()
        hidden = [jnp.where(n * BUNDLE + i < at, 0.0, -masked_score) for i in range(BUNDLE)]
        blocks = [kv.at[n, i] for i in range(BUNDLE)]
        state = lax.cond(
            n * BUNDLE < at,
            lambda s, blocks=blocks, hidden=hidden: attend(q_ref, blocks, s, hidden),
            lambda s: s,
            state,
        )
    result = jnp.concatenate([state[h][2] / state[h][1] for h in range(2)], axis=0).T.astype(bf16)
    result = jnp.concatenate([result, conv_ref[...]], axis=1)
    share = ROWS // N_TP
    for f in range(N_FS):
        weight = jnp.concatenate([second_ref[f, 128:, :], third_ref[f]], axis=0)
        part = jnp.dot(result, weight, preferred_element_type=f32).astype(bf16)
        for r in range(N_TP):
            out_ref[r, :, f * 512 : (f + 1) * 512] = part[r * share : (r + 1) * share]


def total_kernel(in_ref, out_ref):
    total = in_ref[0].astype(f32)
    for g in range(1, N_TP):
        total = total + in_ref[g].astype(f32)
    out_ref[...] = total.astype(bf16)


def assemble_kernel(core_ref, mine_ref, other_ref, out_ref):
    share = ROWS // N_TP

    def place(first, second):
        for x in range(N_TP // 2):
            out_ref[2 * x * share : (2 * x + 1) * share, :] = first[x]
            out_ref[(2 * x + 1) * share : (2 * x + 2) * share, :] = second[x]

    pl.when(core_ref[0] == 0)(lambda: place(mine_ref, other_ref))
    pl.when(core_ref[0] == 1)(lambda: place(other_ref, mine_ref))


def rotation_tables(positions):
    inverse_freq = 1.0 / rope_base ** (jnp.arange(0, QK_ROPE, 2, dtype=f32) / QK_ROPE)
    angles = positions.astype(f32)[None, :] * inverse_freq[:, None]
    return jnp.cos(angles), jnp.sin(angles)


def local(
    tokens,
    mix_gain,
    query_down,
    memory_down,
    rope_weight,
    query_up,
    key_up,
    value_up,
    latent_gain,
    memory_gain,
    query_gain,
    key_gain,
    conv_value,
    conv_gate,
    conv_kernel,
    channel_gain,
    channel_shift,
    heads_out,
    conv_out,
):
    at = lax.axis_index("sp")
    hbm = pl.BlockSpec(memory_space=pltpu.HBM)
    vmem = pl.BlockSpec(memory_space=pltpu.VMEM)
    def kept(*arrays):
        return [pltpu.with_memory_space_constraint(a, pltpu.HBM) for a in arrays]

    narrow, rope_w, gain = call(
        pack_kernel,
        (
            jax.ShapeDtypeStruct((224, 512), bf16),
            jax.ShapeDtypeStruct((QK_ROPE, 2048), bf16),
            jax.ShapeDtypeStruct((1, 2048), f32),
        ),
        [pltpu.SemaphoreType.DMA((8,))],
        specs=[hbm] * 6,
    )(
        *kept(
            query_down.T, memory_down.T, key_up, value_up, rope_weight.T, mix_gain[None, :]
        )
    )
    narrow_all = lax.all_gather(narrow, "fs")
    positions = at * ROWS + jnp.arange(ROWS, dtype=jnp.int32)
    cosine, sine = rotation_tables(positions)
    table = jax.ShapeDtypeStruct((ROWS, LANES), f32)
    latents, rope_rows, normed, cosine, sine_up, sine_down = call(
        project_kernel,
        (
            jax.ShapeDtypeStruct((320, LANES), bf16),
            jax.ShapeDtypeStruct((ROWS, LANES), bf16),
            jax.ShapeDtypeStruct((ROWS, 2048), bf16),
            table,
            table,
            table,
        ),
        [pltpu.VMEM((ROWS, 2048), bf16), pltpu.SemaphoreType.DMA((4,))],
        specs=[hbm] + [vmem] * 5,
    )(pltpu.with_memory_space_constraint(tokens[0], pltpu.HBM), gain, rope_w, cosine, sine, narrow_all)
    latents = lax.all_gather(latents, "tp")

    def row(vector, width):
        return jnp.pad(vector, (0, width - vector.shape[0]))[None, :]

    own = call(
        keys_values_kernel,
        jax.ShapeDtypeStruct((6 * LANES, LANES), bf16),
        [pltpu.VMEM((ROWS, KV_LAT), bf16), pltpu.VMEM((KV_LAT, 256), bf16)],
    )(
        latents, rope_rows, narrow_all, memory_gain[None, :], row(key_gain, LANES),
        cosine, sine_up, sine_down,
    )
    own, *rest = lax.optimization_barrier(
        (own, query_up, conv_value, conv_gate, heads_out, conv_out)
    )
    pieces = lax.all_gather(own, "sp")
    packed = call(
        pack_rest_kernel,
        tuple(jax.ShapeDtypeStruct((rows, 512), bf16) for rows in (224, 192, 192)),
        [pltpu.VMEM((192, 192), bf16), pltpu.SemaphoreType.DMA((12,))],
        specs=[hbm] * 5,
    )(*kept(*rest))
    first_all, second_all = (lax.all_gather(p, "fs") for p in packed[:2])
    queries = call(
        queries_kernel,
        jax.ShapeDtypeStruct((ROWS, 2 * LANES), bf16),
        [pltpu.VMEM((ROWS, Q_LAT), bf16)],
    )(
        latents, first_all, latent_gain[None, :], row(query_gain, LANES),
        cosine, sine_up, sine_down,
    )
    gated = call(gated_kernel, jax.ShapeDtypeStruct((ROWS, LANES), bf16))(normed, first_all, second_all)
    halo = lax.ppermute(gated[ROWS - HALO :], "sp", [(i, i + 1) for i in range(N_SP - 1)])
    taps = jnp.pad(conv_kernel.astype(f32), ((0, 1), (0, 0)))
    conv_sum, stats = call(
        conv_kernel_body,
        (jax.ShapeDtypeStruct((ROWS, LANES), f32), jax.ShapeDtypeStruct((8, LANES), f32)),
        [pltpu.VMEM((ROWS + HALO, LANES), f32)],
    )(halo, gated, taps)
    stats = lax.all_gather(stats, "tp")
    conv_result = call(channel_kernel, jax.ShapeDtypeStruct((ROWS, LANES), bf16))(
        conv_sum, stats, channel_gain[None, :], channel_shift[None, :]
    )
    stat, acc = call(
        own_kernel,
        (jax.ShapeDtypeStruct((8, ROWS), f32), jax.ShapeDtypeStruct((2 * V_DIM, ROWS), f32)),
    )(queries, own)
    third_all = lax.all_gather(packed[2], "fs")
    core = jnp.bitwise_and(lax.axis_index("tp"), 1)[None]
    pieces = pltpu.with_memory_space_constraint(
        pieces.reshape(N_SP // BUNDLE, BUNDLE, 6 * LANES, LANES), pltpu.HBM
    )
    partial = call(
        attention_kernel,
        jax.ShapeDtypeStruct((N_TP, ROWS // N_TP, 2048), bf16),
        [
            pltpu.VMEM((N_SP // BUNDLE, BUNDLE, 6 * LANES, LANES), bf16),
            pltpu.SemaphoreType.DMA((N_SP // BUNDLE,)),
        ],
        specs=[
            pl.BlockSpec(memory_space=pltpu.SMEM), vmem, hbm, vmem, vmem, vmem, vmem, vmem,
        ],
    )(at[None], queries, pieces, stat, acc, conv_result, second_all, third_all)
    share = lax.all_to_all(partial, "tp", split_axis=0, concat_axis=0, tiled=True)
    share = call(total_kernel, jax.ShapeDtypeStruct((ROWS // N_TP, 2048), bf16))(share)
    mine = lax.all_gather(share, "tp", axis_index_groups=SAME_CORE)
    other = lax.ppermute(mine, "tp", CORE_PAIRS)
    mixed = call(
        assemble_kernel, jax.ShapeDtypeStruct((ROWS, 2048), bf16), scalars=1, arrays=2
    )(core, mine, other)
    return mixed[None]


def solution(mesh):
    in_specs = (
        P("fs", "sp", None),
        P(),
        P("fs", "tp"),
        P("fs", "tp"),
        P(),
        P("fs", "tp"),
        P("fs", "tp"),
        P("fs", "tp"),
        P(),
        P(),
        P(),
        P(),
        P("fs", "tp"),
        P("fs", "tp"),
        P(None, "tp"),
        P("tp"),
        P("tp"),
        P("tp", "fs"),
        P("tp", "fs"),
    )
    out_specs = P("fs", "sp", None)
    return jax.shard_map(local, mesh=mesh, in_specs=in_specs, out_specs=out_specs, check_vma=False)
```

```python
import jax
import jax.numpy as jnp
from jax import lax
from jax.experimental import pallas as pl
from jax.experimental.pallas import tpu as pltpu
from jax.sharding import PartitionSpec as P

QK_NOPE = 64
QK_ROPE = 32
V_DIM = 64
CONV_W = 1024
SEG = 64
QK_DIM = 96
Q_LAT = 768
KV_LAT = 512
ROWS = 256
TAPS = 31
HALO = 32
LANES = 128
N_FS = 4
N_TP = 8
N_SP = 16
BUNDLE = 4

epsilon = 1e-06
rope_base = 10000.0
masked_score = -1e30
log2_e = 1.4426950408889634
bf16 = jnp.bfloat16
f32 = jnp.float32

CORE_PAIRS = [(i, i ^ 1) for i in range(N_TP)]


def call(kernel, out_shape, scratch=(), scalars=0, arrays=0, specs=None, outs=None):
    extra = {"out_specs": outs} if outs else {}
    if scalars:
        smem = pl.BlockSpec(memory_space=pltpu.SMEM)
        specs = [smem] * scalars + [pl.BlockSpec(memory_space=pltpu.VMEM)] * arrays
    if specs:
        extra["in_specs"] = specs
    return pl.pallas_call(
        kernel,
        out_shape=out_shape,
        scratch_shapes=list(scratch),
        compiler_params=pltpu.CompilerParams(vmem_limit_bytes=16 * 1024 * 1024),
        **extra,
    )


def head_tile(tile, gain, cosine, sine_up, sine_down):
    scale = lax.rsqrt(jnp.sum(tile * tile, axis=-1, keepdims=True) * (1.0 / QK_DIM) + epsilon)
    tile = tile * scale * gain
    half = QK_ROPE // 2
    return (
        tile * cosine
        + pltpu.roll(tile, LANES - half, 1) * sine_up
        + pltpu.roll(tile, half, 1) * sine_down
    )


def copy_all(pairs, sems):
    copies = [
        pltpu.make_async_copy(source, target, sems.at[n]) for n, (source, target) in enumerate(pairs)
    ]
    for copy in copies:
        copy.start()
    for copy in copies:
        copy.wait()


def pack_kernel(qd_ref, md_ref, ku_ref, vu_ref, rope_ref, gain_ref, ho_ref, co_ref, narrow_ref, rope_out, gain_out, outw_ref, sems):
    pairs = [
        (qd_ref, narrow_ref.at[:96, :]),
        (md_ref, narrow_ref.at[96:160, :]),
        (rope_ref, rope_out),
        (gain_ref, gain_out),
        (ho_ref, outw_ref.at[:128, :]),
        (co_ref, outw_ref.at[128:, :]),
    ]
    for n, ref in enumerate((ku_ref, vu_ref)):
        for b in range(2):
            at = (2 * n + b) * LANES
            pairs.append((ref.at[b * 64 : (b + 1) * 64, :], narrow_ref.at[160:, at : at + LANES]))
    copy_all(pairs, sems)


def pack_rest_kernel(qu_ref, cv_ref, cg_ref, first_ref, second_ref, qu_scr, sems):
    pairs = [(qu_ref, qu_scr)]
    for ref, out in ((cv_ref, first_ref), (cg_ref, second_ref)):
        for b in range(4):
            rows = slice(b * 128, (b + 1) * 128)
            pairs.append((ref.at[rows, :], out.at[:128, rows]))
    copy_all(pairs, sems)
    first_ref[128:, :] = jnp.zeros((96, 512), bf16)
    for half in range(2):
        for h in range(2):
            at = half * 256 + h * LANES
            first_ref[128:, at : at + QK_DIM] = qu_scr[
                half * 96 : (half + 1) * 96, h * QK_DIM : (h + 1) * QK_DIM
            ]


def project_kernel(tok_ref, gain_ref, rope_w_ref, cos_ref, sin_ref, w_ref, lat_ref, rope_ref, normed_ref, cosine_ref, up_ref, down_ref, tok_scr, sems):
    block = 64
    copies = []
    for n in range(ROWS // block):
        rows = slice(n * block, (n + 1) * block)
        copies.append(
            pltpu.make_async_copy(tok_ref.at[rows, :], tok_scr.at[rows, :], sems.at[n])
        )
        copies[-1].start()
    turned = (((1,), (1,)), ((), ()))
    for r in range(0, ROWS, block):
        copies[r // block].wait()
        rows = tok_scr[r : r + block, :].astype(f32)
        scale = lax.rsqrt(jnp.mean(rows * rows, axis=-1, keepdims=True) + epsilon)
        normed_ref[r : r + block, :] = (rows * scale * gain_ref[...]).astype(bf16)
    both = jnp.zeros((ROWS, 160), f32)
    for f in range(N_FS):
        both = both + lax.dot_general(
            normed_ref[:, f * 512 : (f + 1) * 512],
            w_ref[f, :160, :],
            turned,
            preferred_element_type=f32,
        )
    both = both.astype(bf16)
    lat_ref[:ROWS, :] = both[:, :LANES]
    for r in range(4):
        lat_ref[ROWS:, r * 32 : (r + 1) * 32] = both[r * 64 : (r + 1) * 64, LANES:]
    rope = lax.dot_general(normed_ref[...], rope_w_ref[...], turned, preferred_element_type=f32)
    rope_ref[...] = jnp.zeros((ROWS, LANES), bf16)
    rope_ref[:, QK_NOPE:QK_DIM] = rope.astype(bf16)
    half = QK_ROPE // 2
    empty = jnp.zeros((ROWS, LANES - half), f32)
    cosine = jnp.concatenate([cos_ref[...].T, empty], axis=1)
    sine = jnp.concatenate([sin_ref[...].T, empty], axis=1)
    lane = lax.broadcasted_iota(jnp.int32, (ROWS, LANES), 1)
    cosine = pltpu.roll(cosine, QK_NOPE, 1) + pltpu.roll(cosine, QK_NOPE + half, 1)
    cosine_ref[...] = jnp.where(lane < QK_NOPE, 1.0, cosine)
    up_ref[...] = -pltpu.roll(sine, QK_NOPE, 1)
    down_ref[...] = pltpu.roll(sine, QK_NOPE + half, 1)


def keys_values_kernel(lat_ref, rope_ref, w_ref, mgain_ref, kgain_ref, cos_ref, up_ref, down_ref, out_ref, m_scr, w_scr):
    for g in range(N_TP):
        at = g * 64
        m_scr[:, at : at + 32] = lat_ref[g, :ROWS, 96:]
        for r in range(4):
            m_scr[r * 64 : (r + 1) * 64, at + 32 : at + 64] = lat_ref[
                g, ROWS:, r * 32 : (r + 1) * 32
            ]
    raw = m_scr[...].astype(f32)
    scale = lax.rsqrt(jnp.mean(raw * raw, axis=-1, keepdims=True) + epsilon)
    m_scr[...] = (raw * scale * mgain_ref[...]).astype(bf16)
    for f in range(N_FS):
        for n in range(2):
            for b in range(2):
                lanes = (2 * n + b) * LANES
                row = f * 128 + b * 64
                w_scr[row : row + 64, n * LANES : (n + 1) * LANES] = w_ref[
                    f, 160:, lanes : lanes + LANES
                ]
    both = jnp.dot(m_scr[...], w_scr[...], preferred_element_type=f32)
    nope = both[:, :LANES]
    lane = lax.broadcasted_iota(jnp.int32, (ROWS, LANES), 1)
    rope = rope_ref[...].astype(f32)
    tiles = []
    for h in range(2):
        part = nope if h == 0 else pltpu.roll(nope, 64, 1)
        tile = jnp.where(lane < QK_NOPE, part, rope)
        tiles.append(head_tile(tile, kgain_ref[...], cos_ref[...], up_ref[...], down_ref[...]))
    for h in range(2):
        out_ref[h * ROWS : (h + 1) * ROWS, :] = tiles[h].astype(bf16)
    values = both[:, LANES:].T.astype(bf16)
    for half in range(2):
        at = 2 * ROWS + half * LANES
        out_ref[at : at + LANES, :] = values[:, half * LANES : (half + 1) * LANES]


def queries_kernel(lat_ref, w_ref, lgain_ref, qgain_ref, cos_ref, up_ref, down_ref, out_ref, q_scr):
    for g in range(N_TP):
        q_scr[:, g * 96 : (g + 1) * 96] = lat_ref[g, :ROWS, :96]
    raw = q_scr[...].astype(f32)
    scale = lax.rsqrt(jnp.mean(raw * raw, axis=-1, keepdims=True) + epsilon)
    q_scr[...] = (raw * scale * lgain_ref[...]).astype(bf16)
    both = jnp.zeros((ROWS, 2 * LANES), f32)
    for f in range(N_FS):
        for half in range(2):
            at = f * 192 + half * 96
            both = both + jnp.dot(
                q_scr[:, at : at + 96],
                w_ref[f, 128:, half * 256 : (half + 1) * 256],
                preferred_element_type=f32,
            )
    lane = lax.broadcasted_iota(jnp.int32, (ROWS, LANES), 1)
    tiles = [
        head_tile(
            both[:, h * LANES : (h + 1) * LANES],
            qgain_ref[...],
            cos_ref[...],
            up_ref[...],
            down_ref[...],
        )
        for h in range(2)
    ]
    for h in range(2):
        out_ref[:, h * LANES : (h + 1) * LANES] = tiles[h].astype(bf16)


def gated_kernel(normed_ref, value_ref, gate_ref, out_ref):
    value = jnp.zeros((ROWS, LANES), f32)
    gate = jnp.zeros((ROWS, LANES), f32)
    for f in range(N_FS):
        for b in range(4):
            rows = normed_ref[:, f * 512 + b * LANES : f * 512 + (b + 1) * LANES]
            cols = slice(b * LANES, (b + 1) * LANES)
            value = value + jnp.dot(rows, value_ref[f, :128, cols], preferred_element_type=f32)
            gate = gate + jnp.dot(rows, gate_ref[f, :128, cols], preferred_element_type=f32)
    out_ref[...] = (value * jax.nn.sigmoid(gate)).astype(bf16)


def conv_kernel_body(halo_ref, gated_ref, taps_ref, gain_ref, shift_ref, out_ref, ext_scr, stat_scr):
    ext_scr[:HALO, :] = halo_ref[...].astype(f32)
    ext_scr[HALO:, :] = gated_ref[...].astype(f32)
    start = HALO - (TAPS - 1)
    block = LANES
    stat_scr[...] = jnp.zeros((16, LANES), f32)
    for n in range(ROWS // block):
        r = n * block
        running = jnp.zeros((block, LANES), f32)
        for j in range(TAPS):
            running = running + ext_scr[pl.ds(r + start + j, block), :] * taps_ref[j : j + 1, :]
        flat = running.T
        mean = jnp.sum(flat, axis=0, keepdims=True) * (1.0 / LANES)
        off = flat - mean
        stat_scr[n : n + 1, :] = mean
        stat_scr[2 + n : 3 + n, :] = jnp.sum(off * off, axis=0, keepdims=True)
        out_ref[r : r + block, :] = off.T.astype(bf16)
    stat_scr[4:5, :] = gain_ref[...]
    stat_scr[5:6, :] = shift_ref[...]
    left = stat_scr[...]
    for part in range(3):
        rounded = left.astype(bf16)
        out_ref[ROWS + part * 16 : ROWS + (part + 1) * 16, :] = rounded
        left = left - rounded.astype(f32)


def channel_kernel(in_ref, out_ref):
    stats = []
    for g in range(N_TP):
        parts = [
            in_ref[g, ROWS + part * 16 : ROWS + (part + 1) * 16, :].astype(f32) for part in range(3)
        ]
        stats.append(parts[0] + (parts[1] + parts[2]))
    for n in range(ROWS // LANES):
        means = [st[n : n + 1] for st in stats]
        mean = means[0]
        for g in range(1, N_TP):
            mean = mean + means[g]
        mean = mean * (1.0 / N_TP)
        spread = jnp.zeros((1, LANES), f32)
        for g in range(N_TP):
            apart = means[g] - mean
            spread = spread + stats[g][2 + n : 3 + n] + LANES * apart * apart
        scale = lax.rsqrt(spread * (1.0 / CONV_W) + epsilon)
        columns = jnp.concatenate(
            [m - mean for m in means] + [scale] + [jnp.zeros((7, LANES), f32)], axis=0
        ).T
        rows = slice(n * LANES, (n + 1) * LANES)
        for g in range(N_TP):
            value = in_ref[g, rows, :].astype(f32) + columns[:, g : g + 1]
            value = value * columns[:, N_TP : N_TP + 1] * stats[g][4:5] + stats[g][5:6]
            out_ref[g, rows, :] = (value / (1.0 + jnp.exp(-value))).astype(bf16)


def attend(q_ref, blocks, state, hidden, mask=None):
    rate = QK_DIM ** (-0.5) * log2_e
    fresh = []
    for h in range(2):
        top, total, weighted = state[h]
        keys = jnp.concatenate([b[h * ROWS : (h + 1) * ROWS, :] for b in blocks], axis=0)
        scores = lax.dot_general(
            keys,
            q_ref[:, h * LANES : (h + 1) * LANES],
            (((1,), (1,)), ((), ())),
            preferred_element_type=f32,
        )
        if mask is not None:
            scores = jnp.where(mask, scores, masked_score)
        new_top = top
        for n, off in enumerate(hidden):
            part = jnp.max(scores[n * ROWS : (n + 1) * ROWS], axis=0, keepdims=True)
            new_top = jnp.maximum(new_top, part - off)
        weights = jnp.concatenate(
            [
                jnp.exp2(scores[n * ROWS : (n + 1) * ROWS] * rate - (new_top * rate + off))
                for n, off in enumerate(hidden)
            ],
            axis=0,
        )
        factor = jnp.exp2((top - new_top) * rate)
        total = total * factor + jnp.sum(weights, axis=0, keepdims=True)
        at = 2 * ROWS + h * V_DIM
        values = jnp.concatenate(
            [b[at + i * LANES : at + i * LANES + V_DIM, :] for b in blocks for i in range(2)],
            axis=1,
        )
        weighted = weighted * factor + jnp.dot(
            values, weights.astype(bf16), preferred_element_type=f32
        )
        fresh.append((new_top, total, weighted))
    return fresh


def own_kernel(q_ref, own_ref, stat_ref, acc_ref):
    key = lax.broadcasted_iota(jnp.int32, (ROWS, ROWS), 0)
    query = lax.broadcasted_iota(jnp.int32, (ROWS, ROWS), 1)
    mask = jnp.right_shift(key, 6) <= jnp.right_shift(query, 6)
    empty = (
        jnp.full((1, ROWS), masked_score, f32),
        jnp.zeros((1, ROWS), f32),
        jnp.zeros((V_DIM, ROWS), f32),
    )
    state = attend(q_ref, [own_ref], [empty, empty], [0.0], mask)
    stat_ref[4:, :] = jnp.zeros((4, ROWS), f32)
    for h in range(2):
        stat_ref[2 * h : 2 * h + 1, :] = state[h][0]
        stat_ref[2 * h + 1 : 2 * h + 2, :] = state[h][1]
        acc_ref[h * V_DIM : (h + 1) * V_DIM, :] = state[h][2]


def attention_kernel(at_ref, q_ref, kv_ref, stat_ref, acc_ref, out_ref, kv, sems):
    at = at_ref[0]
    copies = [
        pltpu.make_async_copy(kv_ref.at[n], kv.at[n], sems.at[n]) for n in range(N_SP // BUNDLE)
    ]
    for copy in copies:
        copy.start()
    state = [
        (
            stat_ref[2 * h : 2 * h + 1, :],
            stat_ref[2 * h + 1 : 2 * h + 2, :],
            acc_ref[h * V_DIM : (h + 1) * V_DIM, :],
        )
        for h in range(2)
    ]
    for n, copy in enumerate(copies):
        copy.wait()
        hidden = [jnp.where(n * BUNDLE + i < at, 0.0, -masked_score) for i in range(BUNDLE)]
        blocks = [kv.at[n, i] for i in range(BUNDLE)]
        state = lax.cond(
            n * BUNDLE < at,
            lambda s, blocks=blocks, hidden=hidden: attend(q_ref, blocks, s, hidden),
            lambda s: s,
            state,
        )
    result = jnp.concatenate([state[h][2] / state[h][1] for h in range(2)], axis=0)
    out_ref[...] = result.T.astype(bf16)


def sources(g):
    other = g + 1 - 2 * lax.rem(g, 2)
    return [lax.rem(first + N_TP - s, N_TP) for first in (g, other) for s in (0, 2, 4, 6)]


def conv_part_kernel(tp_ref, conv_ref, *rest):
    pieces, out_ref = rest[:N_TP], rest[N_TP]
    for f in range(N_FS):
        total = jnp.zeros((ROWS, 512), f32)
        for g, piece in zip(sources(tp_ref[0]), pieces):
            total = total + jnp.dot(conv_ref[g], piece[f, 128:, :], preferred_element_type=f32)
        out_ref[:, f * 512 : (f + 1) * 512] = total


def output_kernel(tp_ref, base_ref, attn_ref, *rest):
    pieces, out_ref = rest[:N_TP], rest[N_TP]
    for f in range(N_FS):
        cols = slice(f * 512, (f + 1) * 512)
        total = base_ref[:, cols]
        for g, piece in zip(sources(tp_ref[0]), pieces):
            total = total + jnp.dot(attn_ref[g], piece[f, :128, :], preferred_element_type=f32)
        out_ref[:, cols] = total.astype(bf16)


def rotation_tables(positions):
    inverse_freq = 1.0 / rope_base ** (jnp.arange(0, QK_ROPE, 2, dtype=f32) / QK_ROPE)
    angles = positions.astype(f32)[None, :] * inverse_freq[:, None]
    return jnp.cos(angles), jnp.sin(angles)


def local(
    tokens,
    mix_gain,
    query_down,
    memory_down,
    rope_weight,
    query_up,
    key_up,
    value_up,
    latent_gain,
    memory_gain,
    query_gain,
    key_gain,
    conv_value,
    conv_gate,
    conv_kernel,
    channel_gain,
    channel_shift,
    heads_out,
    conv_out,
):
    at = lax.axis_index("sp")
    hbm = pl.BlockSpec(memory_space=pltpu.HBM)
    vmem = pl.BlockSpec(memory_space=pltpu.VMEM)
    def kept(*arrays):
        return [pltpu.with_memory_space_constraint(a, pltpu.HBM) for a in arrays]

    narrow, rope_w, gain, outw = call(
        pack_kernel,
        (
            jax.ShapeDtypeStruct((224, 512), bf16),
            jax.ShapeDtypeStruct((QK_ROPE, 2048), bf16),
            jax.ShapeDtypeStruct((1, 2048), f32),
            jax.ShapeDtypeStruct((256, 512), bf16),
        ),
        [pltpu.SemaphoreType.DMA((10,))],
        specs=[hbm] * 8,
        outs=[vmem, vmem, vmem, hbm],
    )(
        *kept(
            query_down.T, memory_down.T, key_up, value_up, rope_weight.T, mix_gain[None, :],
            heads_out, conv_out,
        )
    )
    out_all = lax.all_gather(outw, "fs")
    narrow_all = lax.all_gather(narrow, "fs")
    positions = at * ROWS + jnp.arange(ROWS, dtype=jnp.int32)
    cosine, sine = rotation_tables(positions)
    table = jax.ShapeDtypeStruct((ROWS, LANES), f32)
    latents, rope_rows, normed, cosine, sine_up, sine_down = call(
        project_kernel,
        (
            jax.ShapeDtypeStruct((320, LANES), bf16),
            jax.ShapeDtypeStruct((ROWS, LANES), bf16),
            jax.ShapeDtypeStruct((ROWS, 2048), bf16),
            table,
            table,
            table,
        ),
        [pltpu.VMEM((ROWS, 2048), bf16), pltpu.SemaphoreType.DMA((4,))],
        specs=[hbm] + [vmem] * 5,
    )(pltpu.with_memory_space_constraint(tokens[0], pltpu.HBM), gain, rope_w, cosine, sine, narrow_all)
    latents = lax.all_gather(latents, "tp")

    def row(vector, width):
        return jnp.pad(vector, (0, width - vector.shape[0]))[None, :]

    own = call(
        keys_values_kernel,
        jax.ShapeDtypeStruct((6 * LANES, LANES), bf16),
        [pltpu.VMEM((ROWS, KV_LAT), bf16), pltpu.VMEM((KV_LAT, 256), bf16)],
    )(
        latents, rope_rows, narrow_all, memory_gain[None, :], row(key_gain, LANES),
        cosine, sine_up, sine_down,
    )
    own, out_all, *rest = lax.optimization_barrier(
        (own, out_all, query_up, conv_value, conv_gate)
    )
    pieces = lax.all_gather(own, "sp")
    far = [
        lax.ppermute(out_all, "tp", [(i, (i + by) % N_TP) for i in range(N_TP)]) for by in (4, 2, 6)
    ]
    far = [far[1], far[0], far[2]]
    near = lax.ppermute(out_all, "tp", CORE_PAIRS)
    packed = call(
        pack_rest_kernel,
        tuple(jax.ShapeDtypeStruct((rows, 512), bf16) for rows in (224, 128)),
        [pltpu.VMEM((192, 192), bf16), pltpu.SemaphoreType.DMA((9,))],
        specs=[hbm] * 3,
    )(*kept(*rest))
    first_all, second_all = (lax.all_gather(p, "fs") for p in packed)
    queries = call(
        queries_kernel,
        jax.ShapeDtypeStruct((ROWS, 2 * LANES), bf16),
        [pltpu.VMEM((ROWS, Q_LAT), bf16)],
    )(
        latents, first_all, latent_gain[None, :], row(query_gain, LANES),
        cosine, sine_up, sine_down,
    )
    gated = call(gated_kernel, jax.ShapeDtypeStruct((ROWS, LANES), bf16))(normed, first_all, second_all)
    halo = lax.ppermute(gated[ROWS - HALO :], "sp", [(i, i + 1) for i in range(N_SP - 1)])
    taps = jnp.pad(conv_kernel.astype(f32), ((0, 1), (0, 0)))
    conv_sum = call(
        conv_kernel_body,
        jax.ShapeDtypeStruct((ROWS + 48, LANES), bf16),
        [pltpu.VMEM((ROWS + HALO, LANES), f32), pltpu.VMEM((16, LANES), f32)],
    )(halo, gated, taps, channel_gain[None, :], channel_shift[None, :])
    conv_sum = lax.all_gather(conv_sum, "tp")
    conv_sum, near, *far = lax.optimization_barrier((conv_sum, near, *far))
    crossed = [lax.ppermute(w, "tp", CORE_PAIRS) for w in far]
    weights = [out_all, *far, near, *crossed]
    conv_result = call(channel_kernel, jax.ShapeDtypeStruct((N_TP, ROWS, LANES), bf16))(conv_sum)
    tp = lax.axis_index("tp")[None]
    base = call(
        conv_part_kernel, jax.ShapeDtypeStruct((ROWS, 2048), f32), scalars=1, arrays=1 + N_TP
    )(tp, conv_result, *weights)
    stat, acc = call(
        own_kernel,
        (jax.ShapeDtypeStruct((8, ROWS), f32), jax.ShapeDtypeStruct((2 * V_DIM, ROWS), f32)),
    )(queries, own)
    pieces, base, stat, acc = lax.optimization_barrier((pieces, base, stat, acc))
    pieces = pltpu.with_memory_space_constraint(
        pieces.reshape(N_SP // BUNDLE, BUNDLE, 6 * LANES, LANES), pltpu.HBM
    )
    attention = call(
        attention_kernel,
        jax.ShapeDtypeStruct((ROWS, LANES), bf16),
        [
            pltpu.VMEM((N_SP // BUNDLE, BUNDLE, 6 * LANES, LANES), bf16),
            pltpu.SemaphoreType.DMA((N_SP // BUNDLE,)),
        ],
        specs=[pl.BlockSpec(memory_space=pltpu.SMEM), vmem, hbm, vmem, vmem],
    )(at[None], queries, pieces, stat, acc)
    attention = lax.all_gather(attention, "tp")
    mixed = call(
        output_kernel, jax.ShapeDtypeStruct((ROWS, 2048), bf16), scalars=1, arrays=2 + N_TP
    )(tp, base, attention, *weights)
    return mixed[None]


def solution(mesh):
    in_specs = (
        P("fs", "sp", None),
        P(),
        P("fs", "tp"),
        P("fs", "tp"),
        P(),
        P("fs", "tp"),
        P("fs", "tp"),
        P("fs", "tp"),
        P(),
        P(),
        P(),
        P(),
        P("fs", "tp"),
        P("fs", "tp"),
        P(None, "tp"),
        P("tp"),
        P("tp"),
        P("tp", "fs"),
        P("tp", "fs"),
    )
    out_specs = P("fs", "sp", None)
    return jax.shard_map(local, mesh=mesh, in_specs=in_specs, out_specs=out_specs, check_vma=False)
```

```python
import jax
import jax.numpy as jnp
from jax import lax
from jax.experimental import pallas as pl
from jax.experimental.pallas import tpu as pltpu
from jax.sharding import PartitionSpec as P

QK_NOPE = 64
QK_ROPE = 32
V_DIM = 64
CONV_W = 1024
SEG = 64
QK_DIM = 96
Q_LAT = 768
KV_LAT = 512
ROWS = 256
TAPS = 31
HALO = 32
LANES = 128
N_FS = 4
N_TP = 8
N_SP = 16
BUNDLE = 4

epsilon = 1e-06
rope_base = 10000.0
masked_score = -1e30
log2_e = 1.4426950408889634
bf16 = jnp.bfloat16
f32 = jnp.float32

CORE_PAIRS = [(i, i ^ 1) for i in range(N_TP)]


def call(kernel, out_shape, scratch=(), scalars=0, arrays=0, specs=None, outs=None):
    extra = {"out_specs": outs} if outs else {}
    if scalars:
        smem = pl.BlockSpec(memory_space=pltpu.SMEM)
        specs = [smem] * scalars + [pl.BlockSpec(memory_space=pltpu.VMEM)] * arrays
    if specs:
        extra["in_specs"] = specs
    return pl.pallas_call(
        kernel,
        out_shape=out_shape,
        scratch_shapes=list(scratch),
        compiler_params=pltpu.CompilerParams(vmem_limit_bytes=16 * 1024 * 1024),
        **extra,
    )


def head_tile(tile, gain, cosine, sine_up, sine_down):
    scale = lax.rsqrt(jnp.sum(tile * tile, axis=-1, keepdims=True) * (1.0 / QK_DIM) + epsilon)
    tile = tile * scale * gain
    half = QK_ROPE // 2
    return (
        tile * cosine
        + pltpu.roll(tile, LANES - half, 1) * sine_up
        + pltpu.roll(tile, half, 1) * sine_down
    )


def copy_all(pairs, sems):
    copies = [
        pltpu.make_async_copy(source, target, sems.at[n]) for n, (source, target) in enumerate(pairs)
    ]
    for copy in copies:
        copy.start()
    for copy in copies:
        copy.wait()


def pack_kernel(qd_ref, md_ref, ku_ref, vu_ref, rope_ref, gain_ref, ho_ref, co_ref, narrow_ref, rope_out, gain_out, outw_ref, sems):
    pairs = [
        (qd_ref, narrow_ref.at[:96, :]),
        (md_ref, narrow_ref.at[96:160, :]),
        (rope_ref, rope_out),
        (gain_ref, gain_out),
        (ho_ref, outw_ref.at[:128, :]),
        (co_ref, outw_ref.at[128:, :]),
    ]
    for n, ref in enumerate((ku_ref, vu_ref)):
        for b in range(2):
            at = (2 * n + b) * LANES
            pairs.append((ref.at[b * 64 : (b + 1) * 64, :], narrow_ref.at[160:, at : at + LANES]))
    copy_all(pairs, sems)


def pack_rest_kernel(qu_ref, cv_ref, cg_ref, first_ref, second_ref, qu_scr, sems):
    pairs = [(qu_ref, qu_scr)]
    for ref, out in ((cv_ref, first_ref), (cg_ref, second_ref)):
        for b in range(4):
            rows = slice(b * 128, (b + 1) * 128)
            pairs.append((ref.at[rows, :], out.at[:128, rows]))
    copy_all(pairs, sems)
    first_ref[128:, :] = jnp.zeros((96, 512), bf16)
    for half in range(2):
        for h in range(2):
            at = half * 256 + h * LANES
            first_ref[128:, at : at + QK_DIM] = qu_scr[
                half * 96 : (half + 1) * 96, h * QK_DIM : (h + 1) * QK_DIM
            ]


def project_kernel(tok_ref, gain_ref, rope_w_ref, cos_ref, sin_ref, w_ref, lat_ref, rope_ref, normed_ref, cosine_ref, up_ref, down_ref, tok_scr, sems):
    block = 64
    copies = []
    for n in range(ROWS // block):
        rows = slice(n * block, (n + 1) * block)
        copies.append(
            pltpu.make_async_copy(tok_ref.at[rows, :], tok_scr.at[rows, :], sems.at[n])
        )
        copies[-1].start()
    turned = (((1,), (1,)), ((), ()))
    for r in range(0, ROWS, block):
        copies[r // block].wait()
        rows = tok_scr[r : r + block, :].astype(f32)
        scale = lax.rsqrt(jnp.mean(rows * rows, axis=-1, keepdims=True) + epsilon)
        normed_ref[r : r + block, :] = (rows * scale * gain_ref[...]).astype(bf16)
    both = jnp.zeros((ROWS, 160), f32)
    for f in range(N_FS):
        both = both + lax.dot_general(
            normed_ref[:, f * 512 : (f + 1) * 512],
            w_ref[f, :160, :],
            turned,
            preferred_element_type=f32,
        )
    both = both.astype(bf16)
    lat_ref[:ROWS, :] = both[:, :LANES]
    for r in range(4):
        lat_ref[ROWS:, r * 32 : (r + 1) * 32] = both[r * 64 : (r + 1) * 64, LANES:]
    rope = lax.dot_general(normed_ref[...], rope_w_ref[...], turned, preferred_element_type=f32)
    rope_ref[...] = jnp.zeros((ROWS, LANES), bf16)
    rope_ref[:, QK_NOPE:QK_DIM] = rope.astype(bf16)
    half = QK_ROPE // 2
    empty = jnp.zeros((ROWS, LANES - half), f32)
    cosine = jnp.concatenate([cos_ref[...].T, empty], axis=1)
    sine = jnp.concatenate([sin_ref[...].T, empty], axis=1)
    lane = lax.broadcasted_iota(jnp.int32, (ROWS, LANES), 1)
    cosine = pltpu.roll(cosine, QK_NOPE, 1) + pltpu.roll(cosine, QK_NOPE + half, 1)
    cosine_ref[...] = jnp.where(lane < QK_NOPE, 1.0, cosine)
    up_ref[...] = -pltpu.roll(sine, QK_NOPE, 1)
    down_ref[...] = pltpu.roll(sine, QK_NOPE + half, 1)


def keys_values_kernel(lat_ref, rope_ref, w_ref, mgain_ref, kgain_ref, cos_ref, up_ref, down_ref, out_ref, m_scr, w_scr):
    for g in range(N_TP):
        at = g * 64
        m_scr[:, at : at + 32] = lat_ref[g, :ROWS, 96:]
        for r in range(4):
            m_scr[r * 64 : (r + 1) * 64, at + 32 : at + 64] = lat_ref[
                g, ROWS:, r * 32 : (r + 1) * 32
            ]
    raw = m_scr[...].astype(f32)
    scale = lax.rsqrt(jnp.mean(raw * raw, axis=-1, keepdims=True) + epsilon)
    m_scr[...] = (raw * scale * mgain_ref[...]).astype(bf16)
    for f in range(N_FS):
        for n in range(2):
            for b in range(2):
                lanes = (2 * n + b) * LANES
                row = f * 128 + b * 64
                w_scr[row : row + 64, n * LANES : (n + 1) * LANES] = w_ref[
                    f, 160:, lanes : lanes + LANES
                ]
    both = jnp.dot(m_scr[...], w_scr[...], preferred_element_type=f32)
    nope = both[:, :LANES]
    lane = lax.broadcasted_iota(jnp.int32, (ROWS, LANES), 1)
    rope = rope_ref[...].astype(f32)
    tiles = []
    for h in range(2):
        part = nope if h == 0 else pltpu.roll(nope, 64, 1)
        tile = jnp.where(lane < QK_NOPE, part, rope)
        tiles.append(head_tile(tile, kgain_ref[...], cos_ref[...], up_ref[...], down_ref[...]))
    for h in range(2):
        out_ref[h * ROWS : (h + 1) * ROWS, :] = tiles[h].astype(bf16)
    values = both[:, LANES:].T.astype(bf16)
    for half in range(2):
        at = 2 * ROWS + half * LANES
        out_ref[at : at + LANES, :] = values[:, half * LANES : (half + 1) * LANES]


def queries_kernel(lat_ref, w_ref, lgain_ref, qgain_ref, cos_ref, up_ref, down_ref, out_ref, q_scr):
    for g in range(N_TP):
        q_scr[:, g * 96 : (g + 1) * 96] = lat_ref[g, :ROWS, :96]
    raw = q_scr[...].astype(f32)
    scale = lax.rsqrt(jnp.mean(raw * raw, axis=-1, keepdims=True) + epsilon)
    q_scr[...] = (raw * scale * lgain_ref[...]).astype(bf16)
    both = jnp.zeros((ROWS, 2 * LANES), f32)
    for f in range(N_FS):
        for half in range(2):
            at = f * 192 + half * 96
            both = both + jnp.dot(
                q_scr[:, at : at + 96],
                w_ref[f, 128:, half * 256 : (half + 1) * 256],
                preferred_element_type=f32,
            )
    lane = lax.broadcasted_iota(jnp.int32, (ROWS, LANES), 1)
    tiles = [
        head_tile(
            both[:, h * LANES : (h + 1) * LANES],
            qgain_ref[...],
            cos_ref[...],
            up_ref[...],
            down_ref[...],
        )
        for h in range(2)
    ]
    for h in range(2):
        out_ref[:, h * LANES : (h + 1) * LANES] = tiles[h].astype(bf16)


def gated_kernel(normed_ref, value_ref, gate_ref, out_ref):
    value = jnp.zeros((ROWS, LANES), f32)
    gate = jnp.zeros((ROWS, LANES), f32)
    for f in range(N_FS):
        for b in range(4):
            rows = normed_ref[:, f * 512 + b * LANES : f * 512 + (b + 1) * LANES]
            cols = slice(b * LANES, (b + 1) * LANES)
            value = value + jnp.dot(rows, value_ref[f, :128, cols], preferred_element_type=f32)
            gate = gate + jnp.dot(rows, gate_ref[f, :128, cols], preferred_element_type=f32)
    out_ref[...] = (value * jax.nn.sigmoid(gate)).astype(bf16)


def conv_kernel_body(halo_ref, gated_ref, taps_ref, gain_ref, shift_ref, out_ref, ext_scr, stat_scr):
    ext_scr[:HALO, :] = halo_ref[...].astype(f32)
    ext_scr[HALO:, :] = gated_ref[...].astype(f32)
    start = HALO - (TAPS - 1)
    block = LANES
    stat_scr[...] = jnp.zeros((16, LANES), f32)
    for n in range(ROWS // block):
        r = n * block
        running = jnp.zeros((block, LANES), f32)
        for j in range(TAPS):
            running = running + ext_scr[pl.ds(r + start + j, block), :] * taps_ref[j : j + 1, :]
        flat = running.T
        mean = jnp.sum(flat, axis=0, keepdims=True) * (1.0 / LANES)
        off = flat - mean
        stat_scr[n : n + 1, :] = mean
        stat_scr[2 + n : 3 + n, :] = jnp.sum(off * off, axis=0, keepdims=True)
        out_ref[r : r + block, :] = off.T.astype(bf16)
    stat_scr[4:5, :] = gain_ref[...]
    stat_scr[5:6, :] = shift_ref[...]
    left = stat_scr[...]
    for part in range(3):
        rounded = left.astype(bf16)
        out_ref[ROWS + part * 16 : ROWS + (part + 1) * 16, :] = rounded
        left = left - rounded.astype(f32)


def channel_kernel(in_ref, out_ref):
    stats = []
    for g in range(N_TP):
        parts = [
            in_ref[g, ROWS + part * 16 : ROWS + (part + 1) * 16, :].astype(f32) for part in range(3)
        ]
        stats.append(parts[0] + (parts[1] + parts[2]))
    for n in range(ROWS // LANES):
        means = [st[n : n + 1] for st in stats]
        mean = means[0]
        for g in range(1, N_TP):
            mean = mean + means[g]
        mean = mean * (1.0 / N_TP)
        spread = jnp.zeros((1, LANES), f32)
        for g in range(N_TP):
            apart = means[g] - mean
            spread = spread + stats[g][2 + n : 3 + n] + LANES * apart * apart
        scale = lax.rsqrt(spread * (1.0 / CONV_W) + epsilon)
        columns = jnp.concatenate(
            [m - mean for m in means] + [scale] + [jnp.zeros((7, LANES), f32)], axis=0
        ).T
        rows = slice(n * LANES, (n + 1) * LANES)
        for g in range(N_TP):
            value = in_ref[g, rows, :].astype(f32) + columns[:, g : g + 1]
            value = value * columns[:, N_TP : N_TP + 1] * stats[g][4:5] + stats[g][5:6]
            out_ref[g, rows, :] = (value / (1.0 + jnp.exp(-value))).astype(bf16)


def attend(q_ref, blocks, state, hidden, mask=None):
    rate = QK_DIM ** (-0.5) * log2_e
    fresh = []
    for h in range(2):
        top, total, weighted = state[h]
        keys = jnp.concatenate([b[h * ROWS : (h + 1) * ROWS, :] for b in blocks], axis=0)
        scores = lax.dot_general(
            keys,
            q_ref[:, h * LANES : (h + 1) * LANES],
            (((1,), (1,)), ((), ())),
            preferred_element_type=f32,
        )
        if mask is not None:
            scores = jnp.where(mask, scores, masked_score)
        new_top = top
        for n, off in enumerate(hidden):
            part = jnp.max(scores[n * ROWS : (n + 1) * ROWS], axis=0, keepdims=True)
            new_top = jnp.maximum(new_top, part - off)
        weights = jnp.concatenate(
            [
                jnp.exp2(scores[n * ROWS : (n + 1) * ROWS] * rate - (new_top * rate + off))
                for n, off in enumerate(hidden)
            ],
            axis=0,
        )
        factor = jnp.exp2((top - new_top) * rate)
        total = total * factor + jnp.sum(weights, axis=0, keepdims=True)
        at = 2 * ROWS + h * V_DIM
        values = jnp.concatenate(
            [b[at + i * LANES : at + i * LANES + V_DIM, :] for b in blocks for i in range(2)],
            axis=1,
        )
        weighted = weighted * factor + jnp.dot(
            values, weights.astype(bf16), preferred_element_type=f32
        )
        fresh.append((new_top, total, weighted))
    return fresh


def own_kernel(q_ref, own_ref, stat_ref, acc_ref):
    key = lax.broadcasted_iota(jnp.int32, (ROWS, ROWS), 0)
    query = lax.broadcasted_iota(jnp.int32, (ROWS, ROWS), 1)
    mask = jnp.right_shift(key, 6) <= jnp.right_shift(query, 6)
    empty = (
        jnp.full((1, ROWS), masked_score, f32),
        jnp.zeros((1, ROWS), f32),
        jnp.zeros((V_DIM, ROWS), f32),
    )
    state = attend(q_ref, [own_ref], [empty, empty], [0.0], mask)
    stat_ref[4:, :] = jnp.zeros((4, ROWS), f32)
    for h in range(2):
        stat_ref[2 * h : 2 * h + 1, :] = state[h][0]
        stat_ref[2 * h + 1 : 2 * h + 2, :] = state[h][1]
        acc_ref[h * V_DIM : (h + 1) * V_DIM, :] = state[h][2]


def attention_kernel(at_ref, q_ref, kv_ref, stat_ref, acc_ref, *rest):
    pieces, (out_ref, weight_ref, kv, sems, weight_sems) = rest[:N_TP], rest[N_TP:]
    at = at_ref[0]
    copies = [
        pltpu.make_async_copy(kv_ref.at[n], kv.at[n], sems.at[n]) for n in range(N_SP // BUNDLE)
    ]
    for copy in copies:
        copy.start()
    fetched = [
        pltpu.make_async_copy(piece.at[:, :128, :], weight_ref.at[n], weight_sems.at[n])
        for n, piece in enumerate(pieces)
    ]
    for copy in fetched:
        copy.start()
    state = [
        (
            stat_ref[2 * h : 2 * h + 1, :],
            stat_ref[2 * h + 1 : 2 * h + 2, :],
            acc_ref[h * V_DIM : (h + 1) * V_DIM, :],
        )
        for h in range(2)
    ]
    for n, copy in enumerate(copies):
        copy.wait()
        hidden = [jnp.where(n * BUNDLE + i < at, 0.0, -masked_score) for i in range(BUNDLE)]
        blocks = [kv.at[n, i] for i in range(BUNDLE)]
        state = lax.cond(
            n * BUNDLE < at,
            lambda s, blocks=blocks, hidden=hidden: attend(q_ref, blocks, s, hidden),
            lambda s: s,
            state,
        )
    result = jnp.concatenate([state[h][2] / state[h][1] for h in range(2)], axis=0)
    out_ref[...] = result.T.astype(bf16)
    for copy in fetched:
        copy.wait()


def sources(g):
    other = g + 1 - 2 * lax.rem(g, 2)
    return [lax.rem(first + N_TP - s, N_TP) for first in (g, other) for s in (0, 2, 4, 6)]


def conv_part_kernel(tp_ref, conv_ref, *rest):
    pieces, (out_ref, weights, sems) = rest[:N_TP], rest[N_TP:]
    fetched = [
        pltpu.make_async_copy(piece.at[:, 128:, :], weights.at[n], sems.at[n])
        for n, piece in enumerate(pieces)
    ]
    for copy in fetched:
        copy.start()
    for n, g in enumerate(sources(tp_ref[0])):
        fetched[n].wait()
        left = conv_ref[g]
        for f in range(N_FS):
            cols = slice(f * 512, (f + 1) * 512)
            part = jnp.dot(left, weights[n, f], preferred_element_type=f32)
            out_ref[:, cols] = part if n == 0 else out_ref[:, cols] + part


def output_kernel(tp_ref, base_ref, attn_ref, weight_ref, out_ref):
    owners = sources(tp_ref[0])
    left = jnp.concatenate([attn_ref[g] for g in owners], axis=1)
    for f in range(N_FS):
        cols = slice(f * 512, (f + 1) * 512)
        weight = jnp.concatenate([weight_ref[n, f] for n in range(N_TP)], axis=0)
        total = base_ref[:, cols] + jnp.dot(left, weight, preferred_element_type=f32)
        out_ref[:, cols] = total.astype(bf16)


def rotation_tables(positions):
    inverse_freq = 1.0 / rope_base ** (jnp.arange(0, QK_ROPE, 2, dtype=f32) / QK_ROPE)
    angles = positions.astype(f32)[None, :] * inverse_freq[:, None]
    return jnp.cos(angles), jnp.sin(angles)


def local(
    tokens,
    mix_gain,
    query_down,
    memory_down,
    rope_weight,
    query_up,
    key_up,
    value_up,
    latent_gain,
    memory_gain,
    query_gain,
    key_gain,
    conv_value,
    conv_gate,
    conv_kernel,
    channel_gain,
    channel_shift,
    heads_out,
    conv_out,
):
    at = lax.axis_index("sp")
    hbm = pl.BlockSpec(memory_space=pltpu.HBM)
    vmem = pl.BlockSpec(memory_space=pltpu.VMEM)
    def kept(*arrays):
        return [pltpu.with_memory_space_constraint(a, pltpu.HBM) for a in arrays]

    narrow, rope_w, gain, outw = call(
        pack_kernel,
        (
            jax.ShapeDtypeStruct((224, 512), bf16),
            jax.ShapeDtypeStruct((QK_ROPE, 2048), bf16),
            jax.ShapeDtypeStruct((1, 2048), f32),
            jax.ShapeDtypeStruct((256, 512), bf16),
        ),
        [pltpu.SemaphoreType.DMA((10,))],
        specs=[hbm] * 8,
    )(
        *kept(
            query_down.T, memory_down.T, key_up, value_up, rope_weight.T, mix_gain[None, :],
            heads_out, conv_out,
        )
    )
    out_all = lax.all_gather(outw, "fs")
    narrow_all = lax.all_gather(narrow, "fs")
    positions = at * ROWS + jnp.arange(ROWS, dtype=jnp.int32)
    cosine, sine = rotation_tables(positions)
    table = jax.ShapeDtypeStruct((ROWS, LANES), f32)
    latents, rope_rows, normed, cosine, sine_up, sine_down = call(
        project_kernel,
        (
            jax.ShapeDtypeStruct((320, LANES), bf16),
            jax.ShapeDtypeStruct((ROWS, LANES), bf16),
            jax.ShapeDtypeStruct((ROWS, 2048), bf16),
            table,
            table,
            table,
        ),
        [pltpu.VMEM((ROWS, 2048), bf16), pltpu.SemaphoreType.DMA((4,))],
        specs=[hbm] + [vmem] * 5,
    )(pltpu.with_memory_space_constraint(tokens[0], pltpu.HBM), gain, rope_w, cosine, sine, narrow_all)
    latents = lax.all_gather(latents, "tp")

    def row(vector, width):
        return jnp.pad(vector, (0, width - vector.shape[0]))[None, :]

    own = call(
        keys_values_kernel,
        jax.ShapeDtypeStruct((6 * LANES, LANES), bf16),
        [pltpu.VMEM((ROWS, KV_LAT), bf16), pltpu.VMEM((KV_LAT, 256), bf16)],
    )(
        latents, rope_rows, narrow_all, memory_gain[None, :], row(key_gain, LANES),
        cosine, sine_up, sine_down,
    )
    tp, at = lax.axis_index("tp")[None], at[None]
    own, out_all, tp, at, *rest = lax.optimization_barrier(
        (own, out_all, tp, at, query_up, conv_value, conv_gate)
    )
    pieces = lax.all_gather(own, "sp")
    far = [
        lax.ppermute(out_all, "tp", [(i, (i + by) % N_TP) for i in range(N_TP)]) for by in (4, 2, 6)
    ]
    far = [far[1], far[0], far[2]]
    near = lax.ppermute(out_all, "tp", CORE_PAIRS)
    packed = call(
        pack_rest_kernel,
        tuple(jax.ShapeDtypeStruct((rows, 512), bf16) for rows in (224, 128)),
        [pltpu.VMEM((192, 192), bf16), pltpu.SemaphoreType.DMA((9,))],
        specs=[hbm] * 3,
    )(*kept(*rest))
    first_all, second_all = (lax.all_gather(p, "fs") for p in packed)
    queries = call(
        queries_kernel,
        jax.ShapeDtypeStruct((ROWS, 2 * LANES), bf16),
        [pltpu.VMEM((ROWS, Q_LAT), bf16)],
    )(
        latents, first_all, latent_gain[None, :], row(query_gain, LANES),
        cosine, sine_up, sine_down,
    )
    gated = call(gated_kernel, jax.ShapeDtypeStruct((ROWS, LANES), bf16))(normed, first_all, second_all)
    halo = lax.ppermute(gated[ROWS - HALO :], "sp", [(i, i + 1) for i in range(N_SP - 1)])
    taps = jnp.pad(conv_kernel.astype(f32), ((0, 1), (0, 0)))
    conv_sum = call(
        conv_kernel_body,
        jax.ShapeDtypeStruct((ROWS + 48, LANES), bf16),
        [pltpu.VMEM((ROWS + HALO, LANES), f32), pltpu.VMEM((16, LANES), f32)],
    )(halo, gated, taps, channel_gain[None, :], channel_shift[None, :])
    conv_sum = lax.all_gather(conv_sum, "tp")
    conv_sum, near, *far = lax.optimization_barrier((conv_sum, near, *far))
    crossed = [lax.ppermute(w, "tp", CORE_PAIRS) for w in far]
    weights = kept(out_all, *far, near, *crossed)
    half = (N_TP, N_FS, 128, 512)
    conv_result = call(channel_kernel, jax.ShapeDtypeStruct((N_TP, ROWS, LANES), bf16))(conv_sum)
    base = call(
        conv_part_kernel,
        jax.ShapeDtypeStruct((ROWS, 2048), f32),
        [pltpu.VMEM(half, bf16), pltpu.SemaphoreType.DMA((N_TP,))],
        specs=[pl.BlockSpec(memory_space=pltpu.SMEM), vmem] + [hbm] * N_TP,
    )(tp, conv_result, *weights)
    stat, acc = call(
        own_kernel,
        (jax.ShapeDtypeStruct((8, ROWS), f32), jax.ShapeDtypeStruct((2 * V_DIM, ROWS), f32)),
    )(queries, own)
    pieces, base, stat, acc = lax.optimization_barrier((pieces, base, stat, acc))
    pieces = pltpu.with_memory_space_constraint(
        pieces.reshape(N_SP // BUNDLE, BUNDLE, 6 * LANES, LANES), pltpu.HBM
    )
    attention, weights = call(
        attention_kernel,
        (jax.ShapeDtypeStruct((ROWS, LANES), bf16), jax.ShapeDtypeStruct(half, bf16)),
        [
            pltpu.VMEM((N_SP // BUNDLE, BUNDLE, 6 * LANES, LANES), bf16),
            pltpu.SemaphoreType.DMA((N_SP // BUNDLE,)),
            pltpu.SemaphoreType.DMA((N_TP,)),
        ],
        specs=[pl.BlockSpec(memory_space=pltpu.SMEM), vmem, hbm, vmem, vmem] + [hbm] * N_TP,
    )(at, queries, pieces, stat, acc, *weights)
    attention = lax.all_gather(attention, "tp")
    mixed = call(
        output_kernel, jax.ShapeDtypeStruct((ROWS, 2048), bf16), scalars=1, arrays=3
    )(tp, base, attention, weights)
    return mixed[None]


def solution(mesh):
    in_specs = (
        P("fs", "sp", None),
        P(),
        P("fs", "tp"),
        P("fs", "tp"),
        P(),
        P("fs", "tp"),
        P("fs", "tp"),
        P("fs", "tp"),
        P(),
        P(),
        P(),
        P(),
        P("fs", "tp"),
        P("fs", "tp"),
        P(None, "tp"),
        P("tp"),
        P("tp"),
        P("tp", "fs"),
        P("tp", "fs"),
    )
    out_specs = P("fs", "sp", None)
    return jax.shard_map(local, mesh=mesh, in_specs=in_specs, out_specs=out_specs, check_vma=False)
```

```python
import jax
import jax.numpy as jnp
from jax import lax
from jax.experimental import pallas as pl
from jax.experimental.pallas import tpu as pltpu
from jax.sharding import PartitionSpec as P

QK_NOPE = 64
QK_ROPE = 32
V_DIM = 64
CONV_W = 1024
SEG = 64
QK_DIM = 96
Q_LAT = 768
KV_LAT = 512
ROWS = 256
TAPS = 31
HALO = 32
LANES = 128
N_FS = 4
N_TP = 8
N_SP = 16
BUNDLE = 4

epsilon = 1e-06
rope_base = 10000.0
masked_score = -1e30
log2_e = 1.4426950408889634
bf16 = jnp.bfloat16
f32 = jnp.float32

CORE_PAIRS = [(i, i ^ 1) for i in range(N_TP)]


def call(kernel, out_shape, scratch=(), scalars=0, arrays=0, specs=None, outs=None):
    extra = {"out_specs": outs} if outs else {}
    if scalars:
        smem = pl.BlockSpec(memory_space=pltpu.SMEM)
        specs = [smem] * scalars + [pl.BlockSpec(memory_space=pltpu.VMEM)] * arrays
    if specs:
        extra["in_specs"] = specs
    return pl.pallas_call(
        kernel,
        out_shape=out_shape,
        scratch_shapes=list(scratch),
        compiler_params=pltpu.CompilerParams(vmem_limit_bytes=16 * 1024 * 1024),
        **extra,
    )


def head_tile(tile, gain, cosine, sine_up, sine_down):
    scale = lax.rsqrt(jnp.sum(tile * tile, axis=-1, keepdims=True) * (1.0 / QK_DIM) + epsilon)
    tile = tile * scale * gain
    half = QK_ROPE // 2
    return (
        tile * cosine
        + pltpu.roll(tile, LANES - half, 1) * sine_up
        + pltpu.roll(tile, half, 1) * sine_down
    )


def copy_all(pairs, sems):
    copies = [
        pltpu.make_async_copy(source, target, sems.at[n]) for n, (source, target) in enumerate(pairs)
    ]
    for copy in copies:
        copy.start()
    for copy in copies:
        copy.wait()


def pack_kernel(qd_ref, md_ref, ku_ref, vu_ref, rope_ref, gain_ref, ho_ref, co_ref, qu_ref, cg_ref, narrow_ref, rope_out, gain_out, outw_ref, qu_scr, sems):
    pairs = [
        (qd_ref, narrow_ref.at[:96, :]),
        (md_ref, narrow_ref.at[96:160, :]),
        (rope_ref, rope_out),
        (gain_ref, gain_out),
        (ho_ref, outw_ref.at[:128, :]),
        (co_ref, outw_ref.at[128:256, :]),
        (qu_ref, qu_scr),
    ]
    for n, ref in enumerate((ku_ref, vu_ref)):
        for b in range(2):
            at = (2 * n + b) * LANES
            pairs.append(
                (ref.at[b * 64 : (b + 1) * 64, :], narrow_ref.at[160:224, at : at + LANES])
            )
    for b in range(4):
        rows = slice(b * 128 + 112, (b + 1) * 128)
        pairs.append((cg_ref.at[rows, :], narrow_ref.at[224:, b * 128 : (b + 1) * 128]))
    copy_all(pairs, sems)
    outw_ref[256:, :] = jnp.zeros((96, 512), bf16)
    for half in range(2):
        for h in range(2):
            at = half * 256 + h * LANES
            outw_ref[256:, at : at + QK_DIM] = qu_scr[
                half * 96 : (half + 1) * 96, h * QK_DIM : (h + 1) * QK_DIM
            ]


def pack_rest_kernel(cv_ref, cg_ref, out_ref, sems):
    pairs = []
    for b in range(4):
        cols = slice(b * 128, (b + 1) * 128)
        pairs.append((cv_ref.at[cols, :], out_ref.at[:128, cols]))
        pairs.append((cg_ref.at[b * 128 : b * 128 + 112, :], out_ref.at[128:, cols]))
    copy_all(pairs, sems)


def project_kernel(tok_ref, gain_ref, rope_w_ref, cos_ref, sin_ref, w_ref, lat_ref, rope_ref, normed_ref, cosine_ref, up_ref, down_ref, tok_scr, sems):
    block = 64
    copies = []
    for n in range(ROWS // block):
        rows = slice(n * block, (n + 1) * block)
        copies.append(
            pltpu.make_async_copy(tok_ref.at[rows, :], tok_scr.at[rows, :], sems.at[n])
        )
        copies[-1].start()
    turned = (((1,), (1,)), ((), ()))
    for r in range(0, ROWS, block):
        copies[r // block].wait()
        rows = tok_scr[r : r + block, :].astype(f32)
        scale = lax.rsqrt(jnp.mean(rows * rows, axis=-1, keepdims=True) + epsilon)
        normed_ref[r : r + block, :] = (rows * scale * gain_ref[...]).astype(bf16)
    both = jnp.zeros((ROWS, 160), f32)
    for f in range(N_FS):
        both = both + lax.dot_general(
            normed_ref[:, f * 512 : (f + 1) * 512],
            w_ref[f, :160, :],
            turned,
            preferred_element_type=f32,
        )
    both = both.astype(bf16)
    lat_ref[:ROWS, :] = both[:, :LANES]
    for r in range(4):
        lat_ref[ROWS:, r * 32 : (r + 1) * 32] = both[r * 64 : (r + 1) * 64, LANES:]
    rope = lax.dot_general(normed_ref[...], rope_w_ref[...], turned, preferred_element_type=f32)
    rope_ref[...] = jnp.zeros((ROWS, LANES), bf16)
    rope_ref[:, QK_NOPE:QK_DIM] = rope.astype(bf16)
    half = QK_ROPE // 2
    empty = jnp.zeros((ROWS, LANES - half), f32)
    cosine = jnp.concatenate([cos_ref[...].T, empty], axis=1)
    sine = jnp.concatenate([sin_ref[...].T, empty], axis=1)
    lane = lax.broadcasted_iota(jnp.int32, (ROWS, LANES), 1)
    cosine = pltpu.roll(cosine, QK_NOPE, 1) + pltpu.roll(cosine, QK_NOPE + half, 1)
    cosine_ref[...] = jnp.where(lane < QK_NOPE, 1.0, cosine)
    up_ref[...] = -pltpu.roll(sine, QK_NOPE, 1)
    down_ref[...] = pltpu.roll(sine, QK_NOPE + half, 1)


def keys_values_kernel(lat_ref, rope_ref, w_ref, mgain_ref, kgain_ref, cos_ref, up_ref, down_ref, out_ref, m_scr, w_scr):
    for g in range(N_TP):
        at = g * 64
        m_scr[:, at : at + 32] = lat_ref[g, :ROWS, 96:]
        for r in range(4):
            m_scr[r * 64 : (r + 1) * 64, at + 32 : at + 64] = lat_ref[
                g, ROWS:, r * 32 : (r + 1) * 32
            ]
    raw = m_scr[...].astype(f32)
    scale = lax.rsqrt(jnp.mean(raw * raw, axis=-1, keepdims=True) + epsilon)
    m_scr[...] = (raw * scale * mgain_ref[...]).astype(bf16)
    for f in range(N_FS):
        for n in range(2):
            for b in range(2):
                lanes = (2 * n + b) * LANES
                row = f * 128 + b * 64
                w_scr[row : row + 64, n * LANES : (n + 1) * LANES] = w_ref[
                    f, 160:224, lanes : lanes + LANES
                ]
    both = jnp.dot(m_scr[...], w_scr[...], preferred_element_type=f32)
    nope = both[:, :LANES]
    lane = lax.broadcasted_iota(jnp.int32, (ROWS, LANES), 1)
    rope = rope_ref[...].astype(f32)
    tiles = []
    for h in range(2):
        part = nope if h == 0 else pltpu.roll(nope, 64, 1)
        tile = jnp.where(lane < QK_NOPE, part, rope)
        tiles.append(head_tile(tile, kgain_ref[...], cos_ref[...], up_ref[...], down_ref[...]))
    for h in range(2):
        out_ref[h * ROWS : (h + 1) * ROWS, :] = tiles[h].astype(bf16)
    values = both[:, LANES:].T.astype(bf16)
    for half in range(2):
        at = 2 * ROWS + half * LANES
        out_ref[at : at + LANES, :] = values[:, half * LANES : (half + 1) * LANES]


def queries_kernel(lat_ref, w_hbm, lgain_ref, qgain_ref, cos_ref, up_ref, down_ref, out_ref, q_scr, w_ref, sem):
    copy = pltpu.make_async_copy(w_hbm.at[:, 256:, :], w_ref, sem)
    copy.start()
    for g in range(N_TP):
        q_scr[:, g * 96 : (g + 1) * 96] = lat_ref[g, :ROWS, :96]
    raw = q_scr[...].astype(f32)
    scale = lax.rsqrt(jnp.mean(raw * raw, axis=-1, keepdims=True) + epsilon)
    q_scr[...] = (raw * scale * lgain_ref[...]).astype(bf16)
    both = jnp.zeros((ROWS, 2 * LANES), f32)
    copy.wait()
    for f in range(N_FS):
        for half in range(2):
            at = f * 192 + half * 96
            both = both + jnp.dot(
                q_scr[:, at : at + 96],
                w_ref[f, :, half * 256 : (half + 1) * 256],
                preferred_element_type=f32,
            )
    lane = lax.broadcasted_iota(jnp.int32, (ROWS, LANES), 1)
    tiles = [
        head_tile(
            both[:, h * LANES : (h + 1) * LANES],
            qgain_ref[...],
            cos_ref[...],
            up_ref[...],
            down_ref[...],
        )
        for h in range(2)
    ]
    for h in range(2):
        out_ref[:, h * LANES : (h + 1) * LANES] = tiles[h].astype(bf16)


def gated_kernel(normed_ref, w_ref, narrow_ref, out_ref):
    value = jnp.zeros((ROWS, LANES), f32)
    gate = jnp.zeros((ROWS, LANES), f32)
    for f in range(N_FS):
        for b in range(4):
            rows = normed_ref[:, f * 512 + b * LANES : f * 512 + (b + 1) * LANES]
            cols = slice(b * LANES, (b + 1) * LANES)
            weight = jnp.concatenate([w_ref[f, 128:, cols], narrow_ref[f, 224:, cols]], axis=0)
            value = value + jnp.dot(rows, w_ref[f, :128, cols], preferred_element_type=f32)
            gate = gate + jnp.dot(rows, weight, preferred_element_type=f32)
    out_ref[...] = (value * jax.nn.sigmoid(gate)).astype(bf16)


def conv_kernel_body(halo_ref, gated_ref, taps_ref, gain_ref, shift_ref, out_ref, ext_scr, stat_scr):
    ext_scr[:HALO, :] = halo_ref[...].astype(f32)
    ext_scr[HALO:, :] = gated_ref[...].astype(f32)
    start = HALO - (TAPS - 1)
    block = LANES
    stat_scr[...] = jnp.zeros((16, LANES), f32)
    for n in range(ROWS // block):
        r = n * block
        running = jnp.zeros((block, LANES), f32)
        for j in range(TAPS):
            running = running + ext_scr[pl.ds(r + start + j, block), :] * taps_ref[j : j + 1, :]
        flat = running.T
        mean = jnp.sum(flat, axis=0, keepdims=True) * (1.0 / LANES)
        off = flat - mean
        stat_scr[n : n + 1, :] = mean
        stat_scr[2 + n : 3 + n, :] = jnp.sum(off * off, axis=0, keepdims=True)
        out_ref[r : r + block, :] = off.T.astype(bf16)
    stat_scr[4:5, :] = gain_ref[...]
    stat_scr[5:6, :] = shift_ref[...]
    left = stat_scr[...]
    for part in range(3):
        rounded = left.astype(bf16)
        out_ref[ROWS + part * 16 : ROWS + (part + 1) * 16, :] = rounded
        left = left - rounded.astype(f32)


def channel_kernel(in_ref, out_ref):
    stats = []
    for g in range(N_TP):
        parts = [
            in_ref[g, ROWS + part * 16 : ROWS + (part + 1) * 16, :].astype(f32) for part in range(3)
        ]
        stats.append(parts[0] + (parts[1] + parts[2]))
    for n in range(ROWS // LANES):
        means = [st[n : n + 1] for st in stats]
        mean = means[0]
        for g in range(1, N_TP):
            mean = mean + means[g]
        mean = mean * (1.0 / N_TP)
        spread = jnp.zeros((1, LANES), f32)
        for g in range(N_TP):
            apart = means[g] - mean
            spread = spread + stats[g][2 + n : 3 + n] + LANES * apart * apart
        scale = lax.rsqrt(spread * (1.0 / CONV_W) + epsilon)
        columns = jnp.concatenate(
            [m - mean for m in means] + [scale] + [jnp.zeros((7, LANES), f32)], axis=0
        ).T
        rows = slice(n * LANES, (n + 1) * LANES)
        for g in range(N_TP):
            value = in_ref[g, rows, :].astype(f32) + columns[:, g : g + 1]
            value = value * columns[:, N_TP : N_TP + 1] * stats[g][4:5] + stats[g][5:6]
            out_ref[g, rows, :] = (value / (1.0 + jnp.exp(-value))).astype(bf16)


def attend(q_ref, blocks, state, hidden, mask=None):
    rate = QK_DIM ** (-0.5) * log2_e
    fresh = []
    for h in range(2):
        top, total, weighted = state[h]
        keys = jnp.concatenate([b[h * ROWS : (h + 1) * ROWS, :] for b in blocks], axis=0)
        scores = lax.dot_general(
            keys,
            q_ref[:, h * LANES : (h + 1) * LANES],
            (((1,), (1,)), ((), ())),
            preferred_element_type=f32,
        )
        if mask is not None:
            scores = jnp.where(mask, scores, masked_score)
        new_top = top
        for n, off in enumerate(hidden):
            part = jnp.max(scores[n * ROWS : (n + 1) * ROWS], axis=0, keepdims=True)
            new_top = jnp.maximum(new_top, part - off)
        weights = jnp.concatenate(
            [
                jnp.exp2(scores[n * ROWS : (n + 1) * ROWS] * rate - (new_top * rate + off))
                for n, off in enumerate(hidden)
            ],
            axis=0,
        )
        factor = jnp.exp2((top - new_top) * rate)
        total = total * factor + jnp.sum(weights, axis=0, keepdims=True)
        at = 2 * ROWS + h * V_DIM
        values = jnp.concatenate(
            [b[at + i * LANES : at + i * LANES + V_DIM, :] for b in blocks for i in range(2)],
            axis=1,
        )
        weighted = weighted * factor + jnp.dot(
            values, weights.astype(bf16), preferred_element_type=f32
        )
        fresh.append((new_top, total, weighted))
    return fresh


def own_kernel(q_ref, own_ref, stat_ref, acc_ref):
    key = lax.broadcasted_iota(jnp.int32, (ROWS, ROWS), 0)
    query = lax.broadcasted_iota(jnp.int32, (ROWS, ROWS), 1)
    mask = jnp.right_shift(key, 6) <= jnp.right_shift(query, 6)
    empty = (
        jnp.full((1, ROWS), masked_score, f32),
        jnp.zeros((1, ROWS), f32),
        jnp.zeros((V_DIM, ROWS), f32),
    )
    state = attend(q_ref, [own_ref], [empty, empty], [0.0], mask)
    stat_ref[4:, :] = jnp.zeros((4, ROWS), f32)
    for h in range(2):
        stat_ref[2 * h : 2 * h + 1, :] = state[h][0]
        stat_ref[2 * h + 1 : 2 * h + 2, :] = state[h][1]
        acc_ref[h * V_DIM : (h + 1) * V_DIM, :] = state[h][2]


def attention_kernel(at_ref, q_ref, kv_ref, stat_ref, acc_ref, *rest):
    pieces, (out_ref, weight_ref, kv, sems, weight_sems) = rest[:N_TP], rest[N_TP:]
    at = at_ref[0]
    copies = [
        pltpu.make_async_copy(kv_ref.at[n], kv.at[n], sems.at[n]) for n in range(N_SP // BUNDLE)
    ]
    for copy in copies:
        copy.start()
    fetched = [
        pltpu.make_async_copy(piece.at[:, :128, :], weight_ref.at[n], weight_sems.at[n])
        for n, piece in enumerate(pieces)
    ]
    for copy in fetched:
        copy.start()
    state = [
        (
            stat_ref[2 * h : 2 * h + 1, :],
            stat_ref[2 * h + 1 : 2 * h + 2, :],
            acc_ref[h * V_DIM : (h + 1) * V_DIM, :],
        )
        for h in range(2)
    ]
    for n, copy in enumerate(copies):
        copy.wait()
        hidden = [jnp.where(n * BUNDLE + i < at, 0.0, -masked_score) for i in range(BUNDLE)]
        blocks = [kv.at[n, i] for i in range(BUNDLE)]
        state = lax.cond(
            n * BUNDLE < at,
            lambda s, blocks=blocks, hidden=hidden: attend(q_ref, blocks, s, hidden),
            lambda s: s,
            state,
        )
    result = jnp.concatenate([state[h][2] / state[h][1] for h in range(2)], axis=0)
    out_ref[...] = result.T.astype(bf16)
    for copy in fetched:
        copy.wait()


def sources(g):
    other = g + 1 - 2 * lax.rem(g, 2)
    return [lax.rem(first + N_TP - s, N_TP) for first in (g, other) for s in (0, 2, 4, 6)]


def conv_part_kernel(tp_ref, conv_ref, *rest):
    pieces, (out_ref, weights, sems) = rest[:N_TP], rest[N_TP:]
    fetched = [
        pltpu.make_async_copy(piece.at[:, 128:256, :], weights.at[n], sems.at[n])
        for n, piece in enumerate(pieces)
    ]
    for copy in fetched:
        copy.start()
    for n, g in enumerate(sources(tp_ref[0])):
        fetched[n].wait()
        left = conv_ref[g]
        for f in range(N_FS):
            cols = slice(f * 512, (f + 1) * 512)
            part = jnp.dot(left, weights[n, f], preferred_element_type=f32)
            out_ref[:, cols] = part if n == 0 else out_ref[:, cols] + part


def output_kernel(tp_ref, base_ref, attn_ref, weight_ref, out_ref):
    owners = sources(tp_ref[0])
    left = jnp.concatenate([attn_ref[g] for g in owners], axis=1)
    for f in range(N_FS):
        cols = slice(f * 512, (f + 1) * 512)
        weight = jnp.concatenate([weight_ref[n, f] for n in range(N_TP)], axis=0)
        total = base_ref[:, cols] + jnp.dot(left, weight, preferred_element_type=f32)
        out_ref[:, cols] = total.astype(bf16)


def rotation_tables(positions):
    inverse_freq = 1.0 / rope_base ** (jnp.arange(0, QK_ROPE, 2, dtype=f32) / QK_ROPE)
    angles = positions.astype(f32)[None, :] * inverse_freq[:, None]
    return jnp.cos(angles), jnp.sin(angles)


def local(
    tokens,
    mix_gain,
    query_down,
    memory_down,
    rope_weight,
    query_up,
    key_up,
    value_up,
    latent_gain,
    memory_gain,
    query_gain,
    key_gain,
    conv_value,
    conv_gate,
    conv_kernel,
    channel_gain,
    channel_shift,
    heads_out,
    conv_out,
):
    at = lax.axis_index("sp")
    hbm = pl.BlockSpec(memory_space=pltpu.HBM)
    vmem = pl.BlockSpec(memory_space=pltpu.VMEM)
    def kept(*arrays):
        return [pltpu.with_memory_space_constraint(a, pltpu.HBM) for a in arrays]

    narrow, rope_w, gain, outw = call(
        pack_kernel,
        (
            jax.ShapeDtypeStruct((240, 512), bf16),
            jax.ShapeDtypeStruct((QK_ROPE, 2048), bf16),
            jax.ShapeDtypeStruct((1, 2048), f32),
            jax.ShapeDtypeStruct((352, 512), bf16),
        ),
        [pltpu.VMEM((192, 192), bf16), pltpu.SemaphoreType.DMA((15,))],
        specs=[hbm] * 10,
    )(
        *kept(
            query_down.T, memory_down.T, key_up, value_up, rope_weight.T, mix_gain[None, :],
            heads_out, conv_out, query_up, conv_gate,
        )
    )
    out_all = lax.all_gather(outw, "fs")
    narrow_all = lax.all_gather(narrow, "fs")
    positions = at * ROWS + jnp.arange(ROWS, dtype=jnp.int32)
    cosine, sine = rotation_tables(positions)
    table = jax.ShapeDtypeStruct((ROWS, LANES), f32)
    latents, rope_rows, normed, cosine, sine_up, sine_down = call(
        project_kernel,
        (
            jax.ShapeDtypeStruct((320, LANES), bf16),
            jax.ShapeDtypeStruct((ROWS, LANES), bf16),
            jax.ShapeDtypeStruct((ROWS, 2048), bf16),
            table,
            table,
            table,
        ),
        [pltpu.VMEM((ROWS, 2048), bf16), pltpu.SemaphoreType.DMA((4,))],
        specs=[hbm] + [vmem] * 5,
    )(pltpu.with_memory_space_constraint(tokens[0], pltpu.HBM), gain, rope_w, cosine, sine, narrow_all)
    latents = lax.all_gather(latents, "tp")

    def row(vector, width):
        return jnp.pad(vector, (0, width - vector.shape[0]))[None, :]

    own = call(
        keys_values_kernel,
        jax.ShapeDtypeStruct((6 * LANES, LANES), bf16),
        [pltpu.VMEM((ROWS, KV_LAT), bf16), pltpu.VMEM((KV_LAT, 256), bf16)],
    )(
        latents, rope_rows, narrow_all, memory_gain[None, :], row(key_gain, LANES),
        cosine, sine_up, sine_down,
    )
    tp, at = lax.axis_index("tp")[None], at[None]
    own, out_all, tp, at, *rest = lax.optimization_barrier(
        (own, out_all, tp, at, conv_value, conv_gate)
    )
    pieces = lax.all_gather(own, "sp")
    far = [
        lax.ppermute(out_all, "tp", [(i, (i + by) % N_TP) for i in range(N_TP)]) for by in (4, 2, 6)
    ]
    far = [far[1], far[0], far[2]]
    near = lax.ppermute(out_all, "tp", CORE_PAIRS)
    packed = call(
        pack_rest_kernel,
        jax.ShapeDtypeStruct((240, 512), bf16),
        [pltpu.SemaphoreType.DMA((8,))],
        specs=[hbm] * 2,
    )(*kept(*rest))
    conv_all = lax.all_gather(packed, "fs")
    queries = call(
        queries_kernel,
        jax.ShapeDtypeStruct((ROWS, 2 * LANES), bf16),
        [
            pltpu.VMEM((ROWS, Q_LAT), bf16),
            pltpu.VMEM((N_FS, 96, 512), bf16),
            pltpu.SemaphoreType.DMA(()),
        ],
        specs=[vmem, hbm] + [vmem] * 5,
    )(
        latents, *kept(out_all), latent_gain[None, :], row(query_gain, LANES),
        cosine, sine_up, sine_down,
    )
    stat, acc = call(
        own_kernel,
        (jax.ShapeDtypeStruct((8, ROWS), f32), jax.ShapeDtypeStruct((2 * V_DIM, ROWS), f32)),
    )(queries, own)
    gated = call(gated_kernel, jax.ShapeDtypeStruct((ROWS, LANES), bf16))(normed, conv_all, narrow_all)
    halo = lax.ppermute(gated[ROWS - HALO :], "sp", [(i, i + 1) for i in range(N_SP - 1)])
    halo, stat, acc = lax.optimization_barrier((halo, stat, acc))
    taps = jnp.pad(conv_kernel.astype(f32), ((0, 1), (0, 0)))
    conv_sum = call(
        conv_kernel_body,
        jax.ShapeDtypeStruct((ROWS + 48, LANES), bf16),
        [pltpu.VMEM((ROWS + HALO, LANES), f32), pltpu.VMEM((16, LANES), f32)],
    )(halo, gated, taps, channel_gain[None, :], channel_shift[None, :])
    conv_sum = lax.all_gather(conv_sum, "tp")
    conv_sum, near, *far = lax.optimization_barrier((conv_sum, near, *far))
    crossed = [lax.ppermute(w, "tp", CORE_PAIRS) for w in far]
    weights = kept(out_all, *far, near, *crossed)
    half = (N_TP, N_FS, 128, 512)
    conv_result = call(channel_kernel, jax.ShapeDtypeStruct((N_TP, ROWS, LANES), bf16))(conv_sum)
    base = call(
        conv_part_kernel,
        jax.ShapeDtypeStruct((ROWS, 2048), f32),
        [pltpu.VMEM(half, bf16), pltpu.SemaphoreType.DMA((N_TP,))],
        specs=[pl.BlockSpec(memory_space=pltpu.SMEM), vmem] + [hbm] * N_TP,
    )(tp, conv_result, *weights)
    pieces, base, stat, acc = lax.optimization_barrier((pieces, base, stat, acc))
    pieces = pltpu.with_memory_space_constraint(
        pieces.reshape(N_SP // BUNDLE, BUNDLE, 6 * LANES, LANES), pltpu.HBM
    )
    attention, weights = call(
        attention_kernel,
        (jax.ShapeDtypeStruct((ROWS, LANES), bf16), jax.ShapeDtypeStruct(half, bf16)),
        [
            pltpu.VMEM((N_SP // BUNDLE, BUNDLE, 6 * LANES, LANES), bf16),
            pltpu.SemaphoreType.DMA((N_SP // BUNDLE,)),
            pltpu.SemaphoreType.DMA((N_TP,)),
        ],
        specs=[pl.BlockSpec(memory_space=pltpu.SMEM), vmem, hbm, vmem, vmem] + [hbm] * N_TP,
    )(at, queries, pieces, stat, acc, *weights)
    attention = lax.all_gather(attention, "tp")
    mixed = call(
        output_kernel, jax.ShapeDtypeStruct((ROWS, 2048), bf16), scalars=1, arrays=3
    )(tp, base, attention, weights)
    return mixed[None]


def solution(mesh):
    in_specs = (
        P("fs", "sp", None),
        P(),
        P("fs", "tp"),
        P("fs", "tp"),
        P(),
        P("fs", "tp"),
        P("fs", "tp"),
        P("fs", "tp"),
        P(),
        P(),
        P(),
        P(),
        P("fs", "tp"),
        P("fs", "tp"),
        P(None, "tp"),
        P("tp"),
        P("tp"),
        P("tp", "fs"),
        P("tp", "fs"),
    )
    out_specs = P("fs", "sp", None)
    return jax.shard_map(local, mesh=mesh, in_specs=in_specs, out_specs=out_specs, check_vma=False)
```

```python
import jax
import jax.numpy as jnp
from jax import lax
from jax.experimental import pallas as pl
from jax.experimental.pallas import tpu as pltpu
from jax.sharding import PartitionSpec as P

QK_NOPE = 64
QK_ROPE = 32
V_DIM = 64
CONV_W = 1024
SEG = 64
QK_DIM = 96
Q_LAT = 768
KV_LAT = 512
ROWS = 256
TAPS = 31
HALO = 32
LANES = 128
N_FS = 4
N_TP = 8
N_SP = 16
BUNDLE = 4

epsilon = 1e-06
rope_base = 10000.0
masked_score = -1e30
log2_e = 1.4426950408889634
bf16 = jnp.bfloat16
f32 = jnp.float32

CORE_PAIRS = [(i, i ^ 1) for i in range(N_TP)]


def call(kernel, out_shape, scratch=(), scalars=0, arrays=0, specs=None, outs=None):
    extra = {"out_specs": outs} if outs else {}
    if scalars:
        smem = pl.BlockSpec(memory_space=pltpu.SMEM)
        specs = [smem] * scalars + [pl.BlockSpec(memory_space=pltpu.VMEM)] * arrays
    if specs:
        extra["in_specs"] = specs
    return pl.pallas_call(
        kernel,
        out_shape=out_shape,
        scratch_shapes=list(scratch),
        compiler_params=pltpu.CompilerParams(vmem_limit_bytes=16 * 1024 * 1024),
        **extra,
    )


def head_tile(tile, gain, cosine, sine_up, sine_down):
    scale = lax.rsqrt(jnp.sum(tile * tile, axis=-1, keepdims=True) * (1.0 / QK_DIM) + epsilon)
    tile = tile * scale * gain
    half = QK_ROPE // 2
    return (
        tile * cosine
        + pltpu.roll(tile, LANES - half, 1) * sine_up
        + pltpu.roll(tile, half, 1) * sine_down
    )


def copy_all(pairs, sems):
    copies = [
        pltpu.make_async_copy(source, target, sems.at[n]) for n, (source, target) in enumerate(pairs)
    ]
    for copy in copies:
        copy.start()
    for copy in copies:
        copy.wait()


def pack_kernel(qd_ref, md_ref, ku_ref, vu_ref, rope_ref, gain_ref, ho_ref, co_ref, narrow_ref, rope_out, gain_out, outw_ref, sems):
    pairs = [
        (qd_ref, narrow_ref.at[:96, :]),
        (md_ref, narrow_ref.at[96:160, :]),
        (rope_ref, rope_out),
        (gain_ref, gain_out),
        (ho_ref, outw_ref.at[:128, :]),
        (co_ref, outw_ref.at[128:, :]),
    ]
    for n, ref in enumerate((ku_ref, vu_ref)):
        for b in range(2):
            at = (2 * n + b) * LANES
            pairs.append((ref.at[b * 64 : (b + 1) * 64, :], narrow_ref.at[160:, at : at + LANES]))
    copy_all(pairs, sems)


def pack_rest_kernel(qu_ref, cv_ref, cg_ref, first_ref, second_ref, qu_scr, sems):
    pairs = [(qu_ref, qu_scr)]
    for ref, out in ((cv_ref, first_ref), (cg_ref, second_ref)):
        for b in range(4):
            rows = slice(b * 128, (b + 1) * 128)
            pairs.append((ref.at[rows, :], out.at[:128, rows]))
    copy_all(pairs, sems)
    first_ref[128:, :] = jnp.zeros((96, 512), bf16)
    for half in range(2):
        for h in range(2):
            at = half * 256 + h * LANES
            first_ref[128:, at : at + QK_DIM] = qu_scr[
                half * 96 : (half + 1) * 96, h * QK_DIM : (h + 1) * QK_DIM
            ]


def project_kernel(tok_ref, gain_ref, rope_w_ref, cos_ref, sin_ref, w_ref, lat_ref, rope_ref, normed_ref, cosine_ref, up_ref, down_ref, tok_scr, sems):
    block = 64
    copies = []
    for n in range(ROWS // block):
        rows = slice(n * block, (n + 1) * block)
        copies.append(
            pltpu.make_async_copy(tok_ref.at[rows, :], tok_scr.at[rows, :], sems.at[n])
        )
        copies[-1].start()
    turned = (((1,), (1,)), ((), ()))
    for r in range(0, ROWS, block):
        copies[r // block].wait()
        rows = tok_scr[r : r + block, :].astype(f32)
        scale = lax.rsqrt(jnp.mean(rows * rows, axis=-1, keepdims=True) + epsilon)
        normed_ref[r : r + block, :] = (rows * scale * gain_ref[...]).astype(bf16)
    both = jnp.zeros((ROWS, 160), f32)
    for f in range(N_FS):
        both = both + lax.dot_general(
            normed_ref[:, f * 512 : (f + 1) * 512],
            w_ref[f, :160, :],
            turned,
            preferred_element_type=f32,
        )
    both = both.astype(bf16)
    lat_ref[:ROWS, :] = both[:, :LANES]
    for r in range(4):
        lat_ref[ROWS:, r * 32 : (r + 1) * 32] = both[r * 64 : (r + 1) * 64, LANES:]
    rope = lax.dot_general(normed_ref[...], rope_w_ref[...], turned, preferred_element_type=f32)
    rope_ref[...] = jnp.zeros((ROWS, LANES), bf16)
    rope_ref[:, QK_NOPE:QK_DIM] = rope.astype(bf16)
    half = QK_ROPE // 2
    empty = jnp.zeros((ROWS, LANES - half), f32)
    cosine = jnp.concatenate([cos_ref[...].T, empty], axis=1)
    sine = jnp.concatenate([sin_ref[...].T, empty], axis=1)
    lane = lax.broadcasted_iota(jnp.int32, (ROWS, LANES), 1)
    cosine = pltpu.roll(cosine, QK_NOPE, 1) + pltpu.roll(cosine, QK_NOPE + half, 1)
    cosine_ref[...] = jnp.where(lane < QK_NOPE, 1.0, cosine)
    up_ref[...] = -pltpu.roll(sine, QK_NOPE, 1)
    down_ref[...] = pltpu.roll(sine, QK_NOPE + half, 1)


def keys_values_kernel(lat_ref, rope_ref, w_ref, mgain_ref, kgain_ref, cos_ref, up_ref, down_ref, out_ref, m_scr, w_scr):
    for g in range(N_TP):
        at = g * 64
        m_scr[:, at : at + 32] = lat_ref[g, :ROWS, 96:]
        for r in range(4):
            m_scr[r * 64 : (r + 1) * 64, at + 32 : at + 64] = lat_ref[
                g, ROWS:, r * 32 : (r + 1) * 32
            ]
    raw = m_scr[...].astype(f32)
    scale = lax.rsqrt(jnp.mean(raw * raw, axis=-1, keepdims=True) + epsilon)
    m_scr[...] = (raw * scale * mgain_ref[...]).astype(bf16)
    for f in range(N_FS):
        for n in range(2):
            for b in range(2):
                lanes = (2 * n + b) * LANES
                row = f * 128 + b * 64
                w_scr[row : row + 64, n * LANES : (n + 1) * LANES] = w_ref[
                    f, 160:, lanes : lanes + LANES
                ]
    both = jnp.dot(m_scr[...], w_scr[...], preferred_element_type=f32)
    nope = both[:, :LANES]
    lane = lax.broadcasted_iota(jnp.int32, (ROWS, LANES), 1)
    rope = rope_ref[...].astype(f32)
    tiles = []
    for h in range(2):
        part = nope if h == 0 else pltpu.roll(nope, 64, 1)
        tile = jnp.where(lane < QK_NOPE, part, rope)
        tiles.append(head_tile(tile, kgain_ref[...], cos_ref[...], up_ref[...], down_ref[...]))
    for h in range(2):
        out_ref[h * ROWS : (h + 1) * ROWS, :] = tiles[h].astype(bf16)
    values = both[:, LANES:].T.astype(bf16)
    for half in range(2):
        at = 2 * ROWS + half * LANES
        out_ref[at : at + LANES, :] = values[:, half * LANES : (half + 1) * LANES]


def queries_kernel(lat_ref, w_ref, lgain_ref, qgain_ref, cos_ref, up_ref, down_ref, out_ref, q_scr):
    for g in range(N_TP):
        q_scr[:, g * 96 : (g + 1) * 96] = lat_ref[g, :ROWS, :96]
    raw = q_scr[...].astype(f32)
    scale = lax.rsqrt(jnp.mean(raw * raw, axis=-1, keepdims=True) + epsilon)
    q_scr[...] = (raw * scale * lgain_ref[...]).astype(bf16)
    both = jnp.zeros((ROWS, 2 * LANES), f32)
    for f in range(N_FS):
        for half in range(2):
            at = f * 192 + half * 96
            both = both + jnp.dot(
                q_scr[:, at : at + 96],
                w_ref[f, 128:, half * 256 : (half + 1) * 256],
                preferred_element_type=f32,
            )
    lane = lax.broadcasted_iota(jnp.int32, (ROWS, LANES), 1)
    tiles = [
        head_tile(
            both[:, h * LANES : (h + 1) * LANES],
            qgain_ref[...],
            cos_ref[...],
            up_ref[...],
            down_ref[...],
        )
        for h in range(2)
    ]
    for h in range(2):
        out_ref[:, h * LANES : (h + 1) * LANES] = tiles[h].astype(bf16)


def gated_kernel(normed_ref, value_ref, gate_ref, out_ref):
    value = jnp.zeros((ROWS, LANES), f32)
    gate = jnp.zeros((ROWS, LANES), f32)
    for f in range(N_FS):
        for b in range(4):
            rows = normed_ref[:, f * 512 + b * LANES : f * 512 + (b + 1) * LANES]
            cols = slice(b * LANES, (b + 1) * LANES)
            value = value + jnp.dot(rows, value_ref[f, :128, cols], preferred_element_type=f32)
            gate = gate + jnp.dot(rows, gate_ref[f, :128, cols], preferred_element_type=f32)
    out_ref[...] = (value * jax.nn.sigmoid(gate)).astype(bf16)


def conv_kernel_body(halo_ref, gated_ref, taps_ref, gain_ref, shift_ref, out_ref, ext_scr, stat_scr):
    ext_scr[:HALO, :] = halo_ref[...].astype(f32)
    ext_scr[HALO:, :] = gated_ref[...].astype(f32)
    start = HALO - (TAPS - 1)
    block = LANES
    stat_scr[...] = jnp.zeros((16, LANES), f32)
    for n in range(ROWS // block):
        r = n * block
        running = jnp.zeros((block, LANES), f32)
        for j in range(TAPS):
            running = running + ext_scr[pl.ds(r + start + j, block), :] * taps_ref[j : j + 1, :]
        flat = running.T
        mean = jnp.sum(flat, axis=0, keepdims=True) * (1.0 / LANES)
        off = flat - mean
        stat_scr[n : n + 1, :] = mean
        stat_scr[2 + n : 3 + n, :] = jnp.sum(off * off, axis=0, keepdims=True)
        out_ref[r : r + block, :] = off.T.astype(bf16)
    stat_scr[4:5, :] = gain_ref[...]
    stat_scr[5:6, :] = shift_ref[...]
    left = stat_scr[...]
    for part in range(3):
        rounded = left.astype(bf16)
        out_ref[ROWS + part * 16 : ROWS + (part + 1) * 16, :] = rounded
        left = left - rounded.astype(f32)


def channel_kernel(in_ref, out_ref):
    stats = []
    for g in range(N_TP):
        parts = [
            in_ref[g, ROWS + part * 16 : ROWS + (part + 1) * 16, :].astype(f32) for part in range(3)
        ]
        stats.append(parts[0] + (parts[1] + parts[2]))
    for n in range(ROWS // LANES):
        means = [st[n : n + 1] for st in stats]
        mean = means[0]
        for g in range(1, N_TP):
            mean = mean + means[g]
        mean = mean * (1.0 / N_TP)
        spread = jnp.zeros((1, LANES), f32)
        for g in range(N_TP):
            apart = means[g] - mean
            spread = spread + stats[g][2 + n : 3 + n] + LANES * apart * apart
        scale = lax.rsqrt(spread * (1.0 / CONV_W) + epsilon)
        columns = jnp.concatenate(
            [m - mean for m in means] + [scale] + [jnp.zeros((7, LANES), f32)], axis=0
        ).T
        rows = slice(n * LANES, (n + 1) * LANES)
        for g in range(N_TP):
            value = in_ref[g, rows, :].astype(f32) + columns[:, g : g + 1]
            value = value * columns[:, N_TP : N_TP + 1] * stats[g][4:5] + stats[g][5:6]
            out_ref[g, rows, :] = (value / (1.0 + jnp.exp(-value))).astype(bf16)


def attend(q_ref, blocks, state, hidden, mask=None):
    rate = QK_DIM ** (-0.5) * log2_e
    fresh = []
    for h in range(2):
        top, total, weighted = state[h]
        keys = jnp.concatenate([b[h * ROWS : (h + 1) * ROWS, :] for b in blocks], axis=0)
        scores = lax.dot_general(
            keys,
            q_ref[:, h * LANES : (h + 1) * LANES],
            (((1,), (1,)), ((), ())),
            preferred_element_type=f32,
        )
        if mask is not None:
            scores = jnp.where(mask, scores, masked_score)
        new_top = top
        for n, off in enumerate(hidden):
            part = jnp.max(scores[n * ROWS : (n + 1) * ROWS], axis=0, keepdims=True)
            new_top = jnp.maximum(new_top, part - off)
        weights = jnp.concatenate(
            [
                jnp.exp2(scores[n * ROWS : (n + 1) * ROWS] * rate - (new_top * rate + off))
                for n, off in enumerate(hidden)
            ],
            axis=0,
        )
        factor = jnp.exp2((top - new_top) * rate)
        total = total * factor + jnp.sum(weights, axis=0, keepdims=True)
        at = 2 * ROWS + h * V_DIM
        values = jnp.concatenate(
            [b[at + i * LANES : at + i * LANES + V_DIM, :] for b in blocks for i in range(2)],
            axis=1,
        )
        weighted = weighted * factor + jnp.dot(
            values, weights.astype(bf16), preferred_element_type=f32
        )
        fresh.append((new_top, total, weighted))
    return fresh


def own_kernel(q_ref, own_ref, stat_ref, acc_ref):
    key = lax.broadcasted_iota(jnp.int32, (ROWS, ROWS), 0)
    query = lax.broadcasted_iota(jnp.int32, (ROWS, ROWS), 1)
    mask = jnp.right_shift(key, 6) <= jnp.right_shift(query, 6)
    empty = (
        jnp.full((1, ROWS), masked_score, f32),
        jnp.zeros((1, ROWS), f32),
        jnp.zeros((V_DIM, ROWS), f32),
    )
    state = attend(q_ref, [own_ref], [empty, empty], [0.0], mask)
    stat_ref[4:, :] = jnp.zeros((4, ROWS), f32)
    for h in range(2):
        stat_ref[2 * h : 2 * h + 1, :] = state[h][0]
        stat_ref[2 * h + 1 : 2 * h + 2, :] = state[h][1]
        acc_ref[h * V_DIM : (h + 1) * V_DIM, :] = state[h][2]


def attention_kernel(at_ref, q_ref, kv_ref, stat_ref, acc_ref, *rest):
    pieces, (out_ref, weight_ref, kv, sems, weight_sems) = rest[:N_TP], rest[N_TP:]
    at = at_ref[0]
    copies = [
        pltpu.make_async_copy(kv_ref.at[n], kv.at[n], sems.at[n]) for n in range(N_SP // BUNDLE)
    ]
    for copy in copies:
        copy.start()
    fetched = [
        pltpu.make_async_copy(piece.at[:, :128, :], weight_ref.at[n], weight_sems.at[n])
        for n, piece in enumerate(pieces)
    ]
    for copy in fetched:
        copy.start()
    state = [
        (
            stat_ref[2 * h : 2 * h + 1, :],
            stat_ref[2 * h + 1 : 2 * h + 2, :],
            acc_ref[h * V_DIM : (h + 1) * V_DIM, :],
        )
        for h in range(2)
    ]
    for n, copy in enumerate(copies):
        copy.wait()
        hidden = [jnp.where(n * BUNDLE + i < at, 0.0, -masked_score) for i in range(BUNDLE)]
        blocks = [kv.at[n, i] for i in range(BUNDLE)]
        state = lax.cond(
            n * BUNDLE < at,
            lambda s, blocks=blocks, hidden=hidden: attend(q_ref, blocks, s, hidden),
            lambda s: s,
            state,
        )
    result = jnp.concatenate([state[h][2] / state[h][1] for h in range(2)], axis=0)
    out_ref[...] = result.T.astype(bf16)
    for copy in fetched:
        copy.wait()


def sources(g):
    other = g + 1 - 2 * lax.rem(g, 2)
    return [lax.rem(first + N_TP - s, N_TP) for first in (g, other) for s in (0, 2, 4, 6)]


def conv_part_kernel(tp_ref, conv_ref, *rest):
    pieces, (out_ref, weights, sems) = rest[:N_TP], rest[N_TP:]
    fetched = [
        pltpu.make_async_copy(piece.at[:, 128:, :], weights.at[n], sems.at[n])
        for n, piece in enumerate(pieces)
    ]
    for copy in fetched:
        copy.start()
    for n, g in enumerate(sources(tp_ref[0])):
        fetched[n].wait()
        left = conv_ref[g]
        for f in range(N_FS):
            cols = slice(f * 512, (f + 1) * 512)
            part = jnp.dot(left, weights[n, f], preferred_element_type=f32)
            out_ref[:, cols] = part if n == 0 else out_ref[:, cols] + part


def output_kernel(tp_ref, base_ref, attn_ref, weight_ref, out_ref):
    owners = sources(tp_ref[0])
    left = jnp.concatenate([attn_ref[g] for g in owners], axis=1)
    for f in range(N_FS):
        cols = slice(f * 512, (f + 1) * 512)
        weight = jnp.concatenate([weight_ref[n, f] for n in range(N_TP)], axis=0)
        total = base_ref[:, cols] + jnp.dot(left, weight, preferred_element_type=f32)
        out_ref[:, cols] = total.astype(bf16)


def rotation_tables(positions):
    inverse_freq = 1.0 / rope_base ** (jnp.arange(0, QK_ROPE, 2, dtype=f32) / QK_ROPE)
    angles = positions.astype(f32)[None, :] * inverse_freq[:, None]
    return jnp.cos(angles), jnp.sin(angles)


def local(
    tokens,
    mix_gain,
    query_down,
    memory_down,
    rope_weight,
    query_up,
    key_up,
    value_up,
    latent_gain,
    memory_gain,
    query_gain,
    key_gain,
    conv_value,
    conv_gate,
    conv_kernel,
    channel_gain,
    channel_shift,
    heads_out,
    conv_out,
):
    at = lax.axis_index("sp")
    hbm = pl.BlockSpec(memory_space=pltpu.HBM)
    vmem = pl.BlockSpec(memory_space=pltpu.VMEM)
    def kept(*arrays):
        return [pltpu.with_memory_space_constraint(a, pltpu.HBM) for a in arrays]

    narrow, rope_w, gain, outw = call(
        pack_kernel,
        (
            jax.ShapeDtypeStruct((224, 512), bf16),
            jax.ShapeDtypeStruct((QK_ROPE, 2048), bf16),
            jax.ShapeDtypeStruct((1, 2048), f32),
            jax.ShapeDtypeStruct((256, 512), bf16),
        ),
        [pltpu.SemaphoreType.DMA((10,))],
        specs=[hbm] * 8,
    )(
        *kept(
            query_down.T, memory_down.T, key_up, value_up, rope_weight.T, mix_gain[None, :],
            heads_out, conv_out,
        )
    )
    out_all = lax.all_gather(outw, "fs")
    narrow_all = lax.all_gather(narrow, "fs")
    positions = at * ROWS + jnp.arange(ROWS, dtype=jnp.int32)
    cosine, sine = rotation_tables(positions)
    table = jax.ShapeDtypeStruct((ROWS, LANES), f32)
    latents, rope_rows, normed, cosine, sine_up, sine_down = call(
        project_kernel,
        (
            jax.ShapeDtypeStruct((320, LANES), bf16),
            jax.ShapeDtypeStruct((ROWS, LANES), bf16),
            jax.ShapeDtypeStruct((ROWS, 2048), bf16),
            table,
            table,
            table,
        ),
        [pltpu.VMEM((ROWS, 2048), bf16), pltpu.SemaphoreType.DMA((4,))],
        specs=[hbm] + [vmem] * 5,
    )(pltpu.with_memory_space_constraint(tokens[0], pltpu.HBM), gain, rope_w, cosine, sine, narrow_all)
    latents = lax.all_gather(latents, "tp")

    def row(vector, width):
        return jnp.pad(vector, (0, width - vector.shape[0]))[None, :]

    own = call(
        keys_values_kernel,
        jax.ShapeDtypeStruct((6 * LANES, LANES), bf16),
        [pltpu.VMEM((ROWS, KV_LAT), bf16), pltpu.VMEM((KV_LAT, 256), bf16)],
    )(
        latents, rope_rows, narrow_all, memory_gain[None, :], row(key_gain, LANES),
        cosine, sine_up, sine_down,
    )
    tp, at = lax.axis_index("tp")[None], at[None]
    own, out_all, tp, at, *rest = lax.optimization_barrier(
        (own, out_all, tp, at, query_up, conv_value, conv_gate)
    )
    pieces = lax.all_gather(own, "sp")
    far = [
        lax.ppermute(out_all, "tp", [(i, (i + by) % N_TP) for i in range(N_TP)]) for by in (4, 2, 6)
    ]
    far = [far[1], far[0], far[2]]
    near = lax.ppermute(out_all, "tp", CORE_PAIRS)
    packed = call(
        pack_rest_kernel,
        tuple(jax.ShapeDtypeStruct((rows, 512), bf16) for rows in (224, 128)),
        [pltpu.VMEM((192, 192), bf16), pltpu.SemaphoreType.DMA((9,))],
        specs=[hbm] * 3,
    )(*kept(*rest))
    first_all, second_all = (lax.all_gather(p, "fs") for p in packed)
    queries = call(
        queries_kernel,
        jax.ShapeDtypeStruct((ROWS, 2 * LANES), bf16),
        [pltpu.VMEM((ROWS, Q_LAT), bf16)],
    )(
        latents, first_all, latent_gain[None, :], row(query_gain, LANES),
        cosine, sine_up, sine_down,
    )
    gated = call(gated_kernel, jax.ShapeDtypeStruct((ROWS, LANES), bf16))(normed, first_all, second_all)
    halo = lax.ppermute(gated[ROWS - HALO :], "sp", [(i, i + 1) for i in range(N_SP - 1)])
    stat, acc = call(
        own_kernel,
        (jax.ShapeDtypeStruct((8, ROWS), f32), jax.ShapeDtypeStruct((2 * V_DIM, ROWS), f32)),
    )(queries, own)
    halo, stat, acc = lax.optimization_barrier((halo, stat, acc))
    taps = jnp.pad(conv_kernel.astype(f32), ((0, 1), (0, 0)))
    conv_sum = call(
        conv_kernel_body,
        jax.ShapeDtypeStruct((ROWS + 48, LANES), bf16),
        [pltpu.VMEM((ROWS + HALO, LANES), f32), pltpu.VMEM((16, LANES), f32)],
    )(halo, gated, taps, channel_gain[None, :], channel_shift[None, :])
    conv_sum = lax.all_gather(conv_sum, "tp")
    conv_sum, near, *far = lax.optimization_barrier((conv_sum, near, *far))
    crossed = [lax.ppermute(w, "tp", CORE_PAIRS) for w in far]
    weights = kept(out_all, *far, near, *crossed)
    half = (N_TP, N_FS, 128, 512)
    conv_result = call(channel_kernel, jax.ShapeDtypeStruct((N_TP, ROWS, LANES), bf16))(conv_sum)
    base = call(
        conv_part_kernel,
        jax.ShapeDtypeStruct((ROWS, 2048), f32),
        [pltpu.VMEM(half, bf16), pltpu.SemaphoreType.DMA((N_TP,))],
        specs=[pl.BlockSpec(memory_space=pltpu.SMEM), vmem] + [hbm] * N_TP,
    )(tp, conv_result, *weights)
    pieces, base, stat, acc = lax.optimization_barrier((pieces, base, stat, acc))
    pieces = pltpu.with_memory_space_constraint(
        pieces.reshape(N_SP // BUNDLE, BUNDLE, 6 * LANES, LANES), pltpu.HBM
    )
    attention, weights = call(
        attention_kernel,
        (jax.ShapeDtypeStruct((ROWS, LANES), bf16), jax.ShapeDtypeStruct(half, bf16)),
        [
            pltpu.VMEM((N_SP // BUNDLE, BUNDLE, 6 * LANES, LANES), bf16),
            pltpu.SemaphoreType.DMA((N_SP // BUNDLE,)),
            pltpu.SemaphoreType.DMA((N_TP,)),
        ],
        specs=[pl.BlockSpec(memory_space=pltpu.SMEM), vmem, hbm, vmem, vmem] + [hbm] * N_TP,
    )(at, queries, pieces, stat, acc, *weights)
    attention = lax.all_gather(attention, "tp")
    mixed = call(
        output_kernel, jax.ShapeDtypeStruct((ROWS, 2048), bf16), scalars=1, arrays=3
    )(tp, base, attention, weights)
    return mixed[None]


def solution(mesh):
    in_specs = (
        P("fs", "sp", None),
        P(),
        P("fs", "tp"),
        P("fs", "tp"),
        P(),
        P("fs", "tp"),
        P("fs", "tp"),
        P("fs", "tp"),
        P(),
        P(),
        P(),
        P(),
        P("fs", "tp"),
        P("fs", "tp"),
        P(None, "tp"),
        P("tp"),
        P("tp"),
        P("tp", "fs"),
        P("tp", "fs"),
    )
    out_specs = P("fs", "sp", None)
    return jax.shard_map(local, mesh=mesh, in_specs=in_specs, out_specs=out_specs, check_vma=False)
```

```python
import jax
import jax.numpy as jnp
from jax import lax
from jax.experimental import pallas as pl
from jax.experimental.pallas import tpu as pltpu
from jax.sharding import PartitionSpec as P

QK_NOPE = 64
QK_ROPE = 32
V_DIM = 64
CONV_W = 1024
SEG = 64
QK_DIM = 96
Q_LAT = 768
KV_LAT = 512
ROWS = 256
TAPS = 31
HALO = 32
LANES = 128
N_FS = 4
N_TP = 8
N_SP = 16
BUNDLE = 4

epsilon = 1e-06
rope_base = 10000.0
masked_score = -1e30
log2_e = 1.4426950408889634
bf16 = jnp.bfloat16
f32 = jnp.float32

CORE_PAIRS = [(i, i ^ 1) for i in range(N_TP)]


def call(kernel, out_shape, scratch=(), scalars=0, arrays=0, specs=None, outs=None):
    extra = {"out_specs": outs} if outs else {}
    if scalars:
        smem = pl.BlockSpec(memory_space=pltpu.SMEM)
        specs = [smem] * scalars + [pl.BlockSpec(memory_space=pltpu.VMEM)] * arrays
    if specs:
        extra["in_specs"] = specs
    return pl.pallas_call(
        kernel,
        out_shape=out_shape,
        scratch_shapes=list(scratch),
        compiler_params=pltpu.CompilerParams(vmem_limit_bytes=16 * 1024 * 1024),
        **extra,
    )


def head_tile(tile, gain, cosine, sine_up, sine_down):
    scale = lax.rsqrt(jnp.sum(tile * tile, axis=-1, keepdims=True) * (1.0 / QK_DIM) + epsilon)
    tile = tile * scale * gain
    half = QK_ROPE // 2
    return (
        tile * cosine
        + pltpu.roll(tile, LANES - half, 1) * sine_up
        + pltpu.roll(tile, half, 1) * sine_down
    )


def copy_all(pairs, sems):
    copies = [
        pltpu.make_async_copy(source, target, sems.at[n]) for n, (source, target) in enumerate(pairs)
    ]
    for copy in copies:
        copy.start()
    for copy in copies:
        copy.wait()


def pack_kernel(qd_ref, md_ref, ku_ref, vu_ref, rope_ref, gain_ref, tok_ref, narrow_ref, rope_out, gain_out, tok_out, sems):
    pairs = [
        (qd_ref, narrow_ref.at[:96, :]),
        (md_ref, narrow_ref.at[96:160, :]),
        (rope_ref, rope_out),
        (gain_ref, gain_out),
    ]
    for n, ref in enumerate((ku_ref, vu_ref)):
        for b in range(2):
            at = (2 * n + b) * LANES
            pairs.append((ref.at[b * 64 : (b + 1) * 64, :], narrow_ref.at[160:, at : at + LANES]))
    pairs.append((tok_ref, tok_out))
    copy_all(pairs, sems)


def pack_out_kernel(ho_ref, co_ref, out_ref, sems):
    copy_all([(ho_ref, out_ref.at[:128, :]), (co_ref, out_ref.at[128:, :])], sems)


def pack_rest_kernel(qu_ref, cv_ref, cg_ref, first_ref, second_ref, qu_scr, sems):
    pairs = [(qu_ref, qu_scr)]
    for ref, out in ((cv_ref, first_ref), (cg_ref, second_ref)):
        for b in range(4):
            rows = slice(b * 128, (b + 1) * 128)
            pairs.append((ref.at[rows, :], out.at[:128, rows]))
    copy_all(pairs, sems)
    first_ref[128:, :] = jnp.zeros((96, 512), bf16)
    for half in range(2):
        for h in range(2):
            at = half * 256 + h * LANES
            first_ref[128:, at : at + QK_DIM] = qu_scr[
                half * 96 : (half + 1) * 96, h * QK_DIM : (h + 1) * QK_DIM
            ]


def project_kernel(tok_ref, gain_ref, rope_w_ref, cos_ref, sin_ref, w_ref, lat_ref, rope_ref, normed_ref, cosine_ref, up_ref, down_ref):
    block = 64
    turned = (((1,), (1,)), ((), ()))
    for r in range(0, ROWS, block):
        rows = tok_ref[r : r + block, :].astype(f32)
        scale = lax.rsqrt(jnp.mean(rows * rows, axis=-1, keepdims=True) + epsilon)
        normed_ref[r : r + block, :] = (rows * scale * gain_ref[...]).astype(bf16)
    both = jnp.zeros((ROWS, 160), f32)
    for f in range(N_FS):
        both = both + lax.dot_general(
            normed_ref[:, f * 512 : (f + 1) * 512],
            w_ref[f, :160, :],
            turned,
            preferred_element_type=f32,
        )
    both = both.astype(bf16)
    lat_ref[:ROWS, :] = both[:, :LANES]
    for r in range(4):
        lat_ref[ROWS:, r * 32 : (r + 1) * 32] = both[r * 64 : (r + 1) * 64, LANES:]
    rope = lax.dot_general(normed_ref[...], rope_w_ref[...], turned, preferred_element_type=f32)
    rope_ref[...] = jnp.zeros((ROWS, LANES), bf16)
    rope_ref[:, QK_NOPE:QK_DIM] = rope.astype(bf16)
    half = QK_ROPE // 2
    empty = jnp.zeros((ROWS, LANES - half), f32)
    cosine = jnp.concatenate([cos_ref[...].T, empty], axis=1)
    sine = jnp.concatenate([sin_ref[...].T, empty], axis=1)
    lane = lax.broadcasted_iota(jnp.int32, (ROWS, LANES), 1)
    cosine = pltpu.roll(cosine, QK_NOPE, 1) + pltpu.roll(cosine, QK_NOPE + half, 1)
    cosine_ref[...] = jnp.where(lane < QK_NOPE, 1.0, cosine)
    up_ref[...] = -pltpu.roll(sine, QK_NOPE, 1)
    down_ref[...] = pltpu.roll(sine, QK_NOPE + half, 1)


def keys_values_kernel(lat_ref, rope_ref, w_ref, mgain_ref, kgain_ref, cos_ref, up_ref, down_ref, out_ref, m_scr, w_scr):
    for g in range(N_TP):
        at = g * 64
        m_scr[:, at : at + 32] = lat_ref[g, :ROWS, 96:]
        for r in range(4):
            m_scr[r * 64 : (r + 1) * 64, at + 32 : at + 64] = lat_ref[
                g, ROWS:, r * 32 : (r + 1) * 32
            ]
    raw = m_scr[...].astype(f32)
    scale = lax.rsqrt(jnp.mean(raw * raw, axis=-1, keepdims=True) + epsilon)
    m_scr[...] = (raw * scale * mgain_ref[...]).astype(bf16)
    for f in range(N_FS):
        for n in range(2):
            for b in range(2):
                lanes = (2 * n + b) * LANES
                row = f * 128 + b * 64
                w_scr[row : row + 64, n * LANES : (n + 1) * LANES] = w_ref[
                    f, 160:, lanes : lanes + LANES
                ]
    both = jnp.dot(m_scr[...], w_scr[...], preferred_element_type=f32)
    nope = both[:, :LANES]
    lane = lax.broadcasted_iota(jnp.int32, (ROWS, LANES), 1)
    rope = rope_ref[...].astype(f32)
    tiles = []
    for h in range(2):
        part = nope if h == 0 else pltpu.roll(nope, 64, 1)
        tile = jnp.where(lane < QK_NOPE, part, rope)
        tiles.append(head_tile(tile, kgain_ref[...], cos_ref[...], up_ref[...], down_ref[...]))
    for h in range(2):
        out_ref[h * ROWS : (h + 1) * ROWS, :] = tiles[h].astype(bf16)
    values = both[:, LANES:].T.astype(bf16)
    for half in range(2):
        at = 2 * ROWS + half * LANES
        out_ref[at : at + LANES, :] = values[:, half * LANES : (half + 1) * LANES]


def queries_kernel(lat_ref, w_ref, lgain_ref, qgain_ref, cos_ref, up_ref, down_ref, out_ref, q_scr):
    for g in range(N_TP):
        q_scr[:, g * 96 : (g + 1) * 96] = lat_ref[g, :ROWS, :96]
    raw = q_scr[...].astype(f32)
    scale = lax.rsqrt(jnp.mean(raw * raw, axis=-1, keepdims=True) + epsilon)
    q_scr[...] = (raw * scale * lgain_ref[...]).astype(bf16)
    both = jnp.zeros((ROWS, 2 * LANES), f32)
    for f in range(N_FS):
        for half in range(2):
            at = f * 192 + half * 96
            both = both + jnp.dot(
                q_scr[:, at : at + 96],
                w_ref[f, 128:, half * 256 : (half + 1) * 256],
                preferred_element_type=f32,
            )
    lane = lax.broadcasted_iota(jnp.int32, (ROWS, LANES), 1)
    tiles = [
        head_tile(
            both[:, h * LANES : (h + 1) * LANES],
            qgain_ref[...],
            cos_ref[...],
            up_ref[...],
            down_ref[...],
        )
        for h in range(2)
    ]
    for h in range(2):
        out_ref[:, h * LANES : (h + 1) * LANES] = tiles[h].astype(bf16)


def gated_kernel(normed_ref, value_ref, gate_ref, out_ref):
    value = jnp.zeros((ROWS, LANES), f32)
    gate = jnp.zeros((ROWS, LANES), f32)
    for f in range(N_FS):
        for b in range(4):
            rows = normed_ref[:, f * 512 + b * LANES : f * 512 + (b + 1) * LANES]
            cols = slice(b * LANES, (b + 1) * LANES)
            value = value + jnp.dot(rows, value_ref[f, :128, cols], preferred_element_type=f32)
            gate = gate + jnp.dot(rows, gate_ref[f, :128, cols], preferred_element_type=f32)
    out_ref[...] = (value * jax.nn.sigmoid(gate)).astype(bf16)


def conv_kernel_body(halo_ref, gated_ref, taps_ref, gain_ref, shift_ref, out_ref, ext_scr, stat_scr):
    ext_scr[:HALO, :] = halo_ref[...].astype(f32)
    ext_scr[HALO:, :] = gated_ref[...].astype(f32)
    start = HALO - (TAPS - 1)
    block = LANES
    stat_scr[...] = jnp.zeros((16, LANES), f32)
    for n in range(ROWS // block):
        r = n * block
        running = jnp.zeros((block, LANES), f32)
        for j in range(TAPS):
            running = running + ext_scr[pl.ds(r + start + j, block), :] * taps_ref[j : j + 1, :]
        flat = running.T
        mean = jnp.sum(flat, axis=0, keepdims=True) * (1.0 / LANES)
        off = flat - mean
        stat_scr[n : n + 1, :] = mean
        stat_scr[2 + n : 3 + n, :] = jnp.sum(off * off, axis=0, keepdims=True)
        out_ref[r : r + block, :] = off.T.astype(bf16)
    stat_scr[4:5, :] = gain_ref[...]
    stat_scr[5:6, :] = shift_ref[...]
    left = stat_scr[...]
    for part in range(3):
        rounded = left.astype(bf16)
        out_ref[ROWS + part * 16 : ROWS + (part + 1) * 16, :] = rounded
        left = left - rounded.astype(f32)


def channel_kernel(in_ref, out_ref):
    stats = []
    for g in range(N_TP):
        parts = [
            in_ref[g, ROWS + part * 16 : ROWS + (part + 1) * 16, :].astype(f32) for part in range(3)
        ]
        stats.append(parts[0] + (parts[1] + parts[2]))
    for n in range(ROWS // LANES):
        means = [st[n : n + 1] for st in stats]
        mean = means[0]
        for g in range(1, N_TP):
            mean = mean + means[g]
        mean = mean * (1.0 / N_TP)
        spread = jnp.zeros((1, LANES), f32)
        for g in range(N_TP):
            apart = means[g] - mean
            spread = spread + stats[g][2 + n : 3 + n] + LANES * apart * apart
        scale = lax.rsqrt(spread * (1.0 / CONV_W) + epsilon)
        columns = jnp.concatenate(
            [m - mean for m in means] + [scale] + [jnp.zeros((7, LANES), f32)], axis=0
        ).T
        rows = slice(n * LANES, (n + 1) * LANES)
        for g in range(N_TP):
            value = in_ref[g, rows, :].astype(f32) + columns[:, g : g + 1]
            value = value * columns[:, N_TP : N_TP + 1] * stats[g][4:5] + stats[g][5:6]
            out_ref[g, rows, :] = (value / (1.0 + jnp.exp(-value))).astype(bf16)


def attend(q_ref, blocks, state, hidden, mask=None):
    rate = QK_DIM ** (-0.5) * log2_e
    fresh = []
    for h in range(2):
        top, total, weighted = state[h]
        keys = jnp.concatenate([b[h * ROWS : (h + 1) * ROWS, :] for b in blocks], axis=0)
        scores = lax.dot_general(
            keys,
            q_ref[:, h * LANES : (h + 1) * LANES],
            (((1,), (1,)), ((), ())),
            preferred_element_type=f32,
        )
        if mask is not None:
            scores = jnp.where(mask, scores, masked_score)
        new_top = top
        for n, off in enumerate(hidden):
            part = jnp.max(scores[n * ROWS : (n + 1) * ROWS], axis=0, keepdims=True)
            new_top = jnp.maximum(new_top, part - off)
        weights = jnp.concatenate(
            [
                jnp.exp2(scores[n * ROWS : (n + 1) * ROWS] * rate - (new_top * rate + off))
                for n, off in enumerate(hidden)
            ],
            axis=0,
        )
        factor = jnp.exp2((top - new_top) * rate)
        total = total * factor + jnp.sum(weights, axis=0, keepdims=True)
        at = 2 * ROWS + h * V_DIM
        values = jnp.concatenate(
            [b[at + i * LANES : at + i * LANES + V_DIM, :] for b in blocks for i in range(2)],
            axis=1,
        )
        weighted = weighted * factor + jnp.dot(
            values, weights.astype(bf16), preferred_element_type=f32
        )
        fresh.append((new_top, total, weighted))
    return fresh


def own_kernel(q_ref, own_ref, stat_ref, acc_ref):
    key = lax.broadcasted_iota(jnp.int32, (ROWS, ROWS), 0)
    query = lax.broadcasted_iota(jnp.int32, (ROWS, ROWS), 1)
    mask = jnp.right_shift(key, 6) <= jnp.right_shift(query, 6)
    empty = (
        jnp.full((1, ROWS), masked_score, f32),
        jnp.zeros((1, ROWS), f32),
        jnp.zeros((V_DIM, ROWS), f32),
    )
    state = attend(q_ref, [own_ref], [empty, empty], [0.0], mask)
    stat_ref[4:, :] = jnp.zeros((4, ROWS), f32)
    for h in range(2):
        stat_ref[2 * h : 2 * h + 1, :] = state[h][0]
        stat_ref[2 * h + 1 : 2 * h + 2, :] = state[h][1]
        acc_ref[h * V_DIM : (h + 1) * V_DIM, :] = state[h][2]


def attention_kernel(at_ref, q_ref, kv_ref, stat_ref, acc_ref, *rest):
    pieces, (out_ref, weight_ref, kv, sems, weight_sems) = rest[:N_TP], rest[N_TP:]
    at = at_ref[0]
    copies = [
        pltpu.make_async_copy(kv_ref.at[n], kv.at[n], sems.at[n]) for n in range(N_SP // BUNDLE)
    ]
    for n, copy in enumerate(copies):
        pl.when(n * BUNDLE < at)(copy.start)
    fetched = [
        pltpu.make_async_copy(piece.at[:, :128, :], weight_ref.at[n], weight_sems.at[n])
        for n, piece in enumerate(pieces)
    ]
    for copy in fetched:
        copy.start()
    state = [
        (
            stat_ref[2 * h : 2 * h + 1, :],
            stat_ref[2 * h + 1 : 2 * h + 2, :],
            acc_ref[h * V_DIM : (h + 1) * V_DIM, :],
        )
        for h in range(2)
    ]
    for n, copy in enumerate(copies):
        hidden = [jnp.where(n * BUNDLE + i < at, 0.0, -masked_score) for i in range(BUNDLE)]
        blocks = [kv.at[n, i] for i in range(BUNDLE)]

        def visible(state, blocks=blocks, hidden=hidden, copy=copy):
            copy.wait()
            return attend(q_ref, blocks, state, hidden)

        state = lax.cond(n * BUNDLE < at, visible, lambda s: s, state)
    result = jnp.concatenate([state[h][2] / state[h][1] for h in range(2)], axis=0)
    out_ref[...] = result.T.astype(bf16)
    for copy in fetched:
        copy.wait()


def sources(g):
    other = g + 1 - 2 * lax.rem(g, 2)
    return [lax.rem(first + N_TP - s, N_TP) for first in (g, other) for s in (0, 2, 4, 6)]


def conv_part_kernel(tp_ref, conv_ref, *rest):
    pieces, (out_ref, weights, sems) = rest[:N_TP], rest[N_TP:]
    fetched = [
        pltpu.make_async_copy(piece.at[:, 128:, :], weights.at[n], sems.at[n])
        for n, piece in enumerate(pieces)
    ]
    for copy in fetched:
        copy.start()
    for n, g in enumerate(sources(tp_ref[0])):
        fetched[n].wait()
        left = conv_ref[g]
        for f in range(N_FS):
            cols = slice(f * 512, (f + 1) * 512)
            part = jnp.dot(left, weights[n, f], preferred_element_type=f32)
            out_ref[:, cols] = part if n == 0 else out_ref[:, cols] + part


def output_kernel(tp_ref, base_ref, attn_ref, weight_ref, out_ref):
    owners = sources(tp_ref[0])
    left = jnp.concatenate([attn_ref[g] for g in owners], axis=1)
    for f in range(N_FS):
        cols = slice(f * 512, (f + 1) * 512)
        weight = jnp.concatenate([weight_ref[n, f] for n in range(N_TP)], axis=0)
        total = base_ref[:, cols] + jnp.dot(left, weight, preferred_element_type=f32)
        out_ref[:, cols] = total.astype(bf16)


def rotation_tables(positions):
    inverse_freq = 1.0 / rope_base ** (jnp.arange(0, QK_ROPE, 2, dtype=f32) / QK_ROPE)
    angles = positions.astype(f32)[None, :] * inverse_freq[:, None]
    return jnp.cos(angles), jnp.sin(angles)


def local(
    tokens,
    mix_gain,
    query_down,
    memory_down,
    rope_weight,
    query_up,
    key_up,
    value_up,
    latent_gain,
    memory_gain,
    query_gain,
    key_gain,
    conv_value,
    conv_gate,
    conv_kernel,
    channel_gain,
    channel_shift,
    heads_out,
    conv_out,
):
    at = lax.axis_index("sp")
    hbm = pl.BlockSpec(memory_space=pltpu.HBM)
    vmem = pl.BlockSpec(memory_space=pltpu.VMEM)
    def kept(*arrays):
        return [pltpu.with_memory_space_constraint(a, pltpu.HBM) for a in arrays]

    outw = call(
        pack_out_kernel,
        jax.ShapeDtypeStruct((256, 512), bf16),
        [pltpu.SemaphoreType.DMA((2,))],
        specs=[hbm] * 2,
    )(*kept(heads_out, conv_out))
    out_all = lax.all_gather(outw, "fs")
    narrow, rope_w, gain, own_rows = call(
        pack_kernel,
        (
            jax.ShapeDtypeStruct((224, 512), bf16),
            jax.ShapeDtypeStruct((QK_ROPE, 2048), bf16),
            jax.ShapeDtypeStruct((1, 2048), f32),
            jax.ShapeDtypeStruct((ROWS, 2048), bf16),
        ),
        [pltpu.SemaphoreType.DMA((9,))],
        specs=[hbm] * 7,
    )(
        *kept(
            query_down.T, memory_down.T, key_up, value_up, rope_weight.T, mix_gain[None, :],
            tokens[0],
        )
    )
    narrow_all = lax.all_gather(narrow, "fs")
    positions = at * ROWS + jnp.arange(ROWS, dtype=jnp.int32)
    cosine, sine = rotation_tables(positions)
    table = jax.ShapeDtypeStruct((ROWS, LANES), f32)
    latents, rope_rows, normed, cosine, sine_up, sine_down = call(
        project_kernel,
        (
            jax.ShapeDtypeStruct((320, LANES), bf16),
            jax.ShapeDtypeStruct((ROWS, LANES), bf16),
            jax.ShapeDtypeStruct((ROWS, 2048), bf16),
            table,
            table,
            table,
        ),
    )(own_rows, gain, rope_w, cosine, sine, narrow_all)
    latents = lax.all_gather(latents, "tp")

    def row(vector, width):
        return jnp.pad(vector, (0, width - vector.shape[0]))[None, :]

    own = call(
        keys_values_kernel,
        jax.ShapeDtypeStruct((6 * LANES, LANES), bf16),
        [pltpu.VMEM((ROWS, KV_LAT), bf16), pltpu.VMEM((KV_LAT, 256), bf16)],
    )(
        latents, rope_rows, narrow_all, memory_gain[None, :], row(key_gain, LANES),
        cosine, sine_up, sine_down,
    )
    tp, at = lax.axis_index("tp")[None], at[None]
    own, out_all, tp, at, *rest = lax.optimization_barrier(
        (own, out_all, tp, at, query_up, conv_value, conv_gate)
    )
    pieces = lax.all_gather(own, "sp")
    far = [
        lax.ppermute(out_all, "tp", [(i, (i + by) % N_TP) for i in range(N_TP)]) for by in (4, 2, 6)
    ]
    far = [far[1], far[0], far[2]]
    near = lax.ppermute(out_all, "tp", CORE_PAIRS)
    packed = call(
        pack_rest_kernel,
        tuple(jax.ShapeDtypeStruct((rows, 512), bf16) for rows in (224, 128)),
        [pltpu.VMEM((192, 192), bf16), pltpu.SemaphoreType.DMA((9,))],
        specs=[hbm] * 3,
    )(*kept(*rest))
    first_all, second_all = (lax.all_gather(p, "fs") for p in packed)
    queries = call(
        queries_kernel,
        jax.ShapeDtypeStruct((ROWS, 2 * LANES), bf16),
        [pltpu.VMEM((ROWS, Q_LAT), bf16)],
    )(
        latents, first_all, latent_gain[None, :], row(query_gain, LANES),
        cosine, sine_up, sine_down,
    )
    gated = call(gated_kernel, jax.ShapeDtypeStruct((ROWS, LANES), bf16))(normed, first_all, second_all)
    halo = lax.ppermute(gated[ROWS - HALO :], "sp", [(i, i + 1) for i in range(N_SP - 1)])
    stat, acc = call(
        own_kernel,
        (jax.ShapeDtypeStruct((8, ROWS), f32), jax.ShapeDtypeStruct((2 * V_DIM, ROWS), f32)),
    )(queries, own)
    halo, stat, acc = lax.optimization_barrier((halo, stat, acc))
    taps = jnp.pad(conv_kernel.astype(f32), ((0, 1), (0, 0)))
    conv_sum = call(
        conv_kernel_body,
        jax.ShapeDtypeStruct((ROWS + 48, LANES), bf16),
        [pltpu.VMEM((ROWS + HALO, LANES), f32), pltpu.VMEM((16, LANES), f32)],
    )(halo, gated, taps, channel_gain[None, :], channel_shift[None, :])
    conv_sum = lax.all_gather(conv_sum, "tp")
    conv_sum, near, *far = lax.optimization_barrier((conv_sum, near, *far))
    crossed = [lax.ppermute(w, "tp", CORE_PAIRS) for w in far]
    weights = kept(out_all, *far, near, *crossed)
    half = (N_TP, N_FS, 128, 512)
    conv_result = call(channel_kernel, jax.ShapeDtypeStruct((N_TP, ROWS, LANES), bf16))(conv_sum)
    base = call(
        conv_part_kernel,
        jax.ShapeDtypeStruct((ROWS, 2048), f32),
        [pltpu.VMEM(half, bf16), pltpu.SemaphoreType.DMA((N_TP,))],
        specs=[pl.BlockSpec(memory_space=pltpu.SMEM), vmem] + [hbm] * N_TP,
    )(tp, conv_result, *weights)
    pieces, base, stat, acc = lax.optimization_barrier((pieces, base, stat, acc))
    pieces = pltpu.with_memory_space_constraint(
        pieces.reshape(N_SP // BUNDLE, BUNDLE, 6 * LANES, LANES), pltpu.HBM
    )
    attention, weights = call(
        attention_kernel,
        (jax.ShapeDtypeStruct((ROWS, LANES), bf16), jax.ShapeDtypeStruct(half, bf16)),
        [
            pltpu.VMEM((N_SP // BUNDLE, BUNDLE, 6 * LANES, LANES), bf16),
            pltpu.SemaphoreType.DMA((N_SP // BUNDLE,)),
            pltpu.SemaphoreType.DMA((N_TP,)),
        ],
        specs=[pl.BlockSpec(memory_space=pltpu.SMEM), vmem, hbm, vmem, vmem] + [hbm] * N_TP,
    )(at, queries, pieces, stat, acc, *weights)
    attention = lax.all_gather(attention, "tp")
    mixed = call(
        output_kernel, jax.ShapeDtypeStruct((ROWS, 2048), bf16), scalars=1, arrays=3
    )(tp, base, attention, weights)
    return mixed[None]


def solution(mesh):
    in_specs = (
        P("fs", "sp", None),
        P(),
        P("fs", "tp"),
        P("fs", "tp"),
        P(),
        P("fs", "tp"),
        P("fs", "tp"),
        P("fs", "tp"),
        P(),
        P(),
        P(),
        P(),
        P("fs", "tp"),
        P("fs", "tp"),
        P(None, "tp"),
        P("tp"),
        P("tp"),
        P("tp", "fs"),
        P("tp", "fs"),
    )
    out_specs = P("fs", "sp", None)
    return jax.shard_map(local, mesh=mesh, in_specs=in_specs, out_specs=out_specs, check_vma=False)
```

```python
import jax
import jax.numpy as jnp
from jax import lax
from jax.experimental import pallas as pl
from jax.experimental.pallas import tpu as pltpu
from jax.sharding import PartitionSpec as P

QK_NOPE = 64
QK_ROPE = 32
V_DIM = 64
CONV_W = 1024
SEG = 64
QK_DIM = 96
Q_LAT = 768
KV_LAT = 512
ROWS = 256
TAPS = 31
HALO = 32
LANES = 128
N_FS = 4
N_TP = 8
N_SP = 16
BUNDLE = 4

epsilon = 1e-06
rope_base = 10000.0
masked_score = -1e30
log2_e = 1.4426950408889634
bf16 = jnp.bfloat16
f32 = jnp.float32

CORE_PAIRS = [(i, i ^ 1) for i in range(N_TP)]


def call(kernel, out_shape, scratch=(), scalars=0, arrays=0, specs=None, outs=None):
    extra = {"out_specs": outs} if outs else {}
    if scalars:
        smem = pl.BlockSpec(memory_space=pltpu.SMEM)
        specs = [smem] * scalars + [pl.BlockSpec(memory_space=pltpu.VMEM)] * arrays
    if specs:
        extra["in_specs"] = specs
    return pl.pallas_call(
        kernel,
        out_shape=out_shape,
        scratch_shapes=list(scratch),
        compiler_params=pltpu.CompilerParams(vmem_limit_bytes=16 * 1024 * 1024),
        **extra,
    )


def head_tile(tile, gain, cosine, sine_up, sine_down):
    scale = lax.rsqrt(jnp.sum(tile * tile, axis=-1, keepdims=True) * (1.0 / QK_DIM) + epsilon)
    tile = tile * scale * gain
    half = QK_ROPE // 2
    return (
        tile * cosine
        + pltpu.roll(tile, LANES - half, 1) * sine_up
        + pltpu.roll(tile, half, 1) * sine_down
    )


def copy_all(pairs, sems):
    copies = [
        pltpu.make_async_copy(source, target, sems.at[n]) for n, (source, target) in enumerate(pairs)
    ]
    for copy in copies:
        copy.start()
    for copy in copies:
        copy.wait()


def pack_kernel(qd_ref, md_ref, ku_ref, vu_ref, rope_ref, gain_ref, tok_ref, ho_ref, co_ref, narrow_ref, rope_out, gain_out, tok_out, outw_ref, sems):
    pairs = [
        (qd_ref, narrow_ref.at[:96, :]),
        (md_ref, narrow_ref.at[96:160, :]),
        (rope_ref, rope_out),
        (gain_ref, gain_out),
    ]
    for n, ref in enumerate((ku_ref, vu_ref)):
        for b in range(2):
            at = (2 * n + b) * LANES
            pairs.append((ref.at[b * 64 : (b + 1) * 64, :], narrow_ref.at[160:, at : at + LANES]))
    pairs += [(ho_ref, outw_ref.at[:128, :]), (co_ref, outw_ref.at[128:, :]), (tok_ref, tok_out)]
    copy_all(pairs, sems)


def pack_rest_kernel(qu_ref, cv_ref, cg_ref, first_ref, second_ref, qu_scr, sems):
    pairs = [(qu_ref, qu_scr)]
    for ref, out in ((cv_ref, first_ref), (cg_ref, second_ref)):
        for b in range(4):
            rows = slice(b * 128, (b + 1) * 128)
            pairs.append((ref.at[rows, :], out.at[:128, rows]))
    copy_all(pairs, sems)
    first_ref[128:, :] = jnp.zeros((96, 512), bf16)
    for half in range(2):
        for h in range(2):
            at = half * 256 + h * LANES
            first_ref[128:, at : at + QK_DIM] = qu_scr[
                half * 96 : (half + 1) * 96, h * QK_DIM : (h + 1) * QK_DIM
            ]


def project_kernel(tok_ref, gain_ref, rope_w_ref, cos_ref, sin_ref, w_ref, lat_ref, rope_ref, normed_ref, cosine_ref, up_ref, down_ref):
    block = 64
    turned = (((1,), (1,)), ((), ()))
    for r in range(0, ROWS, block):
        rows = tok_ref[r : r + block, :].astype(f32)
        scale = lax.rsqrt(jnp.mean(rows * rows, axis=-1, keepdims=True) + epsilon)
        normed_ref[r : r + block, :] = (rows * scale * gain_ref[...]).astype(bf16)
    both = jnp.zeros((ROWS, 160), f32)
    for f in range(N_FS):
        both = both + lax.dot_general(
            normed_ref[:, f * 512 : (f + 1) * 512],
            w_ref[f, :160, :],
            turned,
            preferred_element_type=f32,
        )
    both = both.astype(bf16)
    lat_ref[:ROWS, :] = both[:, :LANES]
    for r in range(4):
        lat_ref[ROWS:, r * 32 : (r + 1) * 32] = both[r * 64 : (r + 1) * 64, LANES:]
    rope = lax.dot_general(normed_ref[...], rope_w_ref[...], turned, preferred_element_type=f32)
    rope_ref[...] = jnp.zeros((ROWS, LANES), bf16)
    rope_ref[:, QK_NOPE:QK_DIM] = rope.astype(bf16)
    half = QK_ROPE // 2
    empty = jnp.zeros((ROWS, LANES - half), f32)
    cosine = jnp.concatenate([cos_ref[...].T, empty], axis=1)
    sine = jnp.concatenate([sin_ref[...].T, empty], axis=1)
    lane = lax.broadcasted_iota(jnp.int32, (ROWS, LANES), 1)
    cosine = pltpu.roll(cosine, QK_NOPE, 1) + pltpu.roll(cosine, QK_NOPE + half, 1)
    cosine_ref[...] = jnp.where(lane < QK_NOPE, 1.0, cosine)
    up_ref[...] = -pltpu.roll(sine, QK_NOPE, 1)
    down_ref[...] = pltpu.roll(sine, QK_NOPE + half, 1)


def keys_values_kernel(lat_ref, rope_ref, w_ref, mgain_ref, kgain_ref, cos_ref, up_ref, down_ref, out_ref, m_scr, w_scr):
    for g in range(N_TP):
        at = g * 64
        m_scr[:, at : at + 32] = lat_ref[g, :ROWS, 96:]
        for r in range(4):
            m_scr[r * 64 : (r + 1) * 64, at + 32 : at + 64] = lat_ref[
                g, ROWS:, r * 32 : (r + 1) * 32
            ]
    raw = m_scr[...].astype(f32)
    scale = lax.rsqrt(jnp.mean(raw * raw, axis=-1, keepdims=True) + epsilon)
    m_scr[...] = (raw * scale * mgain_ref[...]).astype(bf16)
    for f in range(N_FS):
        for n in range(2):
            for b in range(2):
                lanes = (2 * n + b) * LANES
                row = f * 128 + b * 64
                w_scr[row : row + 64, n * LANES : (n + 1) * LANES] = w_ref[
                    f, 160:, lanes : lanes + LANES
                ]
    both = jnp.dot(m_scr[...], w_scr[...], preferred_element_type=f32)
    nope = both[:, :LANES]
    lane = lax.broadcasted_iota(jnp.int32, (ROWS, LANES), 1)
    rope = rope_ref[...].astype(f32)
    tiles = []
    for h in range(2):
        part = nope if h == 0 else pltpu.roll(nope, 64, 1)
        tile = jnp.where(lane < QK_NOPE, part, rope)
        tiles.append(head_tile(tile, kgain_ref[...], cos_ref[...], up_ref[...], down_ref[...]))
    for h in range(2):
        out_ref[h * ROWS : (h + 1) * ROWS, :] = tiles[h].astype(bf16)
    values = both[:, LANES:].T.astype(bf16)
    for half in range(2):
        at = 2 * ROWS + half * LANES
        out_ref[at : at + LANES, :] = values[:, half * LANES : (half + 1) * LANES]


def queries_kernel(lat_ref, w_ref, lgain_ref, qgain_ref, cos_ref, up_ref, down_ref, out_ref, q_scr):
    for g in range(N_TP):
        q_scr[:, g * 96 : (g + 1) * 96] = lat_ref[g, :ROWS, :96]
    raw = q_scr[...].astype(f32)
    scale = lax.rsqrt(jnp.mean(raw * raw, axis=-1, keepdims=True) + epsilon)
    q_scr[...] = (raw * scale * lgain_ref[...]).astype(bf16)
    both = jnp.zeros((ROWS, 2 * LANES), f32)
    for f in range(N_FS):
        for half in range(2):
            at = f * 192 + half * 96
            both = both + jnp.dot(
                q_scr[:, at : at + 96],
                w_ref[f, 128:, half * 256 : (half + 1) * 256],
                preferred_element_type=f32,
            )
    lane = lax.broadcasted_iota(jnp.int32, (ROWS, LANES), 1)
    tiles = [
        head_tile(
            both[:, h * LANES : (h + 1) * LANES],
            qgain_ref[...],
            cos_ref[...],
            up_ref[...],
            down_ref[...],
        )
        for h in range(2)
    ]
    for h in range(2):
        out_ref[:, h * LANES : (h + 1) * LANES] = tiles[h].astype(bf16)


def gated_kernel(normed_ref, value_ref, gate_ref, out_ref):
    value = jnp.zeros((ROWS, LANES), f32)
    gate = jnp.zeros((ROWS, LANES), f32)
    for f in range(N_FS):
        for b in range(4):
            rows = normed_ref[:, f * 512 + b * LANES : f * 512 + (b + 1) * LANES]
            cols = slice(b * LANES, (b + 1) * LANES)
            value = value + jnp.dot(rows, value_ref[f, :128, cols], preferred_element_type=f32)
            gate = gate + jnp.dot(rows, gate_ref[f, :128, cols], preferred_element_type=f32)
    out_ref[...] = (value * jax.nn.sigmoid(gate)).astype(bf16)


def conv_kernel_body(halo_ref, gated_ref, taps_ref, gain_ref, shift_ref, out_ref, ext_scr, stat_scr):
    ext_scr[:HALO, :] = halo_ref[...].astype(f32)
    ext_scr[HALO:, :] = gated_ref[...].astype(f32)
    start = HALO - (TAPS - 1)
    block = LANES
    stat_scr[...] = jnp.zeros((16, LANES), f32)
    for n in range(ROWS // block):
        r = n * block
        running = jnp.zeros((block, LANES), f32)
        for j in range(TAPS):
            running = running + ext_scr[pl.ds(r + start + j, block), :] * taps_ref[j : j + 1, :]
        flat = running.T
        mean = jnp.sum(flat, axis=0, keepdims=True) * (1.0 / LANES)
        off = flat - mean
        stat_scr[n : n + 1, :] = mean
        stat_scr[2 + n : 3 + n, :] = jnp.sum(off * off, axis=0, keepdims=True)
        out_ref[r : r + block, :] = off.T.astype(bf16)
    stat_scr[4:5, :] = gain_ref[...]
    stat_scr[5:6, :] = shift_ref[...]
    left = stat_scr[...]
    for part in range(3):
        rounded = left.astype(bf16)
        out_ref[ROWS + part * 16 : ROWS + (part + 1) * 16, :] = rounded
        left = left - rounded.astype(f32)


def channel_kernel(in_ref, out_ref):
    stats = []
    for g in range(N_TP):
        parts = [
            in_ref[g, ROWS + part * 16 : ROWS + (part + 1) * 16, :].astype(f32) for part in range(3)
        ]
        stats.append(parts[0] + (parts[1] + parts[2]))
    for n in range(ROWS // LANES):
        means = [st[n : n + 1] for st in stats]
        mean = means[0]
        for g in range(1, N_TP):
            mean = mean + means[g]
        mean = mean * (1.0 / N_TP)
        spread = jnp.zeros((1, LANES), f32)
        for g in range(N_TP):
            apart = means[g] - mean
            spread = spread + stats[g][2 + n : 3 + n] + LANES * apart * apart
        scale = lax.rsqrt(spread * (1.0 / CONV_W) + epsilon)
        columns = jnp.concatenate(
            [m - mean for m in means] + [scale] + [jnp.zeros((7, LANES), f32)], axis=0
        ).T
        rows = slice(n * LANES, (n + 1) * LANES)
        for g in range(N_TP):
            value = in_ref[g, rows, :].astype(f32) + columns[:, g : g + 1]
            value = value * columns[:, N_TP : N_TP + 1] * stats[g][4:5] + stats[g][5:6]
            out_ref[g, rows, :] = (value / (1.0 + jnp.exp(-value))).astype(bf16)


def attend(q_ref, blocks, state, hidden, mask=None):
    rate = QK_DIM ** (-0.5) * log2_e
    fresh = []
    for h in range(2):
        top, total, weighted = state[h]
        keys = jnp.concatenate([b[h * ROWS : (h + 1) * ROWS, :] for b in blocks], axis=0)
        scores = lax.dot_general(
            keys,
            q_ref[:, h * LANES : (h + 1) * LANES],
            (((1,), (1,)), ((), ())),
            preferred_element_type=f32,
        )
        if mask is not None:
            scores = jnp.where(mask, scores, masked_score)
        new_top = top
        for n, off in enumerate(hidden):
            part = jnp.max(scores[n * ROWS : (n + 1) * ROWS], axis=0, keepdims=True)
            new_top = jnp.maximum(new_top, part - off)
        weights = jnp.concatenate(
            [
                jnp.exp2(scores[n * ROWS : (n + 1) * ROWS] * rate - (new_top * rate + off))
                for n, off in enumerate(hidden)
            ],
            axis=0,
        )
        factor = jnp.exp2((top - new_top) * rate)
        total = total * factor + jnp.sum(weights, axis=0, keepdims=True)
        at = 2 * ROWS + h * V_DIM
        values = jnp.concatenate(
            [b[at + i * LANES : at + i * LANES + V_DIM, :] for b in blocks for i in range(2)],
            axis=1,
        )
        weighted = weighted * factor + jnp.dot(
            values, weights.astype(bf16), preferred_element_type=f32
        )
        fresh.append((new_top, total, weighted))
    return fresh


def own_kernel(q_ref, own_ref, stat_ref, acc_ref):
    key = lax.broadcasted_iota(jnp.int32, (ROWS, ROWS), 0)
    query = lax.broadcasted_iota(jnp.int32, (ROWS, ROWS), 1)
    mask = jnp.right_shift(key, 6) <= jnp.right_shift(query, 6)
    empty = (
        jnp.full((1, ROWS), masked_score, f32),
        jnp.zeros((1, ROWS), f32),
        jnp.zeros((V_DIM, ROWS), f32),
    )
    state = attend(q_ref, [own_ref], [empty, empty], [0.0], mask)
    stat_ref[4:, :] = jnp.zeros((4, ROWS), f32)
    for h in range(2):
        stat_ref[2 * h : 2 * h + 1, :] = state[h][0]
        stat_ref[2 * h + 1 : 2 * h + 2, :] = state[h][1]
        acc_ref[h * V_DIM : (h + 1) * V_DIM, :] = state[h][2]


def attention_kernel(at_ref, q_ref, kv_ref, stat_ref, acc_ref, *rest):
    pieces, (out_ref, weight_ref, kv, sems, weight_sems) = rest[:N_TP], rest[N_TP:]
    at = at_ref[0]
    copies = [
        pltpu.make_async_copy(kv_ref.at[n], kv.at[n], sems.at[n]) for n in range(N_SP // BUNDLE)
    ]
    for n, copy in enumerate(copies):
        pl.when(n * BUNDLE < at)(copy.start)
    fetched = [
        pltpu.make_async_copy(piece.at[:, :128, :], weight_ref.at[n], weight_sems.at[n])
        for n, piece in enumerate(pieces)
    ]
    for copy in fetched:
        copy.start()
    state = [
        (
            stat_ref[2 * h : 2 * h + 1, :],
            stat_ref[2 * h + 1 : 2 * h + 2, :],
            acc_ref[h * V_DIM : (h + 1) * V_DIM, :],
        )
        for h in range(2)
    ]
    for n, copy in enumerate(copies):
        hidden = [jnp.where(n * BUNDLE + i < at, 0.0, -masked_score) for i in range(BUNDLE)]
        blocks = [kv.at[n, i] for i in range(BUNDLE)]

        def visible(state, blocks=blocks, hidden=hidden, copy=copy):
            copy.wait()
            return attend(q_ref, blocks, state, hidden)

        state = lax.cond(n * BUNDLE < at, visible, lambda s: s, state)
    result = jnp.concatenate([state[h][2] / state[h][1] for h in range(2)], axis=0)
    out_ref[...] = result.T.astype(bf16)
    for copy in fetched:
        copy.wait()


def sources(g):
    other = g + 1 - 2 * lax.rem(g, 2)
    return [lax.rem(first + N_TP - s, N_TP) for first in (g, other) for s in (0, 2, 4, 6)]


def conv_part_kernel(tp_ref, conv_ref, *rest):
    pieces, (out_ref, weights, sems) = rest[:N_TP], rest[N_TP:]
    fetched = [
        pltpu.make_async_copy(piece.at[:, 128:, :], weights.at[n], sems.at[n])
        for n, piece in enumerate(pieces)
    ]
    for copy in fetched:
        copy.start()
    for n, g in enumerate(sources(tp_ref[0])):
        fetched[n].wait()
        left = conv_ref[g]
        for f in range(N_FS):
            cols = slice(f * 512, (f + 1) * 512)
            part = jnp.dot(left, weights[n, f], preferred_element_type=f32)
            out_ref[:, cols] = part if n == 0 else out_ref[:, cols] + part


def output_kernel(tp_ref, base_ref, attn_ref, weight_ref, out_ref):
    owners = sources(tp_ref[0])
    left = jnp.concatenate([attn_ref[g] for g in owners], axis=1)
    for f in range(N_FS):
        cols = slice(f * 512, (f + 1) * 512)
        weight = jnp.concatenate([weight_ref[n, f] for n in range(N_TP)], axis=0)
        total = base_ref[:, cols] + jnp.dot(left, weight, preferred_element_type=f32)
        out_ref[:, cols] = total.astype(bf16)


def rotation_tables(positions):
    inverse_freq = 1.0 / rope_base ** (jnp.arange(0, QK_ROPE, 2, dtype=f32) / QK_ROPE)
    angles = positions.astype(f32)[None, :] * inverse_freq[:, None]
    return jnp.cos(angles), jnp.sin(angles)


def local(
    tokens,
    mix_gain,
    query_down,
    memory_down,
    rope_weight,
    query_up,
    key_up,
    value_up,
    latent_gain,
    memory_gain,
    query_gain,
    key_gain,
    conv_value,
    conv_gate,
    conv_kernel,
    channel_gain,
    channel_shift,
    heads_out,
    conv_out,
):
    at = lax.axis_index("sp")
    hbm = pl.BlockSpec(memory_space=pltpu.HBM)
    vmem = pl.BlockSpec(memory_space=pltpu.VMEM)
    def kept(*arrays):
        return [pltpu.with_memory_space_constraint(a, pltpu.HBM) for a in arrays]

    narrow, rope_w, gain, own_rows, outw = call(
        pack_kernel,
        (
            jax.ShapeDtypeStruct((224, 512), bf16),
            jax.ShapeDtypeStruct((QK_ROPE, 2048), bf16),
            jax.ShapeDtypeStruct((1, 2048), f32),
            jax.ShapeDtypeStruct((ROWS, 2048), bf16),
            jax.ShapeDtypeStruct((256, 512), bf16),
        ),
        [pltpu.SemaphoreType.DMA((11,))],
        specs=[hbm] * 9,
    )(
        *kept(
            query_down.T, memory_down.T, key_up, value_up, rope_weight.T, mix_gain[None, :],
            tokens[0], heads_out, conv_out,
        )
    )
    out_all = lax.all_gather(outw, "fs")
    narrow_all = lax.all_gather(narrow, "fs")
    positions = at * ROWS + jnp.arange(ROWS, dtype=jnp.int32)
    cosine, sine = rotation_tables(positions)
    table = jax.ShapeDtypeStruct((ROWS, LANES), f32)
    latents, rope_rows, normed, cosine, sine_up, sine_down = call(
        project_kernel,
        (
            jax.ShapeDtypeStruct((320, LANES), bf16),
            jax.ShapeDtypeStruct((ROWS, LANES), bf16),
            jax.ShapeDtypeStruct((ROWS, 2048), bf16),
            table,
            table,
            table,
        ),
    )(own_rows, gain, rope_w, cosine, sine, narrow_all)
    latents = lax.all_gather(latents, "tp")

    def row(vector, width):
        return jnp.pad(vector, (0, width - vector.shape[0]))[None, :]

    own = call(
        keys_values_kernel,
        jax.ShapeDtypeStruct((6 * LANES, LANES), bf16),
        [pltpu.VMEM((ROWS, KV_LAT), bf16), pltpu.VMEM((KV_LAT, 256), bf16)],
    )(
        latents, rope_rows, narrow_all, memory_gain[None, :], row(key_gain, LANES),
        cosine, sine_up, sine_down,
    )
    tp, at = lax.axis_index("tp")[None], at[None]
    own, out_all, tp, at, *rest = lax.optimization_barrier(
        (own, out_all, tp, at, query_up, conv_value, conv_gate)
    )
    pieces = lax.all_gather(own, "sp")
    far = [
        lax.ppermute(out_all, "tp", [(i, (i + by) % N_TP) for i in range(N_TP)]) for by in (4, 2, 6)
    ]
    far = [far[1], far[0], far[2]]
    near = lax.ppermute(out_all, "tp", CORE_PAIRS)
    packed = call(
        pack_rest_kernel,
        tuple(jax.ShapeDtypeStruct((rows, 512), bf16) for rows in (224, 128)),
        [pltpu.VMEM((192, 192), bf16), pltpu.SemaphoreType.DMA((9,))],
        specs=[hbm] * 3,
    )(*kept(*rest))
    first_all, second_all = (lax.all_gather(p, "fs") for p in packed)
    queries = call(
        queries_kernel,
        jax.ShapeDtypeStruct((ROWS, 2 * LANES), bf16),
        [pltpu.VMEM((ROWS, Q_LAT), bf16)],
    )(
        latents, first_all, latent_gain[None, :], row(query_gain, LANES),
        cosine, sine_up, sine_down,
    )
    gated = call(gated_kernel, jax.ShapeDtypeStruct((ROWS, LANES), bf16))(normed, first_all, second_all)
    halo = lax.ppermute(gated[ROWS - HALO :], "sp", [(i, i + 1) for i in range(N_SP - 1)])
    stat, acc = call(
        own_kernel,
        (jax.ShapeDtypeStruct((8, ROWS), f32), jax.ShapeDtypeStruct((2 * V_DIM, ROWS), f32)),
    )(queries, own)
    halo, stat, acc = lax.optimization_barrier((halo, stat, acc))
    taps = jnp.pad(conv_kernel.astype(f32), ((0, 1), (0, 0)))
    conv_sum = call(
        conv_kernel_body,
        jax.ShapeDtypeStruct((ROWS + 48, LANES), bf16),
        [pltpu.VMEM((ROWS + HALO, LANES), f32), pltpu.VMEM((16, LANES), f32)],
    )(halo, gated, taps, channel_gain[None, :], channel_shift[None, :])
    conv_sum = lax.all_gather(conv_sum, "tp")
    conv_sum, near, *far = lax.optimization_barrier((conv_sum, near, *far))
    crossed = [lax.ppermute(w, "tp", CORE_PAIRS) for w in far]
    weights = kept(out_all, *far, near, *crossed)
    half = (N_TP, N_FS, 128, 512)
    conv_result = call(channel_kernel, jax.ShapeDtypeStruct((N_TP, ROWS, LANES), bf16))(conv_sum)
    base = call(
        conv_part_kernel,
        jax.ShapeDtypeStruct((ROWS, 2048), f32),
        [pltpu.VMEM(half, bf16), pltpu.SemaphoreType.DMA((N_TP,))],
        specs=[pl.BlockSpec(memory_space=pltpu.SMEM), vmem] + [hbm] * N_TP,
    )(tp, conv_result, *weights)
    pieces, base, stat, acc = lax.optimization_barrier((pieces, base, stat, acc))
    pieces = pltpu.with_memory_space_constraint(
        pieces.reshape(N_SP // BUNDLE, BUNDLE, 6 * LANES, LANES), pltpu.HBM
    )
    attention, weights = call(
        attention_kernel,
        (jax.ShapeDtypeStruct((ROWS, LANES), bf16), jax.ShapeDtypeStruct(half, bf16)),
        [
            pltpu.VMEM((N_SP // BUNDLE, BUNDLE, 6 * LANES, LANES), bf16),
            pltpu.SemaphoreType.DMA((N_SP // BUNDLE,)),
            pltpu.SemaphoreType.DMA((N_TP,)),
        ],
        specs=[pl.BlockSpec(memory_space=pltpu.SMEM), vmem, hbm, vmem, vmem] + [hbm] * N_TP,
    )(at, queries, pieces, stat, acc, *weights)
    attention = lax.all_gather(attention, "tp")
    mixed = call(
        output_kernel, jax.ShapeDtypeStruct((ROWS, 2048), bf16), scalars=1, arrays=3
    )(tp, base, attention, weights)
    return mixed[None]


def solution(mesh):
    in_specs = (
        P("fs", "sp", None),
        P(),
        P("fs", "tp"),
        P("fs", "tp"),
        P(),
        P("fs", "tp"),
        P("fs", "tp"),
        P("fs", "tp"),
        P(),
        P(),
        P(),
        P(),
        P("fs", "tp"),
        P("fs", "tp"),
        P(None, "tp"),
        P("tp"),
        P("tp"),
        P("tp", "fs"),
        P("tp", "fs"),
    )
    out_specs = P("fs", "sp", None)
    return jax.shard_map(local, mesh=mesh, in_specs=in_specs, out_specs=out_specs, check_vma=False)
```
